32 devices in a mesh: fs: 16 (over z, y, core), tp: 2 (over x).
Axes of the slice: x: 2, y: 2, z: 4, core: 2. Of those that a mesh axis runs over, the one named last changes fastest.
Arguments:
- tokens: bfloat16 [4096, 2048], P('fs', 'tp'), may hold values from -16 to 16, as said below
- mix_gain: bfloat16 [2048], P('tp'), may hold values from 0.099609375 to 1.8984375
- query_weight: bfloat16 [2048, 512], P('fs', 'tp'), may hold values from -0.125 to 0.125
- key_weight: bfloat16 [2048, 512], P('fs', 'tp'), may hold values from -0.125 to 0.125
- value_weight: bfloat16 [2048, 1024], P('fs', 'tp'), may hold values from -0.125 to 0.125
- output_gate_weight: bfloat16 [2048, 1024], P('fs', 'tp'), may hold values from -0.125 to 0.125
- out_weight: bfloat16 [1024, 2048], P('tp', 'fs'), may hold values from -0.1875 to 0.1875
- head_rates: float32 [8], P('tp'), may hold values from 0 to 1, as said below
- block_scale: float32 [32], P('fs'), may hold values from 0.5 to 2
- ffn_gain: bfloat16 [2048], P('tp'), may hold values from 0.099609375 to 1.8984375
- ff_gate: bfloat16 [2048, 5632], P('fs', 'tp'), may hold values from -0.125 to 0.125
- ff_up: bfloat16 [2048, 5632], P('fs', 'tp'), may hold values from -0.125 to 0.125
- ff_down: bfloat16 [5632, 2048], P('tp', 'fs'), may hold values from -0.078125 to 0.078125
- final_gain: bfloat16 [2048], P('tp'), may hold values from 0.099609375 to 1.8984375
Outputs:
- layer_out: bfloat16 [4096, 2048], P('fs', 'tp')
The draws below stay inside these ranges and needn't reach their ends.
Inputs may be any that keep to these rules, and one draw needn't show every extreme that they name: `tokens`: column blocks of the activations have different scales. `head_rates`: positive rates.
All inputs are finite; a program needn't handle non-finite values.
Results may differ from the reference program's by a relative error of at most 0.014.
Values may be sent and summed in bfloat16 or wider, within the bound.
A program may use at most 128 MiB of HBM per device.

```python
import math
import jax
import jax.numpy as jnp
from jax import lax

D = 2048
HEADS = 8
DK = 64
DV = 128
FF = 5632
BLK = 128
SEQ_LEN = 256
TOKENS = 4096
N_TP = 2


def draw_tokens(key, part):
    first, second, third = jax.random.split(jax.random.fold_in(key, 11), 3)
    groups = 2 * N_TP
    scales = jnp.exp(jax.random.uniform(second, (groups,), jnp.float32, -1.2, 1.2))
    base = jnp.clip(jax.random.normal(first, (TOKENS, D), jnp.float32), -4.0, 4.0)
    shaped = base.reshape(TOKENS, groups, D // groups) * scales[None, :, None]
    return shaped.reshape(TOKENS, D).astype(jnp.bfloat16)


def draw_head_rates(key, part):
    first, second, third = jax.random.split(jax.random.fold_in(key, 23), 3)
    fast = jax.random.uniform(first, (HEADS,), jnp.float32, 2.8, 4.3) / BLK
    slow = jax.random.uniform(second, (HEADS,), jnp.float32, 0.3, 1.0) / SEQ_LEN
    order = jax.random.permutation(third, HEADS)
    quick = order < HEADS // 2
    return jnp.where(quick, fast, slow).astype(jnp.float32)


def block_levels(own_key, dims, cuts, low, largest):
    level, own = 1.0, jax.random.fold_in(own_key, 6)
    for dim, parts in cuts:
        heights = jnp.exp(jax.random.uniform(jax.random.fold_in(own, dim), (parts,), jnp.float32, low / len(cuts), largest / len(cuts)))
        level = level * jnp.repeat(heights, dims[dim] // parts).reshape([-1 if axis == dim else 1 for axis in range(len(dims))])
    return level


def noise(rng, extent, scale, limit, shards=(), held_as=jnp.bfloat16):
    drawn = scale * jax.random.normal(rng, extent, jnp.float32)
    if shards:
        drawn = drawn * block_levels(rng, extent, shards, -0.22, 0.18)
    return jnp.clip(drawn, -limit, limit).astype(held_as)


def setup_inputs(seed: int = 0) -> dict:
    seeds = jax.random.split(jax.random.key(seed), 15)
    tokens = draw_tokens(jax.random.fold_in(seeds[14], 71), 0)
    mix_gain = jnp.clip(1.0 + 0.18 * jax.random.normal(seeds[1], (D,), jnp.float32), 0.099609375, 1.8984375).astype(jnp.bfloat16)
    query_weight = noise(seeds[2], (D, HEADS * DK), D ** -0.5, 0.125, ((0, 16), (1, 2)))
    key_weight = noise(seeds[3], (D, HEADS * DK), D ** -0.5, 0.125, ((0, 16), (1, 2)))
    value_weight = noise(seeds[4], (D, HEADS * DV), D ** -0.5, 0.125, ((0, 16), (1, 2)))
    output_gate_weight = noise(seeds[5], (D, HEADS * DV), D ** -0.5, 0.125, ((0, 16), (1, 2)))
    out_weight = noise(seeds[6], (HEADS * DV, D), (HEADS * DV) ** -0.5, 0.1875, ((0, 2), (1, 16)))
    head_rates = draw_head_rates(jax.random.fold_in(seeds[14], 71), 0)
    block_scale = jnp.clip(jnp.exp(math.log(2.0) - 1.3862944 * jax.random.uniform(seeds[8], (TOKENS // BLK,), jnp.float32) ** block_levels(seeds[8], (TOKENS // BLK,), ((0, 16),), -0.2, 0.2)), 0.5, 2.0)
    ffn_gain = jnp.clip(1.0 + 0.18 * jax.random.normal(seeds[9], (D,), jnp.float32), 0.099609375, 1.8984375).astype(jnp.bfloat16)
    ff_gate = noise(seeds[10], (D, FF), D ** -0.5, 0.125, ((0, 16), (1, 2)))
    ff_up = noise(seeds[11], (D, FF), D ** -0.5, 0.125, ((0, 16), (1, 2)))
    ff_down = noise(seeds[12], (FF, D), FF ** -0.5, 0.078125, ((0, 2), (1, 16)))
    final_gain = jnp.clip(1.0 + 0.18 * jax.random.normal(seeds[13], (D,), jnp.float32), 0.099609375, 1.8984375).astype(jnp.bfloat16)
    return dict(tokens=tokens, mix_gain=mix_gain, query_weight=query_weight, key_weight=key_weight, value_weight=value_weight, output_gate_weight=output_gate_weight, out_weight=out_weight, head_rates=head_rates, block_scale=block_scale, ffn_gain=ffn_gain, ff_gate=ff_gate, ff_up=ff_up, ff_down=ff_down, final_gain=final_gain)


EPS = 1e-06
THETA = 10000.0

def rms_norm(values, gain):
    scale = lax.rsqrt(lax.optimization_barrier(jnp.mean(values * values, axis=-1, keepdims=True)) + EPS)
    return values * scale * gain.astype(jnp.float32)

def rotate(values, positions):
    half = values.shape[-1] // 2
    inverse = THETA ** (-jnp.arange(half, dtype=jnp.float32) / half)
    angle = positions.astype(jnp.float32)[:, None] * inverse
    cosine = jnp.cos(angle)[:, None, :]
    sine = jnp.sin(angle)[:, None, :]
    first = values[..., :half]
    second = values[..., half:]
    return jnp.concatenate([first * cosine - second * sine, second * cosine + first * sine], axis=-1)

def retain(query, key, value, rates, scales):
    rows, heads_here, width_k = query.shape
    width_v = value.shape[-1]
    nblk = rows // BLK
    hi = lax.Precision.HIGHEST
    qblk = query.astype(jnp.float32).reshape(nblk, BLK, heads_here, width_k)
    kblk = key.astype(jnp.float32).reshape(nblk, BLK, heads_here, width_k)
    vblk = value.astype(jnp.float32).reshape(nblk, BLK, heads_here, width_v)
    logdec = -rates[None, :] * scales[:, None]
    steps = jnp.arange(BLK, dtype=jnp.float32)
    offset = steps[:, None] - steps[None, :]
    causal = offset >= 0
    inside = jnp.where(causal[None, None], jnp.exp(logdec[:, :, None, None] * jnp.where(causal, offset, 0.0)[None, None]), 0.0)
    scores = jnp.einsum('nchd,nmhd->nhcm', qblk, kblk, precision=hi) * inside
    inner = jnp.einsum('nhcm,nmhe->nche', scores, vblk, precision=hi)
    zeta = jnp.exp(logdec[:, :, None] * (BLK - 1.0 - steps)[None, None, :])
    kv_block = jnp.einsum('nchd,nche->nhde', kblk * jnp.transpose(zeta, (0, 2, 1))[..., None], vblk, precision=hi)
    hold = jnp.exp(logdec * BLK)
    per_seq = SEQ_LEN // BLK
    fresh = (jnp.arange(nblk, dtype=jnp.int32) % per_seq == 0).astype(jnp.float32)

    def advance(state, inputs):
        kv_now, hold_now, fresh_now = inputs
        before = state * (1.0 - fresh_now)
        return (before * hold_now[:, None, None] + kv_now, before)
    start = jnp.zeros((heads_here, width_k, width_v), jnp.float32)
    _, before = lax.scan(advance, start, (kv_block, hold, fresh))
    xi = jnp.exp(logdec[:, :, None] * (steps + 1.0)[None, None, :])
    cross = jnp.einsum('nchd,nhde->nche', qblk * jnp.transpose(xi, (0, 2, 1))[..., None], before, precision=hi)
    total = inner + cross
    total = total * lax.rsqrt(lax.optimization_barrier(jnp.mean(total * total, axis=-1, keepdims=True)) + EPS)
    return total.reshape(rows, heads_here, width_v)

def grouped_product(left, right, groups):
    width = left.shape[1] // groups
    result = jnp.zeros((left.shape[0], right.shape[1]), jnp.float32)
    for index in range(groups):
        partial_sum = jnp.dot(left[:, index * width:(index + 1) * width], right[index * width:(index + 1) * width], preferred_element_type=jnp.float32)
        result = result + partial_sum.astype(jnp.bfloat16).astype(jnp.float32)
    return result

def reference(tokens, mix_gain, query_weight, key_weight, value_weight, output_gate_weight, out_weight, head_rates, block_scale, ffn_gain, ff_gate, ff_up, ff_down, final_gain):
    rows = tokens.shape[0]
    positions = jnp.arange(rows, dtype=jnp.int32) % SEQ_LEN
    normed = rms_norm(tokens.astype(jnp.float32), mix_gain).astype(jnp.bfloat16)
    qproj = jnp.dot(normed, query_weight, preferred_element_type=jnp.float32).reshape(rows, HEADS, DK)
    kproj = jnp.dot(normed, key_weight, preferred_element_type=jnp.float32).reshape(rows, HEADS, DK)
    vproj = jnp.dot(normed, value_weight, preferred_element_type=jnp.float32)
    gproj = jnp.dot(normed, output_gate_weight, preferred_element_type=jnp.float32)
    query = rotate(qproj, positions).astype(jnp.bfloat16)
    key = (rotate(kproj, positions) * DK ** (-0.5)).astype(jnp.bfloat16)
    value = vproj.astype(jnp.bfloat16).reshape(rows, HEADS, DV)
    normret = retain(query, key, value, head_rates, block_scale).reshape(rows, HEADS * DV)
    gated = (normret * jax.nn.silu(gproj)).astype(jnp.bfloat16)
    mix = grouped_product(gated, out_weight, N_TP)
    resid = (tokens.astype(jnp.float32) + mix).astype(jnp.bfloat16)
    normed2 = rms_norm(resid.astype(jnp.float32), ffn_gain).astype(jnp.bfloat16)
    gate_part = jnp.dot(normed2, ff_gate, preferred_element_type=jnp.float32)
    up_part = jnp.dot(normed2, ff_up, preferred_element_type=jnp.float32)
    hidden = (jax.nn.silu(gate_part) * up_part).astype(jnp.bfloat16)
    ffn = grouped_product(hidden, ff_down, N_TP)
    total = resid.astype(jnp.float32) + ffn
    return rms_norm(total, final_gain).astype(jnp.bfloat16)
```

```python
import functools

import jax
import jax.numpy as jnp
import numpy as np
from jax import lax
from jax.experimental import pallas as pl
from jax.experimental.pallas import tpu as pltpu
from jax.sharding import PartitionSpec as P

D = 2048
DK = 64
DV = 128
BLK = 128
SEQ_LEN = 256


EPS = 1e-06
THETA = 10000.0


def rms_norm(values, gain):
    scale = lax.rsqrt(jnp.mean(values * values, axis=-1, keepdims=True) + EPS)
    return values * scale * gain.astype(jnp.float32)


def rotate(values, positions):
    half = values.shape[-1] // 2
    inverse = THETA ** (-jnp.arange(half, dtype=jnp.float32) / half)
    angle = positions.astype(jnp.float32)[:, None] * inverse
    cosine = jnp.cos(angle)[:, None, :]
    sine = jnp.sin(angle)[:, None, :]
    first = values[..., :half]
    second = values[..., half:]
    return jnp.concatenate(
        [first * cosine - second * sine, second * cosine + first * sine], axis=-1
    )


def retain(query, key, value, rates, scales):
    rows, heads_here, width_k = query.shape
    width_v = value.shape[-1]
    nblk = rows // BLK
    hi = lax.Precision.HIGHEST
    qblk = query.astype(jnp.float32).reshape(nblk, BLK, heads_here, width_k)
    kblk = key.astype(jnp.float32).reshape(nblk, BLK, heads_here, width_k)
    vblk = value.astype(jnp.float32).reshape(nblk, BLK, heads_here, width_v)
    logdec = -rates[None, :] * scales[:, None]
    steps = jnp.arange(BLK, dtype=jnp.float32)
    offset = steps[:, None] - steps[None, :]
    causal = offset >= 0
    inside = jnp.where(
        causal[None, None],
        jnp.exp(logdec[:, :, None, None] * jnp.where(causal, offset, 0.0)[None, None]),
        0.0,
    )
    scores = jnp.einsum("nchd,nmhd->nhcm", qblk, kblk, precision=hi) * inside
    inner = jnp.einsum("nhcm,nmhe->nche", scores, vblk, precision=hi)
    zeta = jnp.exp(logdec[:, :, None] * (BLK - 1.0 - steps)[None, None, :])
    kv_block = jnp.einsum(
        "nchd,nche->nhde", kblk * jnp.transpose(zeta, (0, 2, 1))[..., None], vblk, precision=hi
    )
    hold = jnp.exp(logdec * BLK)
    per_seq = SEQ_LEN // BLK
    fresh = (jnp.arange(nblk, dtype=jnp.int32) % per_seq == 0).astype(jnp.float32)

    def advance(state, inputs):
        kv_now, hold_now, fresh_now = inputs
        before = state * (1.0 - fresh_now)
        return (before * hold_now[:, None, None] + kv_now, before)

    start = jnp.zeros((heads_here, width_k, width_v), jnp.float32)
    _, before = lax.scan(advance, start, (kv_block, hold, fresh), unroll=True)
    xi = jnp.exp(logdec[:, :, None] * (steps + 1.0)[None, None, :])
    cross = jnp.einsum(
        "nchd,nhde->nche", qblk * jnp.transpose(xi, (0, 2, 1))[..., None], before, precision=hi
    )
    total = inner + cross
    total = total * lax.rsqrt(jnp.mean(total * total, axis=-1, keepdims=True) + EPS)
    return total.reshape(rows, heads_here * width_v)


def chip_ring(size):
    chips = size // 2
    return list(range(0, chips, 2)) + list(range(1, chips, 2))[::-1]


def ring_place(size):
    ring = chip_ring(size)
    me = lax.axis_index("fs")
    chip = me // 2
    place = jnp.zeros((), jnp.int32)
    for index, member in enumerate(ring):
        place = jnp.where(chip == member, index, place)
    return place, me % 2


def after(value, *others):
    return lax.optimization_barrier((value,) + tuple(others))[0]


def circulate(block, axis, gates=()):
    size = lax.axis_size("fs")
    ring = chip_ring(size)
    chips = len(ring)
    onward = [
        (2 * ring[i] + core, 2 * ring[(i + 1) % chips] + core)
        for i in range(chips)
        for core in range(2)
    ]
    back = [(target, source) for source, target in onward]
    swap = [(i, i ^ 1) for i in range(size)]
    held = {0: block}
    reach = (chips - 1) // 2
    down = up = block
    for step in range(1, reach + 1):
        if len(gates) >= step and gates[step - 1]:
            down = after(down, *gates[step - 1])
            up = after(up, *gates[step - 1])
        down = lax.ppermute(down, "fs", onward)
        up = lax.ppermute(up, "fs", back)
        held[-step] = down
        held[step] = up
    if chips % 2 == 0 and chips > 1:
        cut = 1 - axis
        half = block.shape[cut] // 2
        if len(gates) > reach and gates[reach]:
            down = after(down, *gates[reach])
            up = after(up, *gates[reach])
        first = lax.ppermute(lax.slice_in_dim(down, 0, half, axis=cut), "fs", onward)
        second = lax.ppermute(lax.slice_in_dim(up, half, None, axis=cut), "fs", back)
        held[reach + 1] = jnp.concatenate([first, second], axis=cut)
    groups = []
    for offsets in order_of(size):
        own = jnp.concatenate([held[o] for o in offsets], axis=axis)
        groups.append((own, lax.ppermute(own, "fs", swap)))
    return held, groups


def order_of(size):
    chips = size // 2
    reach = (chips - 1) // 2
    groups = [list(range(-reach, reach + 1))]
    if chips > 1 and chips % 2 == 0:
        groups.append([reach + 1])
    return groups


def lane_of(values, lane, wide):
    count = values.shape[1] // (2 * wide)
    return [values[:, (2 * c + lane) * wide : (2 * c + lane + 1) * wide] for c in range(count)]


def to_ring(values, place, core):
    size = lax.axis_size("fs")
    wide = values.shape[1] // size
    ring = chip_ring(size)
    chips = len(ring)
    groups = order_of(size)
    start = (place + groups[0][0] + chips) % chips
    lanes = []
    for lane in range(2):
        pieces = lane_of(values, lane, wide)
        ringed = jnp.concatenate([pieces[c] for c in ring] * 2, axis=1)
        lanes.append(lax.dynamic_slice_in_dim(ringed, start * wide, chips * wide, axis=1))
    own = jnp.where(core == 0, lanes[0], lanes[1])
    other = jnp.where(core == 0, lanes[1], lanes[0])
    result, edge = [], 0
    for offsets in groups:
        end = edge + len(offsets) * wide
        result.append((own[:, edge:end], other[:, edge:end]))
        edge = end
    return result


def from_ring(groups, place, core):
    size = lax.axis_size("fs")
    ring = chip_ring(size)
    chips = len(ring)
    own = jnp.concatenate([own for own, _ in groups], axis=1)
    other = jnp.concatenate([other for _, other in groups], axis=1)
    wide = own.shape[1] // chips
    start = (2 * chips - place - order_of(size)[0][0]) % chips
    lanes = []
    for lane in range(2):
        straight = jnp.where(core == lane, own, other)
        doubled = jnp.concatenate([straight, straight], axis=1)
        lanes.append(lax.dynamic_slice_in_dim(doubled, start * wide, chips * wide, axis=1))
    spot = {c: i for i, c in enumerate(ring)}
    return jnp.concatenate(
        [
            lanes[lane][:, spot[c] * wide : (spot[c] + 1) * wide]
            for c in range(chips)
            for lane in range(2)
        ],
        axis=1,
    )


def tp_gather(values, axis):
    if lax.axis_size("tp") != 2:
        return lax.all_gather(values, "tp", axis=axis, tiled=True)
    other = lax.ppermute(values, "tp", [(0, 1), (1, 0)])
    mine = lax.axis_index("tp") == 0
    return jnp.concatenate(
        [jnp.where(mine, values, other), jnp.where(mine, other, values)], axis=axis
    )


def tp_sum(values):
    if lax.axis_size("tp") != 2:
        return lax.psum(values, "tp")
    return values + lax.ppermute(values, "tp", [(0, 1), (1, 0)])


def tp_scatter_sum(partial):
    if lax.axis_size("tp") != 2:
        pieces = lax.all_to_all(
            partial.reshape(partial.shape[0], lax.axis_size("tp"), -1), "tp", 1, 1
        )
        return jnp.sum(pieces.astype(jnp.float32), axis=1)
    half = partial.shape[1] // 2
    low = lax.axis_index("tp") == 0
    keep = jnp.where(low, partial[:, :half], partial[:, half:])
    send = jnp.where(low, partial[:, half:], partial[:, :half])
    got = lax.ppermute(send, "tp", [(0, 1), (1, 0)])
    return keep.astype(jnp.float32) + got.astype(jnp.float32)


def product_rows(left, groups, columns=slice(None), result=0.0):
    for pieces, blocks in zip(left, groups):
        for piece, block in zip(pieces, blocks):
            result = result + jnp.dot(
                piece, block[:, columns], preferred_element_type=jnp.float32
            )
    return result


def product_columns(left, groups, place, core, columns=None):
    terms = []
    for blocks in groups:
        pair = []
        for block in blocks:
            if columns is None:
                dims, right = (((1,), (0,)), ((), ())), block
            else:
                dims, right = (((1,), (1,)), ((), ())), block[:, columns]
            term = lax.dot_general(left, right, dims, preferred_element_type=jnp.float32)
            pair.append(term.astype(jnp.bfloat16))
        terms.append(pair)
    return from_ring(terms, place, core)


def body(
    tokens,
    mix_gain,
    query_weight,
    key_weight,
    value_weight,
    output_gate_weight,
    out_weight,
    head_rates,
    block_scale,
    ffn_gain,
    ff_gate,
    ff_up,
    ff_down,
    final_gain,
):
    rows = tokens.shape[0]
    heads_here = head_rates.shape[0]
    size = lax.axis_size("fs")
    place, core = ring_place(size)
    reach = (size // 2 - 1) // 2
    positions = jnp.arange(rows, dtype=jnp.int32) % SEQ_LEN

    bundle = jnp.concatenate(
        [query_weight, key_weight, value_weight, output_gate_weight, out_weight.T], axis=1
    )
    hops, proj = circulate(bundle, 0)
    last = (hops[-reach], hops[reach])

    whole = tp_gather(tokens, 1)
    gains = tp_gather(jnp.stack([mix_gain, ffn_gain]), 1)
    normed = rms_norm(whole.astype(jnp.float32), gains[0]).astype(jnp.bfloat16)
    width = bundle.shape[1] - out_weight.shape[0]
    projected = product_rows(to_ring(normed, place, core), proj, slice(0, width))
    ends = [query_weight.shape[1], key_weight.shape[1], value_weight.shape[1]]
    qproj, kproj, vproj, gproj = jnp.split(
        projected, [ends[0], ends[0] + ends[1], sum(ends)], axis=1
    )
    query = rotate(qproj.reshape(rows, heads_here, DK), positions).astype(jnp.bfloat16)
    key = (rotate(kproj.reshape(rows, heads_here, DK), positions) * DK ** (-0.5)).astype(
        jnp.bfloat16
    )
    value = vproj.astype(jnp.bfloat16).reshape(rows, heads_here, DV)
    normret = retain(query, key, value, head_rates, block_scale)
    gated = (normret * jax.nn.silu(gproj)).astype(jnp.bfloat16)
    opposite = tuple(hops[o] for o in order_of(size)[-1])
    gate_hops, gates = circulate(ff_gate, 0, ((), opposite, (projected,)))
    up_hops, ups = circulate(ff_up, 0, (last, (), (gated,)))
    mix = tp_scatter_sum(product_columns(gated, proj, place, core, slice(width, None)))
    resid = (tokens.astype(jnp.float32) + mix).astype(jnp.bfloat16)
    whole2 = tp_gather(resid, 1)
    normed2 = to_ring(
        rms_norm(whole2.astype(jnp.float32), gains[1]).astype(jnp.bfloat16), place, core
    )
    gate_part = product_rows(normed2[:1], gates[:1])
    up_part = product_rows(normed2[:1], ups[:1])
    early_parts = (gate_part, up_part)
    gate_part = product_rows(normed2[1:], gates[1:], result=gate_part)
    up_part = product_rows(normed2[1:], ups[1:], result=up_part)
    hidden = (jax.nn.silu(gate_part) * up_part).astype(jnp.bfloat16)
    near = (gate_hops[-reach], gate_hops[reach])
    far = order_of(size)[-1][-1]
    second = (normed2[0][0], up_hops[-reach], up_hops[reach])
    third = early_parts + (gate_hops[far], up_hops[far])
    _, downs = circulate(ff_down, 1, (near, second, third))
    ffn = tp_scatter_sum(product_columns(hidden, downs, place, core))
    total = resid.astype(jnp.float32) + ffn
    squares = tp_sum(jnp.sum(total * total, axis=-1))[:, None]
    scale = lax.rsqrt(squares / D + EPS)
    return (total * scale * final_gain.astype(jnp.float32)).astype(jnp.bfloat16)


MESH = pl.DeviceIdType.MESH
F32 = jnp.float32
BF16 = jnp.bfloat16
WIDE = 256


def silu(v):
    return v / (1.0 + jnp.exp(-v))


def mm(a, b):
    return jnp.dot(a, b, preferred_element_type=F32)


def layer_kernel(
    tok_h,
    gain_h,
    q_h,
    k_h,
    v_h,
    g_h,
    o_h,
    rate_s,
    scale_s,
    fg_h,
    fu_h,
    fd_h,
    cos_ref,
    sin_ref,
    out_ref,
    tok,
    gn,
    P,
    O,
    G,
    U,
    Dn,
    nrm,
    pr,
    gated,
    pm,
    rm,
    R,
    N2,
    hid,
    sx,
    rx,
    pmine,
    sz,
    rz,
    tot,
    ss_s,
    ss_r,
    lsem,
    ssem,
    wsem,
    asem,
):
    rows, feat = tok_h.shape
    width = 2 * feat
    rw = q_h.shape[0]
    cw = o_h.shape[1]
    half_ff = fg_h.shape[1] // 2
    heads = rate_s.shape[0]
    f = lax.axis_index("fs")
    x = lax.axis_index("tp")
    c = f % 2
    y = (f // 2) % 2
    z = f // 4
    b = z // 2
    zp = 4 * b + 1 - z
    zm = 3 - z
    near_o = 2 - b
    far_o = 3 * (1 - b)
    near = jnp.logical_or(z == 1, z == 2)
    y1, c1, x1 = 1 - y, 1 - c, 1 - x

    def dev(zz, yy, cc, xx):
        return ((zz * 2 + yy) * 2 + cc, xx)

    sends = []

    def put(src, dst, sem, to, cond=None):
        copy = pltpu.make_async_remote_copy(
            src_ref=src,
            dst_ref=dst,
            send_sem=ssem.at[len(sends)],
            recv_sem=sem,
            device_id=to,
            device_id_type=MESH,
        )
        if cond is None:
            copy.start()
        else:
            pl.when(cond)(copy.start)
        sends.append((cond, copy))

    def got(ref, sem, cond=None):
        copy = pltpu.make_async_remote_copy(
            src_ref=ref,
            dst_ref=ref,
            send_sem=ssem.at[0],
            recv_sem=sem,
            device_id=dev(z, y, c1, x),
            device_id_type=MESH,
        )
        if cond is None:
            copy.wait_recv()
        else:
            pl.when(cond)(copy.wait_recv)

    local = []

    def take(src, dst):
        copy = pltpu.make_async_copy(src, dst, lsem.at[len(local)])
        copy.start()
        local.append(copy)
        return copy

    def row_slot(buf):
        def slot(zz, yy, cc):
            start = pl.multiple_of(((zz * 2 + yy) * 2 + cc) * rw, rw)
            return buf.at[pl.ds(start, rw), :]

        return slot

    def col_slot(buf):
        def slot(zz, yy, cc):
            return buf.at[zz * 2 + yy, :, pl.ds(pl.multiple_of(cc * cw, cw), cw)]

        return slot

    sP, sO, sG, sU, sD = row_slot(P), col_slot(O), row_slot(G), row_slot(U), col_slot(Dn)
    slots = (sP, sO, sG, sU, sD)

    def sem_of(kind, zz, yy, cc):
        return wsem.at[kind, (zz * 2 + yy) * 2 + cc]

    def fwd(kind, zz, yy, cc, to, cond=None):
        ref = slots[kind](zz, yy, cc)
        put(ref, ref, sem_of(kind, zz, yy, cc), to, cond)

    def arrive(kind, zz, yy, cc, cond=None):
        got(slots[kind](zz, yy, cc), sem_of(kind, zz, yy, cc), cond)

    sib = dev(z, y, c1, x)
    row = dev(z, y1, c, x)
    peer = dev(zp, y, c, x)
    xdev = dev(z, y, c, x1)
    mirror = dev(zm, y, c, x)

    ends = np.cumsum([0, q_h.shape[1], k_h.shape[1], v_h.shape[1], g_h.shape[1]])
    mine = pl.multiple_of(((z * 2 + y) * 2 + c) * rw, rw)
    own_p = [
        take(ref, P.at[pl.ds(mine, rw), pl.ds(int(ends[i]), ref.shape[1])])
        for i, ref in enumerate((q_h, k_h, v_h, g_h))
    ]
    own_o = take(o_h, sO(z, y, c))
    own_t = [take(tok_h, tok.at[x]), take(gain_h, gn.at[x])]
    at_b = pl.multiple_of(b * half_ff, 128)
    at_o = pl.multiple_of((1 - b) * half_ff, 128)
    own_g = take(fg_h.at[:, pl.ds(at_b, half_ff)], sG(z, y, c))
    own_u = take(fu_h.at[:, pl.ds(at_b, half_ff)], sU(z, y, c))
    own_d = take(fd_h.at[pl.ds(at_b, half_ff), :], sD(z, y, c))

    barrier = pltpu.get_barrier_semaphore()
    friends = [sib, row, xdev] + [dev((z + k) % 4, y, c, x) for k in (1, 2, 3)]
    for to in friends:
        pl.semaphore_signal(barrier, inc=1, device_id=to, device_id_type=MESH)
    pl.semaphore_wait(barrier, len(friends))

    put(tok_h, tok.at[x], asem.at[0], xdev)
    put(gain_h, gn.at[x], asem.at[1], xdev)

    up_ok, down_ok = z < 3, z > 0
    above, below = dev((z + 1) % 4, y, c, x), dev((z + 3) % 4, y, c, x)

    for copy in own_p:
        copy.wait()
    own_o.wait()
    for kind in (0, 1):
        fwd(kind, z, y, c, row)
        fwd(kind, z, y, c, above, up_ok)
        fwd(kind, z, y, c, below, down_ok)
        fwd(kind, z, y, c, sib)

    def stage0(kind, own, other):
        own.wait()
        fwd(kind, z, y, c, row)
        fwd(kind, z, y, c, peer)
        put(other, slots[kind](z, y, c), sem_of(kind, z, y, c), dev(near_o, y, c, x))
        fwd(kind, z, y, c, sib)

    def stage1(kind):
        arrive(kind, zp, y, c)
        fwd(kind, zp, y, c, row)
        fwd(kind, zp, y, c, sib)

    def stage2(kind):
        for zz in (near_o, far_o):
            arrive(kind, zz, y, c)
            fwd(kind, zz, y, c, peer, near)
            fwd(kind, zz, y, c, row)
            fwd(kind, zz, y, c, sib)

    def stage4(kind):
        for zz in (z, zp, near_o, far_o):
            arrive(kind, zz, y1, c)
            fwd(kind, zz, y1, c, sib)

    def line(d):
        for step in (-d, d):
            src = (z + step + 4) % 4
            ok = z + step >= 0 if step < 0 else z + step <= 3
            on, more = (above, up_ok) if step < 0 else (below, down_ok)
            for kind in (0, 1):
                arrive(kind, src, y, c, ok)
                fwd(kind, src, y, c, row, ok)
                fwd(kind, src, y, c, on, jnp.logical_and(ok, more))
                fwd(kind, src, y, c, sib, ok)

    def across(d):
        for step in (-d, d) if d else (0,):
            src = (z + step + 4) % 4
            ok = None
            if d:
                ok = z + step >= 0 if step < 0 else z + step <= 3
            for kind in (0, 1):
                arrive(kind, src, y1, c, ok)
                fwd(kind, src, y1, c, sib, ok)

    stage0(2, own_g, fg_h.at[:, pl.ds(at_o, half_ff)])

    for copy in own_t:
        copy.wait()
    got(tok.at[x1], asem.at[0])
    got(gn.at[x1], asem.at[1])

    def norm_rows(first, second, gain_row, dst, base):
        chunk = 32

        @pl.loop(0, rows // chunk)
        def _(i):
            at = pl.ds(pl.multiple_of(i * chunk, chunk), chunk)
            one = first[at, :].astype(F32)
            two = second[at, :].astype(F32)
            total = jnp.sum(one * one, axis=1, keepdims=True) + jnp.sum(two * two, axis=1, keepdims=True)
            scale = lax.rsqrt(total / width + EPS)
            to = pl.ds(pl.multiple_of(base + i * chunk, chunk), chunk)
            dst[to, 0:feat] = (one * scale * gn[0, gain_row : gain_row + 1, :]).astype(BF16)
            dst[to, feat:width] = (two * scale * gn[1, gain_row : gain_row + 1, :]).astype(BF16)

    norm_rows(tok.at[0], tok.at[1], 0, nrm, 0)

    line(1)
    stage0(3, own_u, fu_h.at[:, pl.ds(at_o, half_ff)])
    line(2)
    stage1(2)
    line(3)
    for d in range(4):
        across(d)
    stage2(2)
    stage0(4, own_d, fd_h.at[pl.ds(at_o, half_ff), :])
    for zz in range(4):
        for yy in range(2):
            arrive(0, zz, yy, c1)
            arrive(1, zz, yy, c1)

    @pl.loop(0, P.shape[1] // WIDE)
    def _(j):
        at = pl.ds(pl.multiple_of(j * WIDE, WIDE), WIDE)
        pr[:, at] = mm(nrm[...], P[:, at])

    blk = rows // 2
    t = lax.broadcasted_iota(jnp.int32, (rows, rows), 0)
    s = lax.broadcasted_iota(jnp.int32, (rows, rows), 1)
    late_t, late_s = t >= blk, s >= blk
    apart = (t - s).astype(F32)
    into = (t - (blk - 1)).astype(F32)
    left = ((blk - 1) - s).astype(F32)
    causal = t >= s
    lane = lax.broadcasted_iota(jnp.int32, (rows, 2 * DK), 1)
    early = (lane % DK) < DK // 2
    first_head = lane < DK

    def turn(v):
        swapped = jnp.where(early, pltpu.roll(v, 2 * DK - DK // 2, 1), pltpu.roll(v, DK // 2, 1))
        return v * cos_ref[...] + swapped * sin_ref[...]

    for pair in range(heads // 2):
        cols = slice(pair * 2 * DK, (pair + 1) * 2 * DK)
        query = turn(pr[:, cols]).astype(BF16)
        kcols = slice(int(ends[1]) + pair * 2 * DK, int(ends[1]) + (pair + 1) * 2 * DK)
        key = (turn(pr[:, kcols]) * DK ** (-0.5)).astype(BF16)
        for side in range(2):
            h = 2 * pair + side
            keep = first_head if side == 0 else jnp.logical_not(first_head)
            part = jnp.where(keep, query, jnp.zeros_like(query))
            scores = lax.dot_general(part, key, (((1,), (1,)), ((), ())), preferred_element_type=F32)
            la0 = -(rate_s[h] * scale_s[0])
            la1 = -(rate_s[h] * scale_s[1])
            power = jnp.where(late_t, la1, la0) * apart
            power = jnp.where(jnp.logical_and(late_t, jnp.logical_not(late_s)), la1 * into + la0 * left, power)
            scores = scores * jnp.where(causal, jnp.exp(jnp.where(causal, power, 0.0)), 0.0)
            high = scores.astype(BF16)
            low = (scores - high.astype(F32)).astype(BF16)
            vcols = slice(int(ends[2]) + h * DV, int(ends[2]) + (h + 1) * DV)
            value = pr[:, vcols].astype(BF16)
            ret = mm(high, value) + mm(low, value)
            ret = ret * lax.rsqrt(jnp.mean(ret * ret, axis=1, keepdims=True) + EPS)
            gcols = slice(int(ends[3]) + h * DV, int(ends[3]) + (h + 1) * DV)
            gated[:, h * DV : (h + 1) * DV] = (ret * silu(pr[:, gcols])).astype(BF16)

    per = feat // WIDE
    for side in (x1, x):
        for j in range(per):
            pm[side, :, j * WIDE : (j + 1) * WIDE] = mm(gated[...], O[side * per + j]).astype(BF16)
        if side is x1:
            put(pm.at[x1], rm, asem.at[2], xdev)

    stage1(3)
    stage2(3)

    got(rm, asem.at[2])

    @pl.loop(0, rows // 32)
    def _(i):
        at = pl.ds(pl.multiple_of(i * 32, 32), 32)
        mix = pm[x, at, :].astype(F32) + rm[at, :].astype(F32)
        R[0, x, at, :] = (tok[x, at, :].astype(F32) + mix).astype(BF16)

    put(R.at[0, x], R.at[0, x], asem.at[3], xdev)
    put(R.at[0, x], R.at[1, x], asem.at[4], mirror)
    stage4(2)
    stage1(4)
    got(R.at[1, x], asem.at[4])
    put(R.at[1, x], R.at[1, x], asem.at[5], xdev)
    got(R.at[0, x1], asem.at[3])
    norm_rows(R.at[0, 0], R.at[0, 1], 1, N2, 0)
    stage2(4)
    got(R.at[1, x1], asem.at[5])
    norm_rows(R.at[1, 0], R.at[1, 1], 1, N2, rows)
    stage4(3)
    for kind in (2, 3):
        for zz in range(4):
            for yy in range(2):
                arrive(kind, zz, yy, c1)

    def hidden(at):
        gate = mm(N2[...], G[:, at])
        up = mm(N2[...], U[:, at])
        hid[:, at] = (silu(gate) * up).astype(BF16)

    whole = half_ff // WIDE

    @pl.loop(0, whole)
    def _(j):
        hidden(pl.ds(pl.multiple_of(j * WIDE, WIDE), WIDE))

    if half_ff % WIDE:
        hidden(pl.ds(whole * WIDE, half_ff % WIDE))

    order = [(y, 0), (y, 1), (y1, 0), (y1, 1)]

    def chip(half, i):
        yy, far = order[i]
        return (3 * half if far else 1 + half), yy

    def columns(i):
        zz, yy = chip(x, i)
        return pl.ds(pl.multiple_of(((zz - 2 * x) * 2 + yy) * WIDE, WIDE), WIDE)

    def produce(i):
        zt, yt = chip(x1, i)
        zk, yk = chip(x, i)
        arrive(4, zt, yt, c1)
        sx[i] = mm(hid[...], Dn[zt * 2 + yt]).astype(BF16)
        put(sx.at[i], rx.at[i], asem.at[6 + i], xdev)
        arrive(4, zk, yk, c1)
        pmine[i] = mm(hid[...], Dn[zk * 2 + yk])

    def combine(i):
        got(rx.at[i], asem.at[6 + i])
        sz[i] = (pmine[i, rows : 2 * rows, :] + rx[i, rows : 2 * rows, :].astype(F32)).astype(BF16)
        put(sz.at[i], rz.at[i], asem.at[10 + i], mirror)
        resid = R[0, x, :, columns(i)].astype(F32)
        tot[i] = resid + (pmine[i, 0:rows, :] + rx[i, 0:rows, :].astype(F32))

    def close(i):
        got(rz.at[i], asem.at[10 + i])
        now = tot[i] + rz[i].astype(F32)
        tot[i] = now
        square = now * now
        square = square[:, : WIDE // 2] + square[:, WIDE // 2 :]
        ss_s[...] = square if i == 0 else ss_s[...] + square

    produce(0)
    produce(1)
    combine(0)
    stage4(4)
    produce(2)
    combine(1)
    close(0)
    produce(3)
    combine(2)
    close(1)
    combine(3)
    close(2)
    close(3)

    put(ss_s, ss_r, asem.at[14], xdev)
    got(ss_r, asem.at[14])
    total = jnp.sum(ss_s[...] + ss_r[...], axis=1, keepdims=True)
    scale = lax.rsqrt(total / width + EPS)
    for i in range(4):
        out_ref[:, columns(i)] = (tot[i] * scale * gn[x, 2:3, columns(i)]).astype(out_ref.dtype)

    for cond, copy in sends:
        if cond is None:
            copy.wait_send()
        else:
            pl.when(cond)(copy.wait_send)


def tables(rows):
    half = DK // 2
    inverse = np.float32(THETA) ** (-np.arange(half, dtype=np.float32) / np.float32(half))
    angle = (np.arange(rows, dtype=np.float32) % SEQ_LEN)[:, None] * inverse
    cosine, sine = np.cos(angle), np.sin(angle)
    return (
        np.concatenate([cosine] * 4, axis=1).astype(np.float32),
        np.concatenate([-sine, sine, -sine, sine], axis=1).astype(np.float32),
    )


def fused(
    tokens,
    mix_gain,
    query_weight,
    key_weight,
    value_weight,
    output_gate_weight,
    out_weight,
    head_rates,
    block_scale,
    ffn_gain,
    ff_gate,
    ff_up,
    ff_down,
    final_gain,
):
    rows, feat = tokens.shape
    size = lax.axis_size("fs")
    chips = size // 2
    width = 2 * feat
    half_ff = ff_gate.shape[1] // 2
    joint = sum(w.shape[1] for w in (query_weight, key_weight, value_weight, output_gate_weight))
    heads = head_rates.shape[0]
    gains = jnp.stack([mix_gain, ffn_gain, final_gain] + [final_gain] * 5).astype(F32)
    cosine, sine = tables(rows)
    cw = out_weight.shape[1]
    hbm = pl.BlockSpec(memory_space=pl.ANY)
    smem = pl.BlockSpec(memory_space=pltpu.SMEM)
    vmem = pl.BlockSpec(memory_space=pltpu.VMEM)
    dma = pltpu.SemaphoreType.DMA
    return pl.pallas_call(
        layer_kernel,
        out_shape=jax.ShapeDtypeStruct((rows, feat), BF16),
        in_specs=[hbm] * 7 + [smem] * 2 + [hbm] * 3 + [vmem] * 2,
        out_specs=vmem,
        scratch_shapes=[
            pltpu.VMEM((2, rows, feat), BF16),
            pltpu.VMEM((2, 8, feat), F32),
            pltpu.VMEM((width, joint), BF16),
            pltpu.VMEM((chips, out_weight.shape[0], 2 * cw), BF16),
            pltpu.VMEM((width, half_ff), BF16),
            pltpu.VMEM((width, half_ff), BF16),
            pltpu.VMEM((chips, half_ff, 2 * cw), BF16),
            pltpu.VMEM((rows, width), BF16),
            pltpu.VMEM((rows, joint), F32),
            pltpu.VMEM((rows, heads * DV), BF16),
            pltpu.VMEM((2, rows, feat), BF16),
            pltpu.VMEM((rows, feat), BF16),
            pltpu.VMEM((2, 2, rows, feat), BF16),
            pltpu.VMEM((2 * rows, width), BF16),
            pltpu.VMEM((2 * rows, half_ff), BF16),
            pltpu.VMEM((4, 2 * rows, WIDE), BF16),
            pltpu.VMEM((4, 2 * rows, WIDE), BF16),
            pltpu.VMEM((4, 2 * rows, WIDE), F32),
            pltpu.VMEM((4, rows, WIDE), BF16),
            pltpu.VMEM((4, rows, WIDE), BF16),
            pltpu.VMEM((4, rows, WIDE), F32),
            pltpu.VMEM((rows, WIDE // 2), F32),
            pltpu.VMEM((rows, WIDE // 2), F32),
            dma((12,)),
            dma((160,)),
            dma((5, size)),
            dma((16,)),
        ],
        compiler_params=pltpu.CompilerParams(
            collective_id=0, has_side_effects=True, vmem_limit_bytes=60 * 2**20
        ),
    )(
        tokens,
        gains,
        query_weight,
        key_weight,
        value_weight,
        output_gate_weight,
        out_weight,
        head_rates,
        block_scale,
        ff_gate,
        ff_up,
        ff_down,
        cosine,
        sine,
    )


def kernel_fits(mesh, tokens, query_weight, ff_gate, head_rates):
    size, parts = mesh.shape["fs"], mesh.shape["tp"]
    if size != 4 * 2 * 2 or parts != 2:
        return False
    rows, width = tokens.shape[0] // size, tokens.shape[1]
    return (
        rows == SEQ_LEN
        and SEQ_LEN == 2 * BLK
        and width // size * 2 == WIDE
        and ff_gate.shape[1] % (4 * 128) == 0
        and head_rates.shape[0] % (2 * parts) == 0
    )


def dispatch(mesh, *args):
    fits = kernel_fits(mesh, args[0], args[2], args[10], args[7])
    return jax.shard_map(
        fused if fits else body,
        mesh=mesh,
        in_specs=SPECS,
        out_specs=P("fs", "tp"),
        check_vma=False,
    )(*args)


SPECS = (
    P("fs", "tp"),
    P("tp"),
    P("fs", "tp"),
    P("fs", "tp"),
    P("fs", "tp"),
    P("fs", "tp"),
    P("tp", "fs"),
    P("tp"),
    P("fs"),
    P("tp"),
    P("fs", "tp"),
    P("fs", "tp"),
    P("tp", "fs"),
    P("tp"),
)


def solution(mesh):
    return functools.partial(dispatch, mesh)
```

```python
import functools

import jax
import jax.numpy as jnp
import numpy as np
from jax import lax
from jax.experimental import pallas as pl
from jax.experimental.pallas import tpu as pltpu
from jax.sharding import PartitionSpec as P

D = 2048
DK = 64
DV = 128
BLK = 128
SEQ_LEN = 256


EPS = 1e-06
THETA = 10000.0


def rms_norm(values, gain):
    scale = lax.rsqrt(jnp.mean(values * values, axis=-1, keepdims=True) + EPS)
    return values * scale * gain.astype(jnp.float32)


def rotate(values, positions):
    half = values.shape[-1] // 2
    inverse = THETA ** (-jnp.arange(half, dtype=jnp.float32) / half)
    angle = positions.astype(jnp.float32)[:, None] * inverse
    cosine = jnp.cos(angle)[:, None, :]
    sine = jnp.sin(angle)[:, None, :]
    first = values[..., :half]
    second = values[..., half:]
    return jnp.concatenate(
        [first * cosine - second * sine, second * cosine + first * sine], axis=-1
    )


def retain(query, key, value, rates, scales):
    rows, heads_here, width_k = query.shape
    width_v = value.shape[-1]
    nblk = rows // BLK
    hi = lax.Precision.HIGHEST
    qblk = query.astype(jnp.float32).reshape(nblk, BLK, heads_here, width_k)
    kblk = key.astype(jnp.float32).reshape(nblk, BLK, heads_here, width_k)
    vblk = value.astype(jnp.float32).reshape(nblk, BLK, heads_here, width_v)
    logdec = -rates[None, :] * scales[:, None]
    steps = jnp.arange(BLK, dtype=jnp.float32)
    offset = steps[:, None] - steps[None, :]
    causal = offset >= 0
    inside = jnp.where(
        causal[None, None],
        jnp.exp(logdec[:, :, None, None] * jnp.where(causal, offset, 0.0)[None, None]),
        0.0,
    )
    scores = jnp.einsum("nchd,nmhd->nhcm", qblk, kblk, precision=hi) * inside
    inner = jnp.einsum("nhcm,nmhe->nche", scores, vblk, precision=hi)
    zeta = jnp.exp(logdec[:, :, None] * (BLK - 1.0 - steps)[None, None, :])
    kv_block = jnp.einsum(
        "nchd,nche->nhde", kblk * jnp.transpose(zeta, (0, 2, 1))[..., None], vblk, precision=hi
    )
    hold = jnp.exp(logdec * BLK)
    per_seq = SEQ_LEN // BLK
    fresh = (jnp.arange(nblk, dtype=jnp.int32) % per_seq == 0).astype(jnp.float32)

    def advance(state, inputs):
        kv_now, hold_now, fresh_now = inputs
        before = state * (1.0 - fresh_now)
        return (before * hold_now[:, None, None] + kv_now, before)

    start = jnp.zeros((heads_here, width_k, width_v), jnp.float32)
    _, before = lax.scan(advance, start, (kv_block, hold, fresh), unroll=True)
    xi = jnp.exp(logdec[:, :, None] * (steps + 1.0)[None, None, :])
    cross = jnp.einsum(
        "nchd,nhde->nche", qblk * jnp.transpose(xi, (0, 2, 1))[..., None], before, precision=hi
    )
    total = inner + cross
    total = total * lax.rsqrt(jnp.mean(total * total, axis=-1, keepdims=True) + EPS)
    return total.reshape(rows, heads_here * width_v)


def chip_ring(size):
    chips = size // 2
    return list(range(0, chips, 2)) + list(range(1, chips, 2))[::-1]


def ring_place(size):
    ring = chip_ring(size)
    me = lax.axis_index("fs")
    chip = me // 2
    place = jnp.zeros((), jnp.int32)
    for index, member in enumerate(ring):
        place = jnp.where(chip == member, index, place)
    return place, me % 2


def after(value, *others):
    return lax.optimization_barrier((value,) + tuple(others))[0]


def circulate(block, axis, gates=()):
    size = lax.axis_size("fs")
    ring = chip_ring(size)
    chips = len(ring)
    onward = [
        (2 * ring[i] + core, 2 * ring[(i + 1) % chips] + core)
        for i in range(chips)
        for core in range(2)
    ]
    back = [(target, source) for source, target in onward]
    swap = [(i, i ^ 1) for i in range(size)]
    held = {0: block}
    reach = (chips - 1) // 2
    down = up = block
    for step in range(1, reach + 1):
        if len(gates) >= step and gates[step - 1]:
            down = after(down, *gates[step - 1])
            up = after(up, *gates[step - 1])
        down = lax.ppermute(down, "fs", onward)
        up = lax.ppermute(up, "fs", back)
        held[-step] = down
        held[step] = up
    if chips % 2 == 0 and chips > 1:
        cut = 1 - axis
        half = block.shape[cut] // 2
        if len(gates) > reach and gates[reach]:
            down = after(down, *gates[reach])
            up = after(up, *gates[reach])
        first = lax.ppermute(lax.slice_in_dim(down, 0, half, axis=cut), "fs", onward)
        second = lax.ppermute(lax.slice_in_dim(up, half, None, axis=cut), "fs", back)
        held[reach + 1] = jnp.concatenate([first, second], axis=cut)
    groups = []
    for offsets in order_of(size):
        own = jnp.concatenate([held[o] for o in offsets], axis=axis)
        groups.append((own, lax.ppermute(own, "fs", swap)))
    return held, groups


def order_of(size):
    chips = size // 2
    reach = (chips - 1) // 2
    groups = [list(range(-reach, reach + 1))]
    if chips > 1 and chips % 2 == 0:
        groups.append([reach + 1])
    return groups


def lane_of(values, lane, wide):
    count = values.shape[1] // (2 * wide)
    return [values[:, (2 * c + lane) * wide : (2 * c + lane + 1) * wide] for c in range(count)]


def to_ring(values, place, core):
    size = lax.axis_size("fs")
    wide = values.shape[1] // size
    ring = chip_ring(size)
    chips = len(ring)
    groups = order_of(size)
    start = (place + groups[0][0] + chips) % chips
    lanes = []
    for lane in range(2):
        pieces = lane_of(values, lane, wide)
        ringed = jnp.concatenate([pieces[c] for c in ring] * 2, axis=1)
        lanes.append(lax.dynamic_slice_in_dim(ringed, start * wide, chips * wide, axis=1))
    own = jnp.where(core == 0, lanes[0], lanes[1])
    other = jnp.where(core == 0, lanes[1], lanes[0])
    result, edge = [], 0
    for offsets in groups:
        end = edge + len(offsets) * wide
        result.append((own[:, edge:end], other[:, edge:end]))
        edge = end
    return result


def from_ring(groups, place, core):
    size = lax.axis_size("fs")
    ring = chip_ring(size)
    chips = len(ring)
    own = jnp.concatenate([own for own, _ in groups], axis=1)
    other = jnp.concatenate([other for _, other in groups], axis=1)
    wide = own.shape[1] // chips
    start = (2 * chips - place - order_of(size)[0][0]) % chips
    lanes = []
    for lane in range(2):
        straight = jnp.where(core == lane, own, other)
        doubled = jnp.concatenate([straight, straight], axis=1)
        lanes.append(lax.dynamic_slice_in_dim(doubled, start * wide, chips * wide, axis=1))
    spot = {c: i for i, c in enumerate(ring)}
    return jnp.concatenate(
        [
            lanes[lane][:, spot[c] * wide : (spot[c] + 1) * wide]
            for c in range(chips)
            for lane in range(2)
        ],
        axis=1,
    )


def tp_gather(values, axis):
    if lax.axis_size("tp") != 2:
        return lax.all_gather(values, "tp", axis=axis, tiled=True)
    other = lax.ppermute(values, "tp", [(0, 1), (1, 0)])
    mine = lax.axis_index("tp") == 0
    return jnp.concatenate(
        [jnp.where(mine, values, other), jnp.where(mine, other, values)], axis=axis
    )


def tp_sum(values):
    if lax.axis_size("tp") != 2:
        return lax.psum(values, "tp")
    return values + lax.ppermute(values, "tp", [(0, 1), (1, 0)])


def tp_scatter_sum(partial):
    if lax.axis_size("tp") != 2:
        pieces = lax.all_to_all(
            partial.reshape(partial.shape[0], lax.axis_size("tp"), -1), "tp", 1, 1
        )
        return jnp.sum(pieces.astype(jnp.float32), axis=1)
    half = partial.shape[1] // 2
    low = lax.axis_index("tp") == 0
    keep = jnp.where(low, partial[:, :half], partial[:, half:])
    send = jnp.where(low, partial[:, half:], partial[:, :half])
    got = lax.ppermute(send, "tp", [(0, 1), (1, 0)])
    return keep.astype(jnp.float32) + got.astype(jnp.float32)


def product_rows(left, groups, columns=slice(None), result=0.0):
    for pieces, blocks in zip(left, groups):
        for piece, block in zip(pieces, blocks):
            result = result + jnp.dot(
                piece, block[:, columns], preferred_element_type=jnp.float32
            )
    return result


def product_columns(left, groups, place, core, columns=None):
    terms = []
    for blocks in groups:
        pair = []
        for block in blocks:
            if columns is None:
                dims, right = (((1,), (0,)), ((), ())), block
            else:
                dims, right = (((1,), (1,)), ((), ())), block[:, columns]
            term = lax.dot_general(left, right, dims, preferred_element_type=jnp.float32)
            pair.append(term.astype(jnp.bfloat16))
        terms.append(pair)
    return from_ring(terms, place, core)


def body(
    tokens,
    mix_gain,
    query_weight,
    key_weight,
    value_weight,
    output_gate_weight,
    out_weight,
    head_rates,
    block_scale,
    ffn_gain,
    ff_gate,
    ff_up,
    ff_down,
    final_gain,
):
    rows = tokens.shape[0]
    heads_here = head_rates.shape[0]
    size = lax.axis_size("fs")
    place, core = ring_place(size)
    reach = (size // 2 - 1) // 2
    positions = jnp.arange(rows, dtype=jnp.int32) % SEQ_LEN

    bundle = jnp.concatenate(
        [query_weight, key_weight, value_weight, output_gate_weight, out_weight.T], axis=1
    )
    hops, proj = circulate(bundle, 0)
    last = (hops[-reach], hops[reach])

    whole = tp_gather(tokens, 1)
    gains = tp_gather(jnp.stack([mix_gain, ffn_gain]), 1)
    normed = rms_norm(whole.astype(jnp.float32), gains[0]).astype(jnp.bfloat16)
    width = bundle.shape[1] - out_weight.shape[0]
    projected = product_rows(to_ring(normed, place, core), proj, slice(0, width))
    ends = [query_weight.shape[1], key_weight.shape[1], value_weight.shape[1]]
    qproj, kproj, vproj, gproj = jnp.split(
        projected, [ends[0], ends[0] + ends[1], sum(ends)], axis=1
    )
    query = rotate(qproj.reshape(rows, heads_here, DK), positions).astype(jnp.bfloat16)
    key = (rotate(kproj.reshape(rows, heads_here, DK), positions) * DK ** (-0.5)).astype(
        jnp.bfloat16
    )
    value = vproj.astype(jnp.bfloat16).reshape(rows, heads_here, DV)
    normret = retain(query, key, value, head_rates, block_scale)
    gated = (normret * jax.nn.silu(gproj)).astype(jnp.bfloat16)
    opposite = tuple(hops[o] for o in order_of(size)[-1])
    gate_hops, gates = circulate(ff_gate, 0, ((), opposite, (projected,)))
    up_hops, ups = circulate(ff_up, 0, (last, (), (gated,)))
    mix = tp_scatter_sum(product_columns(gated, proj, place, core, slice(width, None)))
    resid = (tokens.astype(jnp.float32) + mix).astype(jnp.bfloat16)
    whole2 = tp_gather(resid, 1)
    normed2 = to_ring(
        rms_norm(whole2.astype(jnp.float32), gains[1]).astype(jnp.bfloat16), place, core
    )
    gate_part = product_rows(normed2[:1], gates[:1])
    up_part = product_rows(normed2[:1], ups[:1])
    early_parts = (gate_part, up_part)
    gate_part = product_rows(normed2[1:], gates[1:], result=gate_part)
    up_part = product_rows(normed2[1:], ups[1:], result=up_part)
    hidden = (jax.nn.silu(gate_part) * up_part).astype(jnp.bfloat16)
    near = (gate_hops[-reach], gate_hops[reach])
    far = order_of(size)[-1][-1]
    second = (normed2[0][0], up_hops[-reach], up_hops[reach])
    third = early_parts + (gate_hops[far], up_hops[far])
    _, downs = circulate(ff_down, 1, (near, second, third))
    ffn = tp_scatter_sum(product_columns(hidden, downs, place, core))
    total = resid.astype(jnp.float32) + ffn
    squares = tp_sum(jnp.sum(total * total, axis=-1))[:, None]
    scale = lax.rsqrt(squares / D + EPS)
    return (total * scale * final_gain.astype(jnp.float32)).astype(jnp.bfloat16)


MESH = pl.DeviceIdType.MESH
F32 = jnp.float32
BF16 = jnp.bfloat16
WIDE = 256


def silu(v):
    return v / (1.0 + jnp.exp(-v))


def mm(a, b):
    return jnp.dot(a, b, preferred_element_type=F32)


def layer_kernel(
    tok_h,
    gain_h,
    q_h,
    k_h,
    v_h,
    g_h,
    o_h,
    rate_s,
    scale_s,
    fg_h,
    fu_h,
    fd_h,
    cos_ref,
    sin_ref,
    out_ref,
    tok,
    gn,
    P,
    O,
    G,
    U,
    Dn,
    nrm,
    pr,
    gated,
    pm,
    rm,
    R,
    N2,
    hid,
    sx,
    rx,
    pmine,
    sz,
    rz,
    tot,
    ss_s,
    ss_r,
    lsem,
    ssem,
    wsem,
    asem,
):
    rows, feat = tok_h.shape
    width = 2 * feat
    rw = q_h.shape[0]
    cw = o_h.shape[1]
    half_ff = fg_h.shape[1] // 2
    heads = rate_s.shape[0]
    f = lax.axis_index("fs")
    x = lax.axis_index("tp")
    c = f % 2
    y = (f // 2) % 2
    z = f // 4
    b = z // 2
    zp = 4 * b + 1 - z
    zm = 3 - z
    near_o = 2 - b
    far_o = 3 * (1 - b)
    near = jnp.logical_or(z == 1, z == 2)
    far = jnp.logical_not(near)
    y1, c1, x1 = 1 - y, 1 - c, 1 - x

    def dev(zz, yy, cc, xx):
        return ((zz * 2 + yy) * 2 + cc, xx)

    sends = []
    role = [None]

    def put(src, dst, sem, to):
        index = len(sends)

        def copy():
            return pltpu.make_async_remote_copy(
                src_ref=src(),
                dst_ref=dst(),
                send_sem=ssem.at[index],
                recv_sem=sem(),
                device_id=to,
                device_id_type=MESH,
            )

        copy().start()
        sends.append((role[0], copy))

    def only(who, *acts):
        @pl.when(who)
        def _():
            role[0] = who
            for act, *args in acts:
                act(*args)
            role[0] = None

    def got(ref, sem, name="got"):
        copy = pltpu.make_async_remote_copy(
            src_ref=ref,
            dst_ref=ref,
            send_sem=ssem.at[0],
            recv_sem=sem,
            device_id=dev(z, y, c1, x),
            device_id_type=MESH,
        )
        with jax.named_scope(name):
            copy.wait_recv()

    local = []

    def take(src, dst):
        copy = pltpu.make_async_copy(src, dst, lsem.at[len(local)])
        copy.start()
        local.append(copy)
        return copy

    def row_slot(buf):
        def slot(zz, yy, cc):
            start = pl.multiple_of(((zz * 2 + yy) * 2 + cc) * rw, rw)
            return buf.at[pl.ds(start, rw), :]

        return slot

    def col_slot(buf):
        def slot(zz, yy, cc):
            return buf.at[zz * 2 + yy, :, pl.ds(pl.multiple_of(cc * cw, cw), cw)]

        return slot

    sP, sO, sG, sU, sD = row_slot(P), col_slot(O), row_slot(G), row_slot(U), col_slot(Dn)
    slots = (sP, sO, sG, sU, sD)

    def sem_of(kind, zz, yy, cc):
        return wsem.at[kind, (zz * 2 + yy) * 2 + cc]

    def fwd(kind, zz, yy, cc, to):
        ref = functools.partial(slots[kind], zz, yy, cc)
        put(ref, ref, functools.partial(sem_of, kind, zz, yy, cc), to)

    def arrive(kind, zz, yy, cc):
        side = "sib" if cc is c1 else "row" if yy is y1 else "col"
        got(slots[kind](zz, yy, cc), sem_of(kind, zz, yy, cc), f"{side}{kind}")

    sib = dev(z, y, c1, x)
    row = dev(z, y1, c, x)
    peer = dev(zp, y, c, x)
    xdev = dev(z, y, c, x1)
    mirror = dev(zm, y, c, x)

    ends = np.cumsum([0, q_h.shape[1], k_h.shape[1], v_h.shape[1], g_h.shape[1]])
    mine = pl.multiple_of(((z * 2 + y) * 2 + c) * rw, rw)
    own_p = [
        take(ref, P.at[pl.ds(mine, rw), pl.ds(int(ends[i]), ref.shape[1])])
        for i, ref in enumerate((q_h, k_h, v_h, g_h))
    ]
    own_o = take(o_h, sO(z, y, c))
    own_t = [take(tok_h, tok.at[x]), take(gain_h, gn.at[x])]
    at_b = pl.multiple_of(b * half_ff, 128)
    at_o = pl.multiple_of((1 - b) * half_ff, 128)
    own_g = take(fg_h.at[:, pl.ds(at_b, half_ff)], sG(z, y, c))
    own_u = take(fu_h.at[:, pl.ds(at_b, half_ff)], sU(z, y, c))
    own_d = take(fd_h.at[pl.ds(at_b, half_ff), :], sD(z, y, c))

    barrier = pltpu.get_barrier_semaphore()
    friends = [sib, row, xdev] + [dev((z + k) % 4, y, c, x) for k in (1, 2, 3)]
    for to in friends:
        pl.semaphore_signal(barrier, inc=1, device_id=to, device_id_type=MESH)
    pl.semaphore_wait(barrier, len(friends))

    put(lambda: tok_h, lambda: tok.at[x], lambda: asem.at[0], xdev)
    put(lambda: gain_h, lambda: gn.at[x], lambda: asem.at[1], xdev)

    other = {
        2: lambda: fg_h.at[:, pl.ds(at_o, half_ff)],
        3: lambda: fu_h.at[:, pl.ds(at_o, half_ff)],
        4: lambda: fd_h.at[pl.ds(at_o, half_ff), :],
    }
    beyond = dev(near_o, y, c, x)

    def own(kind, to):
        fwd(kind, z, y, c, to)

    def cross(kind):
        slot = functools.partial(slots[kind], z, y, c)
        put(other[kind], slot, functools.partial(sem_of, kind, z, y, c), beyond)

    def relay(kind, zz, *to):
        arrive(kind, zz, y, c)
        for device in to + (row, sib):
            fwd(kind, zz, y, c, device)

    def share(kind):
        for zz in (z, zp, near_o, far_o):
            arrive(kind, zz, y1, c)
            fwd(kind, zz, y1, c, sib)

    for copy in own_p:
        copy.wait()
    own_o.wait()
    own(0, row)
    own(0, peer)
    own(1, row)
    own(1, peer)
    only(near, (own, 0, beyond), (own, 1, beyond))
    own(0, sib)
    own(1, sib)
    own_g.wait()
    own(2, row)
    own(2, sib)
    only(far, (own, 2, peer), (relay, 0, zp), (relay, 1, zp))
    only(
        near,
        (relay, 0, zp, beyond),
        (relay, 0, near_o, peer),
        (relay, 1, zp, beyond),
        (relay, 1, near_o, peer),
    )

    for copy in own_t:
        copy.wait()
    got(tok.at[x1], asem.at[0])
    got(gn.at[x1], asem.at[1])

    def norm_rows(first, second, gain_row, dst, base):
        chunk = 32

        @pl.loop(0, rows // chunk)
        def _(i):
            at = pl.ds(pl.multiple_of(i * chunk, chunk), chunk)
            one = first[at, :].astype(F32)
            two = second[at, :].astype(F32)
            total = jnp.sum(one * one, axis=1, keepdims=True) + jnp.sum(two * two, axis=1, keepdims=True)
            scale = lax.rsqrt(total / width + EPS)
            to = pl.ds(pl.multiple_of(base + i * chunk, chunk), chunk)
            dst[to, 0:feat] = (one * scale * gn[0, gain_row : gain_row + 1, :]).astype(BF16)
            dst[to, feat:width] = (two * scale * gn[1, gain_row : gain_row + 1, :]).astype(BF16)

    norm_rows(tok.at[0], tok.at[1], 0, nrm, 0)

    own_u.wait()
    own_d.wait()
    only(
        far,
        (relay, 0, near_o),
        (relay, 1, near_o),
        (cross, 2),
        (relay, 0, far_o),
        (relay, 1, far_o),
        (own, 3, peer),
        (cross, 3),
        (relay, 2, zp),
        (relay, 2, near_o),
    )
    only(
        near,
        (relay, 0, far_o, peer),
        (relay, 1, far_o, peer),
        (own, 2, peer),
        (cross, 2),
        (relay, 2, zp),
        (relay, 2, near_o, peer),
        (relay, 2, far_o, peer),
        (own, 3, peer),
        (cross, 3),
    )
    share(0)
    share(1)
    for zz in range(4):
        for yy in range(2):
            arrive(0, zz, yy, c1)
            arrive(1, zz, yy, c1)

    @pl.loop(0, P.shape[1] // WIDE)
    def _(j):
        at = pl.ds(pl.multiple_of(j * WIDE, WIDE), WIDE)
        pr[:, at] = mm(nrm[...], P[:, at])

    blk = rows // 2
    t = lax.broadcasted_iota(jnp.int32, (rows, rows), 0)
    s = lax.broadcasted_iota(jnp.int32, (rows, rows), 1)
    late_t, late_s = t >= blk, s >= blk
    apart = (t - s).astype(F32)
    into = (t - (blk - 1)).astype(F32)
    left = ((blk - 1) - s).astype(F32)
    causal = t >= s
    lane = lax.broadcasted_iota(jnp.int32, (rows, 2 * DK), 1)
    early = (lane % DK) < DK // 2
    first_head = lane < DK

    def turn(v):
        swapped = jnp.where(early, pltpu.roll(v, 2 * DK - DK // 2, 1), pltpu.roll(v, DK // 2, 1))
        return v * cos_ref[...] + swapped * sin_ref[...]

    for pair in range(heads // 2):
        cols = slice(pair * 2 * DK, (pair + 1) * 2 * DK)
        query = turn(pr[:, cols]).astype(BF16)
        kcols = slice(int(ends[1]) + pair * 2 * DK, int(ends[1]) + (pair + 1) * 2 * DK)
        key = (turn(pr[:, kcols]) * DK ** (-0.5)).astype(BF16)
        for side in range(2):
            h = 2 * pair + side
            keep = first_head if side == 0 else jnp.logical_not(first_head)
            part = jnp.where(keep, query, jnp.zeros_like(query))
            scores = lax.dot_general(part, key, (((1,), (1,)), ((), ())), preferred_element_type=F32)
            la0 = -(rate_s[h] * scale_s[0])
            la1 = -(rate_s[h] * scale_s[1])
            power = jnp.where(late_t, la1, la0) * apart
            power = jnp.where(jnp.logical_and(late_t, jnp.logical_not(late_s)), la1 * into + la0 * left, power)
            scores = scores * jnp.where(causal, jnp.exp(jnp.where(causal, power, 0.0)), 0.0)
            high = scores.astype(BF16)
            low = (scores - high.astype(F32)).astype(BF16)
            vcols = slice(int(ends[2]) + h * DV, int(ends[2]) + (h + 1) * DV)
            value = pr[:, vcols].astype(BF16)
            ret = mm(high, value) + mm(low, value)
            ret = ret * lax.rsqrt(jnp.mean(ret * ret, axis=1, keepdims=True) + EPS)
            gcols = slice(int(ends[3]) + h * DV, int(ends[3]) + (h + 1) * DV)
            gated[:, h * DV : (h + 1) * DV] = (ret * silu(pr[:, gcols])).astype(BF16)

    per = feat // WIDE
    for side in (x1, x):
        for j in range(per):
            pm[side, :, j * WIDE : (j + 1) * WIDE] = mm(gated[...], O[side * per + j]).astype(BF16)
        if side is x1:
            put(lambda: pm.at[x1], lambda: rm, lambda: asem.at[2], xdev)

    only(far, (relay, 2, far_o), (own, 3, row), (own, 3, sib), (cross, 4), (own, 4, peer), (relay, 3, zp))
    only(
        near,
        (own, 3, row),
        (own, 3, sib),
        (relay, 3, zp),
        (relay, 3, near_o, peer),
        (relay, 3, far_o, peer),
        (cross, 4),
        (own, 4, peer),
    )
    got(rm, asem.at[2], "mix")

    @pl.loop(0, rows // 32)
    def _(i):
        at = pl.ds(pl.multiple_of(i * 32, 32), 32)
        mix = pm[x, at, :].astype(F32) + rm[at, :].astype(F32)
        R[0, x, at, :] = (tok[x, at, :].astype(F32) + mix).astype(BF16)

    put(lambda: R.at[0, x], lambda: R.at[0, x], lambda: asem.at[3], xdev)
    put(lambda: R.at[0, x], lambda: R.at[1, x], lambda: asem.at[4], mirror)
    only(far, (relay, 3, near_o), (relay, 3, far_o))
    own(4, row)
    own(4, sib)
    got(R.at[1, x], asem.at[4], "R1")
    put(lambda: R.at[1, x], lambda: R.at[1, x], lambda: asem.at[5], xdev)
    share(2)
    only(near, (relay, 4, zp), (relay, 4, near_o, peer))
    only(far, (relay, 4, zp))
    got(R.at[0, x1], asem.at[3], "R0x")
    norm_rows(R.at[0, 0], R.at[0, 1], 1, N2, 0)
    only(near, (relay, 4, far_o, peer))
    got(R.at[1, x1], asem.at[5], "R1x")
    norm_rows(R.at[1, 0], R.at[1, 1], 1, N2, rows)
    share(3)
    for kind in (2, 3):
        for zz in range(4):
            for yy in range(2):
                arrive(kind, zz, yy, c1)

    theirs, ours = slice(rows, 2 * rows), slice(0, rows)

    def hidden(part):
        def block(at):
            gate = mm(N2[part, :], G[:, at])
            up = mm(N2[part, :], U[:, at])
            hid[part, at] = (silu(gate) * up).astype(BF16)

        whole = half_ff // WIDE

        @pl.loop(0, whole)
        def _(j):
            block(pl.ds(pl.multiple_of(j * WIDE, WIDE), WIDE))

        if half_ff % WIDE:
            block(pl.ds(whole * WIDE, half_ff % WIDE))

    here = x == b
    away = jnp.logical_not(here)
    at_end = far.astype(jnp.int32)

    def chip(half, i):
        return jnp.where(i % 2 == 1, 3 * half, 1 + half), jnp.where(i >= 2, y1, y)

    def columns(i):
        zz, yy = chip(x, i)
        return pl.ds(pl.multiple_of(((zz - 2 * x) * 2 + yy) * WIDE, WIDE), WIDE)

    def send_x(i, k, start):
        at = pl.ds(start, rows)
        put(lambda: sx.at[i, at, :], lambda: rx.at[i, at, :], lambda: asem.at[6 + 2 * i + k], xdev)

    def give(zz, yy, i, *parts):
        for k, part in enumerate((theirs, ours)):
            if part in parts:
                sx[i, part, :] = mm(hid[part, :], Dn[zz * 2 + yy]).astype(BF16)
                send_x(i, k, part.start)

    def keep(zz, yy, i, *parts):
        for part in parts:
            pmine[i, part, :] = mm(hid[part, :], Dn[zz * 2 + yy])

    def ready(zz):
        arrive(4, zz, y1, c)
        fwd(4, zz, y1, c, sib)

    def event(zz, yy, i, first, *parts):
        only(here if first else away, (keep, zz, yy, i) + parts)
        only(away if first else here, (give, zz, yy, i) + parts)

    def combine(i):
        got(rx.at[i, pl.ds(rows, rows), :], asem.at[6 + 2 * i], "rx")
        sz[i] = (pmine[i, theirs, :] + rx[i, theirs, :].astype(F32)).astype(BF16)
        put(lambda: sz.at[i], lambda: rz.at[i], lambda: asem.at[14 + i], mirror)

    def add(i):
        got(rx.at[i, pl.ds(0, rows), :], asem.at[7 + 2 * i], "rx")
        resid = R[0, x, :, columns(i)].astype(F32)
        tot[i] = resid + (pmine[i, ours, :] + rx[i, ours, :].astype(F32))

    def close(i):
        got(rz.at[i], asem.at[14 + i], "rz")
        now = tot[i] + rz[i].astype(F32)
        tot[i] = now
        square = now * now
        return square[:, : WIDE // 2] + square[:, WIDE // 2 :]

    first = (at_end, 1 - at_end, 2 + at_end, 3 - at_end)
    order = [jnp.where(here, i, k) for k, i in enumerate(first)]
    hidden(theirs)
    for zz, i in ((z, 0), (zp, 1)):
        arrive(4, zz, y, c1)
        event(zz, y, first[i], True, theirs)
    only(far, (relay, 4, near_o))
    hidden(ours)
    for zz, i in ((z, 0), (zp, 1)):
        event(zz, y, first[i], True, ours)
    only(far, (relay, 4, far_o))
    arrive(4, near_o, y, c1)
    event(near_o, y, 0, False, theirs, ours)
    ready(z)
    arrive(4, far_o, y, c1)
    event(far_o, y, 1, False, theirs, ours)
    ready(zp)
    combine(order[0])
    arrive(4, z, y1, c1)
    event(z, y1, first[2], True, theirs, ours)
    combine(order[1])
    arrive(4, zp, y1, c1)
    event(zp, y1, first[3], True, theirs, ours)
    add(order[0])
    add(order[1])
    ready(near_o)
    arrive(4, near_o, y1, c1)
    event(near_o, y1, 2, False, theirs, ours)
    ready(far_o)
    squares = close(order[0])
    arrive(4, far_o, y1, c1)
    event(far_o, y1, 3, False, theirs, ours)
    squares = squares + close(order[1])
    for k in (2, 3):
        combine(order[k])
        add(order[k])
    squares = squares + close(order[2])
    squares = squares + close(order[3])
    mine_sq = jnp.broadcast_to(jnp.sum(squares, axis=1, keepdims=True), (rows, 128))
    ss_s[...] = mine_sq.T[0:8, :]
    put(lambda: ss_s, lambda: ss_r, lambda: asem.at[18], xdev)
    got(ss_r, asem.at[18], "ss")
    total = ss_s[0:1, :] + ss_r[0:1, :]
    total = jnp.broadcast_to(total, (128, rows)).T[:, 0:1]
    scale = lax.rsqrt(total / width + EPS)
    for i in range(4):
        out_ref[:, columns(i)] = (tot[i] * scale * gn[x, 2:3, columns(i)]).astype(out_ref.dtype)

    for who in (None, near, far, here, away):
        copies = [copy for owner, copy in sends if owner is who]

        def drain(copies=copies):
            for copy in copies:
                copy().wait_send()

        drain() if who is None else pl.when(who)(drain)


def tables(rows):
    half = DK // 2
    inverse = np.float32(THETA) ** (-np.arange(half, dtype=np.float32) / np.float32(half))
    angle = (np.arange(rows, dtype=np.float32) % SEQ_LEN)[:, None] * inverse
    cosine, sine = np.cos(angle), np.sin(angle)
    return (
        np.concatenate([cosine] * 4, axis=1).astype(np.float32),
        np.concatenate([-sine, sine, -sine, sine], axis=1).astype(np.float32),
    )


def fused(
    tokens,
    mix_gain,
    query_weight,
    key_weight,
    value_weight,
    output_gate_weight,
    out_weight,
    head_rates,
    block_scale,
    ffn_gain,
    ff_gate,
    ff_up,
    ff_down,
    final_gain,
):
    rows, feat = tokens.shape
    size = lax.axis_size("fs")
    chips = size // 2
    width = 2 * feat
    half_ff = ff_gate.shape[1] // 2
    joint = sum(w.shape[1] for w in (query_weight, key_weight, value_weight, output_gate_weight))
    heads = head_rates.shape[0]
    line = lax.broadcasted_iota(jnp.int32, (8, feat), 0)
    gains = jnp.where(line == 0, mix_gain[None], jnp.where(line == 1, ffn_gain[None], final_gain[None])).astype(F32)
    cosine, sine = tables(rows)
    cw = out_weight.shape[1]
    hbm = pl.BlockSpec(memory_space=pl.ANY)
    smem = pl.BlockSpec(memory_space=pltpu.SMEM)
    vmem = pl.BlockSpec(memory_space=pltpu.VMEM)
    dma = pltpu.SemaphoreType.DMA
    return pl.pallas_call(
        layer_kernel,
        out_shape=jax.ShapeDtypeStruct((rows, feat), BF16),
        in_specs=[hbm] * 7 + [smem] * 2 + [hbm] * 3 + [vmem] * 2,
        out_specs=vmem,
        scratch_shapes=[
            pltpu.VMEM((2, rows, feat), BF16),
            pltpu.VMEM((2, 8, feat), F32),
            pltpu.VMEM((width, joint), BF16),
            pltpu.VMEM((chips, out_weight.shape[0], 2 * cw), BF16),
            pltpu.VMEM((width, half_ff), BF16),
            pltpu.VMEM((width, half_ff), BF16),
            pltpu.VMEM((chips, half_ff, 2 * cw), BF16),
            pltpu.VMEM((rows, width), BF16),
            pltpu.VMEM((rows, joint), F32),
            pltpu.VMEM((rows, heads * DV), BF16),
            pltpu.VMEM((2, rows, feat), BF16),
            pltpu.VMEM((rows, feat), BF16),
            pltpu.VMEM((2, 2, rows, feat), BF16),
            pltpu.VMEM((2 * rows, width), BF16),
            pltpu.VMEM((2 * rows, half_ff), BF16),
            pltpu.VMEM((4, 2 * rows, WIDE), BF16),
            pltpu.VMEM((4, 2 * rows, WIDE), BF16),
            pltpu.VMEM((4, 2 * rows, WIDE), F32),
            pltpu.VMEM((4, rows, WIDE), BF16),
            pltpu.VMEM((4, rows, WIDE), BF16),
            pltpu.VMEM((4, rows, WIDE), F32),
            pltpu.VMEM((8, rows), F32),
            pltpu.VMEM((8, rows), F32),
            dma((12,)),
            dma((160,)),
            dma((5, size)),
            dma((20,)),
        ],
        compiler_params=pltpu.CompilerParams(
            collective_id=0, has_side_effects=True, vmem_limit_bytes=60 * 2**20
        ),
    )(
        tokens,
        gains,
        query_weight,
        key_weight,
        value_weight,
        output_gate_weight,
        out_weight,
        head_rates,
        block_scale,
        ff_gate,
        ff_up,
        ff_down,
        cosine,
        sine,
    )


def kernel_fits(mesh, tokens, query_weight, ff_gate, head_rates):
    size, parts = mesh.shape["fs"], mesh.shape["tp"]
    if size != 4 * 2 * 2 or parts != 2:
        return False
    rows, width = tokens.shape[0] // size, tokens.shape[1]
    return (
        rows == SEQ_LEN
        and SEQ_LEN == 2 * BLK
        and width // size * 2 == WIDE
        and ff_gate.shape[1] % (4 * 128) == 0
        and head_rates.shape[0] % (2 * parts) == 0
    )


def dispatch(mesh, *args):
    fits = kernel_fits(mesh, args[0], args[2], args[10], args[7])
    return jax.shard_map(
        fused if fits else body,
        mesh=mesh,
        in_specs=SPECS,
        out_specs=P("fs", "tp"),
        check_vma=False,
    )(*args)


SPECS = (
    P("fs", "tp"),
    P("tp"),
    P("fs", "tp"),
    P("fs", "tp"),
    P("fs", "tp"),
    P("fs", "tp"),
    P("tp", "fs"),
    P("tp"),
    P("fs"),
    P("tp"),
    P("fs", "tp"),
    P("fs", "tp"),
    P("tp", "fs"),
    P("tp"),
)


def solution(mesh):
    return functools.partial(dispatch, mesh)
```

```python
import functools

import jax
import jax.numpy as jnp
import numpy as np
from jax import lax
from jax.experimental import pallas as pl
from jax.experimental.pallas import tpu as pltpu
from jax.sharding import PartitionSpec as P

D = 2048
DK = 64
DV = 128
BLK = 128
SEQ_LEN = 256


EPS = 1e-06
THETA = 10000.0


def rms_norm(values, gain):
    scale = lax.rsqrt(jnp.mean(values * values, axis=-1, keepdims=True) + EPS)
    return values * scale * gain.astype(jnp.float32)


def rotate(values, positions):
    half = values.shape[-1] // 2
    inverse = THETA ** (-jnp.arange(half, dtype=jnp.float32) / half)
    angle = positions.astype(jnp.float32)[:, None] * inverse
    cosine = jnp.cos(angle)[:, None, :]
    sine = jnp.sin(angle)[:, None, :]
    first = values[..., :half]
    second = values[..., half:]
    return jnp.concatenate(
        [first * cosine - second * sine, second * cosine + first * sine], axis=-1
    )


def retain(query, key, value, rates, scales):
    rows, heads_here, width_k = query.shape
    width_v = value.shape[-1]
    nblk = rows // BLK
    hi = lax.Precision.HIGHEST
    qblk = query.astype(jnp.float32).reshape(nblk, BLK, heads_here, width_k)
    kblk = key.astype(jnp.float32).reshape(nblk, BLK, heads_here, width_k)
    vblk = value.astype(jnp.float32).reshape(nblk, BLK, heads_here, width_v)
    logdec = -rates[None, :] * scales[:, None]
    steps = jnp.arange(BLK, dtype=jnp.float32)
    offset = steps[:, None] - steps[None, :]
    causal = offset >= 0
    inside = jnp.where(
        causal[None, None],
        jnp.exp(logdec[:, :, None, None] * jnp.where(causal, offset, 0.0)[None, None]),
        0.0,
    )
    scores = jnp.einsum("nchd,nmhd->nhcm", qblk, kblk, precision=hi) * inside
    inner = jnp.einsum("nhcm,nmhe->nche", scores, vblk, precision=hi)
    zeta = jnp.exp(logdec[:, :, None] * (BLK - 1.0 - steps)[None, None, :])
    kv_block = jnp.einsum(
        "nchd,nche->nhde", kblk * jnp.transpose(zeta, (0, 2, 1))[..., None], vblk, precision=hi
    )
    hold = jnp.exp(logdec * BLK)
    per_seq = SEQ_LEN // BLK
    fresh = (jnp.arange(nblk, dtype=jnp.int32) % per_seq == 0).astype(jnp.float32)

    def advance(state, inputs):
        kv_now, hold_now, fresh_now = inputs
        before = state * (1.0 - fresh_now)
        return (before * hold_now[:, None, None] + kv_now, before)

    start = jnp.zeros((heads_here, width_k, width_v), jnp.float32)
    _, before = lax.scan(advance, start, (kv_block, hold, fresh), unroll=True)
    xi = jnp.exp(logdec[:, :, None] * (steps + 1.0)[None, None, :])
    cross = jnp.einsum(
        "nchd,nhde->nche", qblk * jnp.transpose(xi, (0, 2, 1))[..., None], before, precision=hi
    )
    total = inner + cross
    total = total * lax.rsqrt(jnp.mean(total * total, axis=-1, keepdims=True) + EPS)
    return total.reshape(rows, heads_here * width_v)


def chip_ring(size):
    chips = size // 2
    return list(range(0, chips, 2)) + list(range(1, chips, 2))[::-1]


def ring_place(size):
    ring = chip_ring(size)
    me = lax.axis_index("fs")
    chip = me // 2
    place = jnp.zeros((), jnp.int32)
    for index, member in enumerate(ring):
        place = jnp.where(chip == member, index, place)
    return place, me % 2


def after(value, *others):
    return lax.optimization_barrier((value,) + tuple(others))[0]


def circulate(block, axis, gates=()):
    size = lax.axis_size("fs")
    ring = chip_ring(size)
    chips = len(ring)
    onward = [
        (2 * ring[i] + core, 2 * ring[(i + 1) % chips] + core)
        for i in range(chips)
        for core in range(2)
    ]
    back = [(target, source) for source, target in onward]
    swap = [(i, i ^ 1) for i in range(size)]
    held = {0: block}
    reach = (chips - 1) // 2
    down = up = block
    for step in range(1, reach + 1):
        if len(gates) >= step and gates[step - 1]:
            down = after(down, *gates[step - 1])
            up = after(up, *gates[step - 1])
        down = lax.ppermute(down, "fs", onward)
        up = lax.ppermute(up, "fs", back)
        held[-step] = down
        held[step] = up
    if chips % 2 == 0 and chips > 1:
        cut = 1 - axis
        half = block.shape[cut] // 2
        if len(gates) > reach and gates[reach]:
            down = after(down, *gates[reach])
            up = after(up, *gates[reach])
        first = lax.ppermute(lax.slice_in_dim(down, 0, half, axis=cut), "fs", onward)
        second = lax.ppermute(lax.slice_in_dim(up, half, None, axis=cut), "fs", back)
        held[reach + 1] = jnp.concatenate([first, second], axis=cut)
    groups = []
    for offsets in order_of(size):
        own = jnp.concatenate([held[o] for o in offsets], axis=axis)
        groups.append((own, lax.ppermute(own, "fs", swap)))
    return held, groups


def order_of(size):
    chips = size // 2
    reach = (chips - 1) // 2
    groups = [list(range(-reach, reach + 1))]
    if chips > 1 and chips % 2 == 0:
        groups.append([reach + 1])
    return groups


def lane_of(values, lane, wide):
    count = values.shape[1] // (2 * wide)
    return [values[:, (2 * c + lane) * wide : (2 * c + lane + 1) * wide] for c in range(count)]


def to_ring(values, place, core):
    size = lax.axis_size("fs")
    wide = values.shape[1] // size
    ring = chip_ring(size)
    chips = len(ring)
    groups = order_of(size)
    start = (place + groups[0][0] + chips) % chips
    lanes = []
    for lane in range(2):
        pieces = lane_of(values, lane, wide)
        ringed = jnp.concatenate([pieces[c] for c in ring] * 2, axis=1)
        lanes.append(lax.dynamic_slice_in_dim(ringed, start * wide, chips * wide, axis=1))
    own = jnp.where(core == 0, lanes[0], lanes[1])
    other = jnp.where(core == 0, lanes[1], lanes[0])
    result, edge = [], 0
    for offsets in groups:
        end = edge + len(offsets) * wide
        result.append((own[:, edge:end], other[:, edge:end]))
        edge = end
    return result


def from_ring(groups, place, core):
    size = lax.axis_size("fs")
    ring = chip_ring(size)
    chips = len(ring)
    own = jnp.concatenate([own for own, _ in groups], axis=1)
    other = jnp.concatenate([other for _, other in groups], axis=1)
    wide = own.shape[1] // chips
    start = (2 * chips - place - order_of(size)[0][0]) % chips
    lanes = []
    for lane in range(2):
        straight = jnp.where(core == lane, own, other)
        doubled = jnp.concatenate([straight, straight], axis=1)
        lanes.append(lax.dynamic_slice_in_dim(doubled, start * wide, chips * wide, axis=1))
    spot = {c: i for i, c in enumerate(ring)}
    return jnp.concatenate(
        [
            lanes[lane][:, spot[c] * wide : (spot[c] + 1) * wide]
            for c in range(chips)
            for lane in range(2)
        ],
        axis=1,
    )


def tp_gather(values, axis):
    if lax.axis_size("tp") != 2:
        return lax.all_gather(values, "tp", axis=axis, tiled=True)
    other = lax.ppermute(values, "tp", [(0, 1), (1, 0)])
    mine = lax.axis_index("tp") == 0
    return jnp.concatenate(
        [jnp.where(mine, values, other), jnp.where(mine, other, values)], axis=axis
    )


def tp_sum(values):
    if lax.axis_size("tp") != 2:
        return lax.psum(values, "tp")
    return values + lax.ppermute(values, "tp", [(0, 1), (1, 0)])


def tp_scatter_sum(partial):
    if lax.axis_size("tp") != 2:
        pieces = lax.all_to_all(
            partial.reshape(partial.shape[0], lax.axis_size("tp"), -1), "tp", 1, 1
        )
        return jnp.sum(pieces.astype(jnp.float32), axis=1)
    half = partial.shape[1] // 2
    low = lax.axis_index("tp") == 0
    keep = jnp.where(low, partial[:, :half], partial[:, half:])
    send = jnp.where(low, partial[:, half:], partial[:, :half])
    got = lax.ppermute(send, "tp", [(0, 1), (1, 0)])
    return keep.astype(jnp.float32) + got.astype(jnp.float32)


def product_rows(left, groups, columns=slice(None), result=0.0):
    for pieces, blocks in zip(left, groups):
        for piece, block in zip(pieces, blocks):
            result = result + jnp.dot(
                piece, block[:, columns], preferred_element_type=jnp.float32
            )
    return result


def product_columns(left, groups, place, core, columns=None):
    terms = []
    for blocks in groups:
        pair = []
        for block in blocks:
            if columns is None:
                dims, right = (((1,), (0,)), ((), ())), block
            else:
                dims, right = (((1,), (1,)), ((), ())), block[:, columns]
            term = lax.dot_general(left, right, dims, preferred_element_type=jnp.float32)
            pair.append(term.astype(jnp.bfloat16))
        terms.append(pair)
    return from_ring(terms, place, core)


def body(
    tokens,
    mix_gain,
    query_weight,
    key_weight,
    value_weight,
    output_gate_weight,
    out_weight,
    head_rates,
    block_scale,
    ffn_gain,
    ff_gate,
    ff_up,
    ff_down,
    final_gain,
):
    rows = tokens.shape[0]
    heads_here = head_rates.shape[0]
    size = lax.axis_size("fs")
    place, core = ring_place(size)
    reach = (size // 2 - 1) // 2
    positions = jnp.arange(rows, dtype=jnp.int32) % SEQ_LEN

    bundle = jnp.concatenate(
        [query_weight, key_weight, value_weight, output_gate_weight, out_weight.T], axis=1
    )
    hops, proj = circulate(bundle, 0)
    last = (hops[-reach], hops[reach])

    whole = tp_gather(tokens, 1)
    gains = tp_gather(jnp.stack([mix_gain, ffn_gain]), 1)
    normed = rms_norm(whole.astype(jnp.float32), gains[0]).astype(jnp.bfloat16)
    width = bundle.shape[1] - out_weight.shape[0]
    projected = product_rows(to_ring(normed, place, core), proj, slice(0, width))
    ends = [query_weight.shape[1], key_weight.shape[1], value_weight.shape[1]]
    qproj, kproj, vproj, gproj = jnp.split(
        projected, [ends[0], ends[0] + ends[1], sum(ends)], axis=1
    )
    query = rotate(qproj.reshape(rows, heads_here, DK), positions).astype(jnp.bfloat16)
    key = (rotate(kproj.reshape(rows, heads_here, DK), positions) * DK ** (-0.5)).astype(
        jnp.bfloat16
    )
    value = vproj.astype(jnp.bfloat16).reshape(rows, heads_here, DV)
    normret = retain(query, key, value, head_rates, block_scale)
    gated = (normret * jax.nn.silu(gproj)).astype(jnp.bfloat16)
    opposite = tuple(hops[o] for o in order_of(size)[-1])
    gate_hops, gates = circulate(ff_gate, 0, ((), opposite, (projected,)))
    up_hops, ups = circulate(ff_up, 0, (last, (), (gated,)))
    mix = tp_scatter_sum(product_columns(gated, proj, place, core, slice(width, None)))
    resid = (tokens.astype(jnp.float32) + mix).astype(jnp.bfloat16)
    whole2 = tp_gather(resid, 1)
    normed2 = to_ring(
        rms_norm(whole2.astype(jnp.float32), gains[1]).astype(jnp.bfloat16), place, core
    )
    gate_part = product_rows(normed2[:1], gates[:1])
    up_part = product_rows(normed2[:1], ups[:1])
    early_parts = (gate_part, up_part)
    gate_part = product_rows(normed2[1:], gates[1:], result=gate_part)
    up_part = product_rows(normed2[1:], ups[1:], result=up_part)
    hidden = (jax.nn.silu(gate_part) * up_part).astype(jnp.bfloat16)
    near = (gate_hops[-reach], gate_hops[reach])
    far = order_of(size)[-1][-1]
    second = (normed2[0][0], up_hops[-reach], up_hops[reach])
    third = early_parts + (gate_hops[far], up_hops[far])
    _, downs = circulate(ff_down, 1, (near, second, third))
    ffn = tp_scatter_sum(product_columns(hidden, downs, place, core))
    total = resid.astype(jnp.float32) + ffn
    squares = tp_sum(jnp.sum(total * total, axis=-1))[:, None]
    scale = lax.rsqrt(squares / D + EPS)
    return (total * scale * final_gain.astype(jnp.float32)).astype(jnp.bfloat16)


MESH = pl.DeviceIdType.MESH
F32 = jnp.float32
BF16 = jnp.bfloat16
WIDE = 256


def silu(v):
    return v / (1.0 + jnp.exp(-v))


def mm(a, b):
    return jnp.dot(a, b, preferred_element_type=F32)


def layer_kernel(
    tok_h,
    gain_h,
    q_h,
    k_h,
    v_h,
    g_h,
    o_h,
    rate_s,
    fg_h,
    fu_h,
    fd_h,
    cos_ref,
    sin_ref,
    out_ref,
    tok,
    gn,
    gr,
    Ps,
    P,
    O,
    G,
    U,
    Dn,
    pr,
    gsend,
    gated,
    sm,
    pm,
    rm,
    R,
    N2,
    gacc,
    uacc,
    hid,
    sx,
    rx,
    pmine,
    sz,
    rz,
    tot,
    ss_s,
    ss_r,
    lsem,
    ssem,
    wsem,
    asem,
):
    rows, feat = tok_h.shape
    width = 2 * feat
    rw = q_h.shape[0]
    cw = o_h.shape[1]
    half_ff = fg_h.shape[1] // 2
    heads = rate_s.shape[0]
    f = lax.axis_index("fs")
    x = lax.axis_index("tp")
    c = f % 2
    y = (f // 2) % 2
    z = f // 4
    b = z // 2
    zp = 4 * b + 1 - z
    zm = 3 - z
    near_o = 2 - b
    far_o = 3 * (1 - b)
    near = jnp.logical_or(z == 1, z == 2)
    far = jnp.logical_not(near)
    y1, c1, x1 = 1 - y, 1 - c, 1 - x

    def dev(zz, yy, cc, xx):
        return ((zz * 2 + yy) * 2 + cc, xx)

    here = x == b
    away = jnp.logical_not(here)
    roles = (None, near, far, here, away)
    pools = ((0, 28), (28, 36), (28, 36), (64, 8), (64, 8))
    sends = [[] for _ in roles]
    role = [0]

    def put(src, dst, sem, to):
        base, size = pools[role[0]]
        copies = sends[role[0]]
        index = base + len(copies) % size

        def copy():
            return pltpu.make_async_remote_copy(
                src_ref=src(),
                dst_ref=dst(),
                send_sem=ssem.at[index],
                recv_sem=sem(),
                device_id=to,
                device_id_type=MESH,
            )

        if len(copies) >= size:
            copies[len(copies) - size]().wait_send()
        copy().start()
        copies.append(copy)

    def only(who, *acts):
        @pl.when(who)
        def _():
            role[0] = [who is r for r in roles].index(True)
            for act, *args in acts:
                act(*args)
            role[0] = 0

    def got(ref, sem, name="got"):
        copy = pltpu.make_async_remote_copy(
            src_ref=ref,
            dst_ref=ref,
            send_sem=ssem.at[0],
            recv_sem=sem,
            device_id=dev(z, y, c1, x),
            device_id_type=MESH,
        )
        with jax.named_scope(name):
            copy.wait_recv()

    local = []

    def take(src, dst):
        copy = pltpu.make_async_copy(src, dst, lsem.at[len(local)])
        copy.start()
        local.append(copy)
        return copy

    def row_slot(buf):
        def slot(zz, yy, cc):
            start = pl.multiple_of(((zz * 2 + yy) * 2 + cc) * rw, rw)
            return buf.at[pl.ds(start, rw), :]

        return slot

    def col_slot(buf):
        def slot(zz, yy, cc):
            return buf.at[zz * 2 + yy, :, pl.ds(pl.multiple_of(cc * cw, cw), cw)]

        return slot

    deep = half_ff // 2

    def down_slot(k):
        def slot(zz, yy, cc):
            return Dn.at[zz * 2 + yy, pl.ds(k * deep, deep), pl.ds(pl.multiple_of(cc * cw, cw), cw)]

        return slot

    sP, sO, sG, sU = row_slot(P), col_slot(O), row_slot(G), row_slot(U)
    slots = (sP, sO, sG, sU, down_slot(0), down_slot(1))
    DOWN = (4, 5)

    def sem_of(kind, zz, yy, cc):
        return wsem.at[kind, (zz * 2 + yy) * 2 + cc]

    def fwd(kind, zz, yy, cc, to):
        ref = functools.partial(slots[kind], zz, yy, cc)
        put(ref, ref, functools.partial(sem_of, kind, zz, yy, cc), to)

    def arrive(kind, zz, yy, cc):
        side = "sib" if cc is c1 else "row" if yy is y1 else "col"
        got(slots[kind](zz, yy, cc), sem_of(kind, zz, yy, cc), f"{side}{kind}")

    sib = dev(z, y, c1, x)
    row = dev(z, y1, c, x)
    peer = dev(zp, y, c, x)
    xdev = dev(z, y, c, x1)
    mirror = dev(zm, y, c, x)

    parts = [ref.shape[1] // 2 for ref in (q_h, k_h, v_h, g_h)]
    ends = np.cumsum([0] + parts).tolist()
    mine = pl.multiple_of(((z * 2 + y) * 2 + c) * rw, rw)
    own_p, stage_p = [], []
    for i, ref in enumerate((q_h, k_h, v_h, g_h)):
        to = pl.ds(ends[i], parts[i])
        at = pl.ds(pl.multiple_of(y * parts[i], 128), parts[i])
        own_p.append(take(ref.at[:, at], P.at[pl.ds(mine, rw), to]))
        at = pl.ds(pl.multiple_of(y1 * parts[i], 128), parts[i])
        stage_p.append(take(ref.at[:, at], Ps.at[:, to]))
    own_o = take(o_h, sO(z, y, c))
    own_t = [take(tok_h, tok.at[0, x]), take(gain_h, gn.at[x])]
    at_b = pl.multiple_of(b * half_ff, 128)
    at_o = pl.multiple_of((1 - b) * half_ff, 128)
    own_g = take(fg_h.at[:, pl.ds(at_b, half_ff)], sG(z, y, c))
    own_u = take(fu_h.at[:, pl.ds(at_b, half_ff)], sU(z, y, c))
    own_d = take(fd_h.at[pl.ds(at_b, half_ff), :], col_slot(Dn)(z, y, c))

    barrier = pltpu.get_barrier_semaphore()
    friends = [sib, row, xdev] + [dev((z + k) % 4, y, c, x) for k in (1, 2, 3)]
    for to in friends:
        pl.semaphore_signal(barrier, inc=1, device_id=to, device_id_type=MESH)
    pl.semaphore_wait(barrier, len(friends))

    put(lambda: tok_h, lambda: tok.at[0, x], lambda: asem.at[0], xdev)
    put(lambda: gain_h, lambda: gn.at[x], lambda: asem.at[1], xdev)

    other = {
        2: lambda: fg_h.at[:, pl.ds(at_o, half_ff)],
        3: lambda: fu_h.at[:, pl.ds(at_o, half_ff)],
        4: lambda: fd_h.at[pl.ds(at_o, deep), :],
        5: lambda: fd_h.at[pl.ds(pl.multiple_of(at_o + deep, 16), deep), :],
    }
    beyond = dev(near_o, y, c, x)

    def own(kind, to):
        fwd(kind, z, y, c, to)

    def cross(kind):
        slot = functools.partial(slots[kind], z, y, c)
        put(other[kind], slot, functools.partial(sem_of, kind, z, y, c), beyond)

    def relay(kind, zz, *to):
        arrive(kind, zz, y, c)
        for device in to + (row, sib):
            fwd(kind, zz, y, c, device)

    def arrive_down(*place):
        for kind in DOWN:
            arrive(kind, *place)

    def down(act, *args):
        return [(act, kind) + args for kind in DOWN]

    def share(kind):
        for zz in (z, zp, near_o, far_o):
            arrive(kind, zz, y1, c)
            fwd(kind, zz, y1, c, sib)

    def line(zz, yy, *to):
        arrive(0, zz, yy, c)
        for device in to + (sib,):
            fwd(0, zz, yy, c, device)

    for copy in stage_p + own_p:
        copy.wait()
    put(lambda: Ps, lambda: sP(z, y, c), lambda: sem_of(0, z, y, c), row)
    own(0, peer)
    only(near, (own, 0, beyond))
    own(0, sib)
    put(lambda: tok_h, lambda: tok.at[1, x], lambda: asem.at[2], row)
    put(lambda: gain_h.at[:, pl.ds(0, 128)], lambda: gr, lambda: asem.at[3], row)
    own_o.wait()
    own(1, row)
    own(1, peer)
    only(near, (own, 1, beyond))
    own(1, sib)
    own_g.wait()
    own(2, row)
    own(2, sib)
    only(far, (line, z, y1, peer), (own, 2, peer), (line, zp, y), (relay, 1, zp), (line, zp, y1))
    only(
        near,
        (line, z, y1, peer, beyond),
        (line, zp, y, beyond),
        (line, near_o, y, peer),
        (relay, 1, zp, beyond),
        (relay, 1, near_o, peer),
        (line, zp, y1, beyond),
        (line, near_o, y1, peer),
    )

    for copy in own_t:
        copy.wait()
    got(tok.at[0, x1], asem.at[0], "tok")
    got(gn.at[x1], asem.at[1])

    def norm_rows(first, second, gain_row, dst, base):
        chunk = 32

        @pl.loop(0, rows // chunk)
        def _(i):
            at = pl.ds(pl.multiple_of(i * chunk, chunk), chunk)
            one = first[at, :].astype(F32)
            two = second[at, :].astype(F32)
            total = jnp.sum(one * one, axis=1, keepdims=True) + jnp.sum(two * two, axis=1, keepdims=True)
            scale = lax.rsqrt(total / width + EPS)
            to = pl.ds(pl.multiple_of(base + i * chunk, chunk), chunk)
            dst[to, 0:feat] = (one * scale * gn[0, gain_row : gain_row + 1, :]).astype(BF16)
            dst[to, feat:width] = (two * scale * gn[1, gain_row : gain_row + 1, :]).astype(BF16)

    norm_rows(tok.at[0, 0], tok.at[0, 1], 0, N2, 0)
    got(tok.at[1, x], asem.at[2], "tok")
    put(lambda: tok.at[1, x], lambda: tok.at[1, x], lambda: asem.at[4], xdev)
    got(gr, asem.at[3])
    own_u.wait()
    own_d.wait()
    only(
        far,
        (line, near_o, y),
        (line, near_o, y1),
        (relay, 1, near_o),
        (cross, 2),
        (line, far_o, y),
        (line, far_o, y1),
        (relay, 1, far_o),
        (own, 3, peer),
        (cross, 3),
    )
    only(
        near,
        (line, far_o, y, peer),
        (line, far_o, y1, peer),
        (relay, 1, far_o, peer),
        (own, 2, peer),
        (cross, 2),
        (relay, 2, zp),
        (cross, 3),
    )
    got(tok.at[1, x1], asem.at[4], "tok")
    norm_rows(tok.at[1, 0], tok.at[1, 1], 0, N2, rows)
    for zz in range(4):
        for yy in range(2):
            arrive(0, zz, yy, c1)

    @pl.loop(0, P.shape[1] // WIDE)
    def _(j):
        at = pl.ds(pl.multiple_of(j * WIDE, WIDE), WIDE)
        pr[:, at] = mm(N2[...], P[:, at])

    blk = rows // 2
    t = lax.broadcasted_iota(jnp.int32, (rows, rows), 0)
    s = lax.broadcasted_iota(jnp.int32, (rows, rows), 1)
    late_t, late_s = t >= blk, s >= blk
    apart = (t - s).astype(F32)
    into = (t - (blk - 1)).astype(F32)
    left = ((blk - 1) - s).astype(F32)
    causal = t >= s
    lane = lax.broadcasted_iota(jnp.int32, (rows, 2 * DK), 1)
    early = (lane % DK) < DK // 2
    first_head = lane < DK

    def turn(v):
        swapped = jnp.where(early, pltpu.roll(v, 2 * DK - DK // 2, 1), pltpu.roll(v, DK // 2, 1))
        return v * cos_ref[...] + swapped * sin_ref[...]

    def retain_rows(at, scales, dst):
        s0, s1 = scales[3:4, 0:1], scales[4:5, 0:1]
        for two in range(heads // 4):
            cols = slice(ends[0] + two * 2 * DK, ends[0] + (two + 1) * 2 * DK)
            query = turn(pr[at, cols]).astype(BF16)
            cols = slice(ends[1] + two * 2 * DK, ends[1] + (two + 1) * 2 * DK)
            key = (turn(pr[at, cols]) * DK ** (-0.5)).astype(BF16)
            for side in range(2):
                h = 2 * two + side
                rate = rate_s[y * (heads // 2) + h]
                keep = first_head if side == 0 else jnp.logical_not(first_head)
                part = jnp.where(keep, query, jnp.zeros_like(query))
                scores = lax.dot_general(part, key, (((1,), (1,)), ((), ())), preferred_element_type=F32)
                la0, la1 = -(rate * s0), -(rate * s1)
                power = jnp.where(late_t, la1, la0) * apart
                power = jnp.where(jnp.logical_and(late_t, jnp.logical_not(late_s)), la1 * into + la0 * left, power)
                scores = scores * jnp.where(causal, jnp.exp(jnp.where(causal, power, 0.0)), 0.0)
                high = scores.astype(BF16)
                low = (scores - high.astype(F32)).astype(BF16)
                value = pr[at, ends[2] + h * DV : ends[2] + (h + 1) * DV].astype(BF16)
                ret = mm(high, value) + mm(low, value)
                ret = ret * lax.rsqrt(jnp.mean(ret * ret, axis=1, keepdims=True) + EPS)
                gate = pr[at, ends[3] + h * DV : ends[3] + (h + 1) * DV]
                dst[:, h * DV : (h + 1) * DV] = (ret * silu(gate)).astype(BF16)

    retain_rows(slice(rows, 2 * rows), gr, gsend)
    put(lambda: gsend, lambda: gated.at[y], lambda: asem.at[5], row)
    retain_rows(slice(0, rows), gn.at[x], gated.at[y])
    only(far, (relay, 2, zp), (own, 3, row), (own, 3, sib))
    only(near, (relay, 2, near_o, peer))
    share(1)
    for zz in range(4):
        for yy in range(2):
            arrive(1, zz, yy, c1)
    got(gated.at[y1], asem.at[5], "gated")

    per = feat // WIDE
    half_o = O.shape[1] // 2

    def out_block(side, j):
        weights = O.at[side * per + j]
        return mm(gated[0], weights[0:half_o, :]) + mm(gated[1], weights[half_o:, :])

    def send_mix(j):
        put(lambda: sm.at[j], lambda: rm.at[j], lambda: asem.at[6 + j], xdev)

    for j in range(per):
        sm[j] = out_block(x1, j).astype(BF16)
        send_mix(j)
    for j in range(per):
        pm[j] = out_block(x, j).astype(BF16)

    only(far, (relay, 2, near_o), *down(own, row), *down(own, sib))
    only(
        near,
        (relay, 2, far_o, peer),
        (own, 3, peer),
        (own, 3, row),
        (own, 3, sib),
        (relay, 3, zp),
    )

    def block(j):
        return pl.ds(j * WIDE, WIDE)

    def send_resid(j):
        put(lambda: R.at[0, x, :, block(j)], lambda: R.at[1, x, :, block(j)], lambda: asem.at[10 + j], mirror)
        put(lambda: R.at[0, x, :, block(j)], lambda: R.at[0, x, :, block(j)], lambda: asem.at[14 + j], xdev)

    def pass_resid(j):
        got(R.at[1, x, :, block(j)], asem.at[10 + j], "R1")
        put(lambda: R.at[1, x, :, block(j)], lambda: R.at[1, x, :, block(j)], lambda: asem.at[18 + j], xdev)

    for j in range(per):
        got(rm.at[j], asem.at[6 + j], "mix")
        mix = pm[j].astype(F32) + rm[j].astype(F32)
        R[0, x, :, block(j)] = (tok[0, x, :, block(j)].astype(F32) + mix).astype(BF16)
        send_resid(j)
    only(far, (relay, 2, far_o), *down(own, peer), (relay, 3, zp))
    only(near, (relay, 3, near_o, peer), (relay, 3, far_o, peer), *down(own, row), *down(own, sib))
    pass_resid(0)
    pass_resid(1)
    only(near, *down(cross), *down(own, peer))
    only(far, *down(cross), (relay, 3, near_o))
    pass_resid(2)
    pass_resid(3)
    only(near, *down(relay, zp))
    only(far, (relay, 3, far_o))
    share(2)
    for j in range(per):
        got(R.at[0, x1, :, block(j)], asem.at[14 + j], "R0x")
    norm_rows(R.at[0, 0], R.at[0, 1], 1, N2, 0)
    for j in range(per):
        got(R.at[1, x1, :, block(j)], asem.at[18 + j], "R1x")
    norm_rows(R.at[1, 0], R.at[1, 1], 1, N2, rows)
    only(far, *down(relay, zp))

    theirs, ours = slice(rows, 2 * rows), slice(0, rows)

    def over_columns(act):
        whole = half_ff // WIDE

        @pl.loop(0, whole)
        def _(j):
            act(pl.ds(pl.multiple_of(j * WIDE, WIDE), WIDE))

        if half_ff % WIDE:
            act(pl.ds(whole * WIDE, half_ff % WIDE))

    def gate_columns(at):
        gacc[:, at] = silu(mm(N2[...], G[:, at]))

    def up_of(part, at, *chips):
        total = 0.0
        for zz, yy in chips:
            deep_at = pl.ds(pl.multiple_of((zz * 2 + yy) * 2 * rw, 2 * rw), 2 * rw)
            total = total + mm(N2[part, deep_at], U[deep_at, at])
        return total

    def up_columns(at):
        for part in (theirs, ours):
            uacc[part, at] = up_of(
                part, at, (z, y), (zp, y), (near_o, y), (far_o, y), (z, y1), (zp, y1), (near_o, y1)
            )

    def hidden_columns(at):
        for part in (theirs, ours):
            up = uacc[part, at] + up_of(part, at, (far_o, y1))
            hid[part, at] = (gacc[part, at] * up).astype(BF16)

    for zz in range(4):
        for yy in range(2):
            arrive(2, zz, yy, c1)
    over_columns(gate_columns)
    only(near, *down(relay, near_o, peer))
    for zz in (z, zp, near_o, far_o):
        arrive(3, zz, y, c1)
    for zz in (z, zp, near_o):
        arrive(3, zz, y1, c)
        fwd(3, zz, y1, c, sib)
    for zz in (z, zp, near_o):
        arrive(3, zz, y1, c1)
    over_columns(up_columns)
    arrive(3, far_o, y1, c)
    fwd(3, far_o, y1, c, sib)
    only(near, *down(relay, far_o, peer))
    only(far, *down(relay, near_o))
    arrive(3, far_o, y1, c1)
    over_columns(hidden_columns)

    at_end = far.astype(jnp.int32)

    def chip(half, i):
        return jnp.where(i % 2 == 1, 3 * half, 1 + half), jnp.where(i >= 2, y1, y)

    def columns(i):
        zz, yy = chip(x, i)
        return pl.ds(pl.multiple_of(((zz - 2 * x) * 2 + yy) * WIDE, WIDE), WIDE)

    def send_x(i, k, start):
        at = pl.ds(start, rows)
        put(lambda: sx.at[i, at, :], lambda: rx.at[i, at, :], lambda: asem.at[22 + 2 * i + k], xdev)

    def give(zz, yy, i, *parts):
        for k, part in enumerate((theirs, ours)):
            if part in parts:
                sx[i, part, :] = mm(hid[part, :], Dn[zz * 2 + yy]).astype(BF16)
                send_x(i, k, part.start)

    def keep(zz, yy, i, *parts):
        pmine[i] = mm(hid[...], Dn[zz * 2 + yy])

    def ready(zz):
        for kind in DOWN:
            arrive(kind, zz, y1, c)
            fwd(kind, zz, y1, c, sib)

    def event(zz, yy, i, first, *parts):
        only(here if first else away, (keep, zz, yy, i) + parts)
        only(away if first else here, (give, zz, yy, i) + parts)

    def combine(i):
        got(rx.at[i, pl.ds(rows, rows), :], asem.at[22 + 2 * i], "rx")
        sz[i] = (pmine[i, theirs, :] + rx[i, theirs, :].astype(F32)).astype(BF16)
        put(lambda: sz.at[i], lambda: rz.at[i], lambda: asem.at[30 + i], mirror)

    def add(i):
        got(rx.at[i, pl.ds(0, rows), :], asem.at[23 + 2 * i], "rx")
        resid = R[0, x, :, columns(i)].astype(F32)
        tot[i] = resid + (pmine[i, ours, :] + rx[i, ours, :].astype(F32))

    def close(i):
        got(rz.at[i], asem.at[30 + i], "rz")
        now = tot[i] + rz[i].astype(F32)
        tot[i] = now
        square = now * now
        return square[:, : WIDE // 2] + square[:, WIDE // 2 :]

    first = (at_end, 1 - at_end, 2 + at_end, 3 - at_end)
    order = [jnp.where(here, i, k) for k, i in enumerate(first)]
    for zz, i in ((z, 0), (zp, 1)):
        arrive_down(zz, y, c1)
        event(zz, y, first[i], True, theirs, ours)
    only(far, *down(relay, far_o))
    arrive_down(near_o, y, c1)
    event(near_o, y, 0, False, theirs, ours)
    ready(z)
    arrive_down(far_o, y, c1)
    event(far_o, y, 1, False, theirs, ours)
    ready(zp)
    combine(order[0])
    arrive_down(z, y1, c1)
    event(z, y1, first[2], True, theirs, ours)
    combine(order[1])
    arrive_down(zp, y1, c1)
    event(zp, y1, first[3], True, theirs, ours)
    add(order[0])
    add(order[1])
    ready(near_o)
    arrive_down(near_o, y1, c1)
    event(near_o, y1, 2, False, theirs, ours)
    ready(far_o)
    squares = close(order[0])
    arrive_down(far_o, y1, c1)
    event(far_o, y1, 3, False, theirs, ours)
    squares = squares + close(order[1])
    for k in (2, 3):
        combine(order[k])
        add(order[k])
    squares = squares + close(order[2])
    squares = squares + close(order[3])
    mine_sq = jnp.broadcast_to(jnp.sum(squares, axis=1, keepdims=True), (rows, 128))
    ss_s[...] = mine_sq.T[0:8, :]
    put(lambda: ss_s, lambda: ss_r, lambda: asem.at[34], xdev)
    for who, (_, size), copies in zip(roles, pools, sends):

        def drain(copies=copies[-size:]):
            for copy in copies:
                copy().wait_send()

        drain() if who is None else pl.when(who)(drain)

    got(ss_r, asem.at[34], "ss")
    total = ss_s[0:1, :] + ss_r[0:1, :]
    total = jnp.broadcast_to(total, (128, rows)).T[:, 0:1]
    scale = lax.rsqrt(total / width + EPS)
    for i in range(4):
        out_ref[:, columns(i)] = (tot[i] * scale * gn[x, 2:3, columns(i)]).astype(out_ref.dtype)


def tables(rows):
    half = DK // 2
    inverse = np.float32(THETA) ** (-np.arange(half, dtype=np.float32) / np.float32(half))
    angle = (np.arange(rows, dtype=np.float32) % SEQ_LEN)[:, None] * inverse
    cosine, sine = np.cos(angle), np.sin(angle)
    return (
        np.concatenate([cosine] * 4, axis=1).astype(np.float32),
        np.concatenate([-sine, sine, -sine, sine], axis=1).astype(np.float32),
    )


def fused(
    tokens,
    mix_gain,
    query_weight,
    key_weight,
    value_weight,
    output_gate_weight,
    out_weight,
    head_rates,
    block_scale,
    ffn_gain,
    ff_gate,
    ff_up,
    ff_down,
    final_gain,
):
    rows, feat = tokens.shape
    size = lax.axis_size("fs")
    chips = size // 2
    width = 2 * feat
    half_ff = ff_gate.shape[1] // 2
    joint = sum(w.shape[1] for w in (query_weight, key_weight, value_weight, output_gate_weight)) // 2
    heads = head_rates.shape[0]
    line = lax.broadcasted_iota(jnp.int32, (8, feat), 0)
    gains = jnp.where(line == 0, mix_gain[None], jnp.where(line == 1, ffn_gain[None], final_gain[None])).astype(F32)
    gains = jnp.where(line == 3, block_scale[0], jnp.where(line == 4, block_scale[1], gains))
    cosine, sine = tables(rows)
    cw = out_weight.shape[1]
    hbm = pl.BlockSpec(memory_space=pl.ANY)
    smem = pl.BlockSpec(memory_space=pltpu.SMEM)
    vmem = pl.BlockSpec(memory_space=pltpu.VMEM)
    dma = pltpu.SemaphoreType.DMA
    return pl.pallas_call(
        layer_kernel,
        out_shape=jax.ShapeDtypeStruct((rows, feat), BF16),
        in_specs=[hbm] * 7 + [smem] + [hbm] * 3 + [vmem] * 2,
        out_specs=vmem,
        scratch_shapes=[
            pltpu.VMEM((2, 2, rows, feat), BF16),
            pltpu.VMEM((2, 8, feat), F32),
            pltpu.VMEM((8, 128), F32),
            pltpu.VMEM((query_weight.shape[0], joint), BF16),
            pltpu.VMEM((width, joint), BF16),
            pltpu.VMEM((chips, out_weight.shape[0], 2 * cw), BF16),
            pltpu.VMEM((width, half_ff), BF16),
            pltpu.VMEM((width, half_ff), BF16),
            pltpu.VMEM((chips, half_ff, 2 * cw), BF16),
            pltpu.VMEM((2 * rows, joint), F32),
            pltpu.VMEM((rows, heads * DV // 2), BF16),
            pltpu.VMEM((2, rows, heads * DV // 2), BF16),
            pltpu.VMEM((feat // WIDE, rows, WIDE), BF16),
            pltpu.VMEM((feat // WIDE, rows, WIDE), BF16),
            pltpu.VMEM((feat // WIDE, rows, WIDE), BF16),
            pltpu.VMEM((2, 2, rows, feat), BF16),
            pltpu.VMEM((2 * rows, width), BF16),
            pltpu.VMEM((2 * rows, half_ff), F32),
            pltpu.VMEM((2 * rows, half_ff), F32),
            pltpu.VMEM((2 * rows, half_ff), BF16),
            pltpu.VMEM((4, 2 * rows, WIDE), BF16),
            pltpu.VMEM((4, 2 * rows, WIDE), BF16),
            pltpu.VMEM((4, 2 * rows, WIDE), F32),
            pltpu.VMEM((4, rows, WIDE), BF16),
            pltpu.VMEM((4, rows, WIDE), BF16),
            pltpu.VMEM((4, rows, WIDE), F32),
            pltpu.VMEM((8, rows), F32),
            pltpu.VMEM((8, rows), F32),
            dma((14,)),
            dma((72,)),
            dma((6, size)),
            dma((35,)),
        ],
        compiler_params=pltpu.CompilerParams(
            collective_id=0, has_side_effects=True, vmem_limit_bytes=60 * 2**20
        ),
    )(
        tokens,
        gains,
        query_weight,
        key_weight,
        value_weight,
        output_gate_weight,
        out_weight,
        head_rates,
        ff_gate,
        ff_up,
        ff_down,
        cosine,
        sine,
    )


def kernel_fits(mesh, tokens, query_weight, ff_gate, head_rates):
    size, parts = mesh.shape["fs"], mesh.shape["tp"]
    if size != 4 * 2 * 2 or parts != 2:
        return False
    rows, width = tokens.shape[0] // size, tokens.shape[1]
    return (
        rows == SEQ_LEN
        and SEQ_LEN == 2 * BLK
        and width // size * 2 == WIDE
        and ff_gate.shape[1] % (4 * 128) == 0
        and head_rates.shape[0] % (4 * parts) == 0
    )


def dispatch(mesh, *args):
    fits = kernel_fits(mesh, args[0], args[2], args[10], args[7])
    return jax.shard_map(
        fused if fits else body,
        mesh=mesh,
        in_specs=SPECS,
        out_specs=P("fs", "tp"),
        check_vma=False,
    )(*args)


SPECS = (
    P("fs", "tp"),
    P("tp"),
    P("fs", "tp"),
    P("fs", "tp"),
    P("fs", "tp"),
    P("fs", "tp"),
    P("tp", "fs"),
    P("tp"),
    P("fs"),
    P("tp"),
    P("fs", "tp"),
    P("fs", "tp"),
    P("tp", "fs"),
    P("tp"),
)


def solution(mesh):
    return functools.partial(dispatch, mesh)
```

```python
import functools

import jax
import jax.numpy as jnp
import numpy as np
from jax import lax
from jax.experimental import pallas as pl
from jax.experimental.pallas import tpu as pltpu
from jax.sharding import PartitionSpec as P

D = 2048
DK = 64
DV = 128
BLK = 128
SEQ_LEN = 256


EPS = 1e-06
THETA = 10000.0


def rms_norm(values, gain):
    scale = lax.rsqrt(jnp.mean(values * values, axis=-1, keepdims=True) + EPS)
    return values * scale * gain.astype(jnp.float32)


def rotate(values, positions):
    half = values.shape[-1] // 2
    inverse = THETA ** (-jnp.arange(half, dtype=jnp.float32) / half)
    angle = positions.astype(jnp.float32)[:, None] * inverse
    cosine = jnp.cos(angle)[:, None, :]
    sine = jnp.sin(angle)[:, None, :]
    first = values[..., :half]
    second = values[..., half:]
    return jnp.concatenate(
        [first * cosine - second * sine, second * cosine + first * sine], axis=-1
    )


def retain(query, key, value, rates, scales):
    rows, heads_here, width_k = query.shape
    width_v = value.shape[-1]
    nblk = rows // BLK
    hi = lax.Precision.HIGHEST
    qblk = query.astype(jnp.float32).reshape(nblk, BLK, heads_here, width_k)
    kblk = key.astype(jnp.float32).reshape(nblk, BLK, heads_here, width_k)
    vblk = value.astype(jnp.float32).reshape(nblk, BLK, heads_here, width_v)
    logdec = -rates[None, :] * scales[:, None]
    steps = jnp.arange(BLK, dtype=jnp.float32)
    offset = steps[:, None] - steps[None, :]
    causal = offset >= 0
    inside = jnp.where(
        causal[None, None],
        jnp.exp(logdec[:, :, None, None] * jnp.where(causal, offset, 0.0)[None, None]),
        0.0,
    )
    scores = jnp.einsum("nchd,nmhd->nhcm", qblk, kblk, precision=hi) * inside
    inner = jnp.einsum("nhcm,nmhe->nche", scores, vblk, precision=hi)
    zeta = jnp.exp(logdec[:, :, None] * (BLK - 1.0 - steps)[None, None, :])
    kv_block = jnp.einsum(
        "nchd,nche->nhde", kblk * jnp.transpose(zeta, (0, 2, 1))[..., None], vblk, precision=hi
    )
    hold = jnp.exp(logdec * BLK)
    per_seq = SEQ_LEN // BLK
    fresh = (jnp.arange(nblk, dtype=jnp.int32) % per_seq == 0).astype(jnp.float32)

    def advance(state, inputs):
        kv_now, hold_now, fresh_now = inputs
        before = state * (1.0 - fresh_now)
        return (before * hold_now[:, None, None] + kv_now, before)

    start = jnp.zeros((heads_here, width_k, width_v), jnp.float32)
    _, before = lax.scan(advance, start, (kv_block, hold, fresh), unroll=True)
    xi = jnp.exp(logdec[:, :, None] * (steps + 1.0)[None, None, :])
    cross = jnp.einsum(
        "nchd,nhde->nche", qblk * jnp.transpose(xi, (0, 2, 1))[..., None], before, precision=hi
    )
    total = inner + cross
    total = total * lax.rsqrt(jnp.mean(total * total, axis=-1, keepdims=True) + EPS)
    return total.reshape(rows, heads_here * width_v)


def chip_ring(size):
    chips = size // 2
    return list(range(0, chips, 2)) + list(range(1, chips, 2))[::-1]


def ring_place(size):
    ring = chip_ring(size)
    me = lax.axis_index("fs")
    chip = me // 2
    place = jnp.zeros((), jnp.int32)
    for index, member in enumerate(ring):
        place = jnp.where(chip == member, index, place)
    return place, me % 2


def after(value, *others):
    return lax.optimization_barrier((value,) + tuple(others))[0]


def circulate(block, axis, gates=()):
    size = lax.axis_size("fs")
    ring = chip_ring(size)
    chips = len(ring)
    onward = [
        (2 * ring[i] + core, 2 * ring[(i + 1) % chips] + core)
        for i in range(chips)
        for core in range(2)
    ]
    back = [(target, source) for source, target in onward]
    swap = [(i, i ^ 1) for i in range(size)]
    held = {0: block}
    reach = (chips - 1) // 2
    down = up = block
    for step in range(1, reach + 1):
        if len(gates) >= step and gates[step - 1]:
            down = after(down, *gates[step - 1])
            up = after(up, *gates[step - 1])
        down = lax.ppermute(down, "fs", onward)
        up = lax.ppermute(up, "fs", back)
        held[-step] = down
        held[step] = up
    if chips % 2 == 0 and chips > 1:
        cut = 1 - axis
        half = block.shape[cut] // 2
        if len(gates) > reach and gates[reach]:
            down = after(down, *gates[reach])
            up = after(up, *gates[reach])
        first = lax.ppermute(lax.slice_in_dim(down, 0, half, axis=cut), "fs", onward)
        second = lax.ppermute(lax.slice_in_dim(up, half, None, axis=cut), "fs", back)
        held[reach + 1] = jnp.concatenate([first, second], axis=cut)
    groups = []
    for offsets in order_of(size):
        own = jnp.concatenate([held[o] for o in offsets], axis=axis)
        groups.append((own, lax.ppermute(own, "fs", swap)))
    return held, groups


def order_of(size):
    chips = size // 2
    reach = (chips - 1) // 2
    groups = [list(range(-reach, reach + 1))]
    if chips > 1 and chips % 2 == 0:
        groups.append([reach + 1])
    return groups


def lane_of(values, lane, wide):
    count = values.shape[1] // (2 * wide)
    return [values[:, (2 * c + lane) * wide : (2 * c + lane + 1) * wide] for c in range(count)]


def to_ring(values, place, core):
    size = lax.axis_size("fs")
    wide = values.shape[1] // size
    ring = chip_ring(size)
    chips = len(ring)
    groups = order_of(size)
    start = (place + groups[0][0] + chips) % chips
    lanes = []
    for lane in range(2):
        pieces = lane_of(values, lane, wide)
        ringed = jnp.concatenate([pieces[c] for c in ring] * 2, axis=1)
        lanes.append(lax.dynamic_slice_in_dim(ringed, start * wide, chips * wide, axis=1))
    own = jnp.where(core == 0, lanes[0], lanes[1])
    other = jnp.where(core == 0, lanes[1], lanes[0])
    result, edge = [], 0
    for offsets in groups:
        end = edge + len(offsets) * wide
        result.append((own[:, edge:end], other[:, edge:end]))
        edge = end
    return result


def from_ring(groups, place, core):
    size = lax.axis_size("fs")
    ring = chip_ring(size)
    chips = len(ring)
    own = jnp.concatenate([own for own, _ in groups], axis=1)
    other = jnp.concatenate([other for _, other in groups], axis=1)
    wide = own.shape[1] // chips
    start = (2 * chips - place - order_of(size)[0][0]) % chips
    lanes = []
    for lane in range(2):
        straight = jnp.where(core == lane, own, other)
        doubled = jnp.concatenate([straight, straight], axis=1)
        lanes.append(lax.dynamic_slice_in_dim(doubled, start * wide, chips * wide, axis=1))
    spot = {c: i for i, c in enumerate(ring)}
    return jnp.concatenate(
        [
            lanes[lane][:, spot[c] * wide : (spot[c] + 1) * wide]
            for c in range(chips)
            for lane in range(2)
        ],
        axis=1,
    )


def tp_gather(values, axis):
    if lax.axis_size("tp") != 2:
        return lax.all_gather(values, "tp", axis=axis, tiled=True)
    other = lax.ppermute(values, "tp", [(0, 1), (1, 0)])
    mine = lax.axis_index("tp") == 0
    return jnp.concatenate(
        [jnp.where(mine, values, other), jnp.where(mine, other, values)], axis=axis
    )


def tp_sum(values):
    if lax.axis_size("tp") != 2:
        return lax.psum(values, "tp")
    return values + lax.ppermute(values, "tp", [(0, 1), (1, 0)])


def tp_scatter_sum(partial):
    if lax.axis_size("tp") != 2:
        pieces = lax.all_to_all(
            partial.reshape(partial.shape[0], lax.axis_size("tp"), -1), "tp", 1, 1
        )
        return jnp.sum(pieces.astype(jnp.float32), axis=1)
    half = partial.shape[1] // 2
    low = lax.axis_index("tp") == 0
    keep = jnp.where(low, partial[:, :half], partial[:, half:])
    send = jnp.where(low, partial[:, half:], partial[:, :half])
    got = lax.ppermute(send, "tp", [(0, 1), (1, 0)])
    return keep.astype(jnp.float32) + got.astype(jnp.float32)


def product_rows(left, groups, columns=slice(None), result=0.0):
    for pieces, blocks in zip(left, groups):
        for piece, block in zip(pieces, blocks):
            result = result + jnp.dot(
                piece, block[:, columns], preferred_element_type=jnp.float32
            )
    return result


def product_columns(left, groups, place, core, columns=None):
    terms = []
    for blocks in groups:
        pair = []
        for block in blocks:
            if columns is None:
                dims, right = (((1,), (0,)), ((), ())), block
            else:
                dims, right = (((1,), (1,)), ((), ())), block[:, columns]
            term = lax.dot_general(left, right, dims, preferred_element_type=jnp.float32)
            pair.append(term.astype(jnp.bfloat16))
        terms.append(pair)
    return from_ring(terms, place, core)


def body(
    tokens,
    mix_gain,
    query_weight,
    key_weight,
    value_weight,
    output_gate_weight,
    out_weight,
    head_rates,
    block_scale,
    ffn_gain,
    ff_gate,
    ff_up,
    ff_down,
    final_gain,
):
    rows = tokens.shape[0]
    heads_here = head_rates.shape[0]
    size = lax.axis_size("fs")
    place, core = ring_place(size)
    reach = (size // 2 - 1) // 2
    positions = jnp.arange(rows, dtype=jnp.int32) % SEQ_LEN

    bundle = jnp.concatenate(
        [query_weight, key_weight, value_weight, output_gate_weight, out_weight.T], axis=1
    )
    hops, proj = circulate(bundle, 0)
    last = (hops[-reach], hops[reach])

    whole = tp_gather(tokens, 1)
    gains = tp_gather(jnp.stack([mix_gain, ffn_gain]), 1)
    normed = rms_norm(whole.astype(jnp.float32), gains[0]).astype(jnp.bfloat16)
    width = bundle.shape[1] - out_weight.shape[0]
    projected = product_rows(to_ring(normed, place, core), proj, slice(0, width))
    ends = [query_weight.shape[1], key_weight.shape[1], value_weight.shape[1]]
    qproj, kproj, vproj, gproj = jnp.split(
        projected, [ends[0], ends[0] + ends[1], sum(ends)], axis=1
    )
    query = rotate(qproj.reshape(rows, heads_here, DK), positions).astype(jnp.bfloat16)
    key = (rotate(kproj.reshape(rows, heads_here, DK), positions) * DK ** (-0.5)).astype(
        jnp.bfloat16
    )
    value = vproj.astype(jnp.bfloat16).reshape(rows, heads_here, DV)
    normret = retain(query, key, value, head_rates, block_scale)
    gated = (normret * jax.nn.silu(gproj)).astype(jnp.bfloat16)
    opposite = tuple(hops[o] for o in order_of(size)[-1])
    gate_hops, gates = circulate(ff_gate, 0, ((), opposite, (projected,)))
    up_hops, ups = circulate(ff_up, 0, (last, (), (gated,)))
    mix = tp_scatter_sum(product_columns(gated, proj, place, core, slice(width, None)))
    resid = (tokens.astype(jnp.float32) + mix).astype(jnp.bfloat16)
    whole2 = tp_gather(resid, 1)
    normed2 = to_ring(
        rms_norm(whole2.astype(jnp.float32), gains[1]).astype(jnp.bfloat16), place, core
    )
    gate_part = product_rows(normed2[:1], gates[:1])
    up_part = product_rows(normed2[:1], ups[:1])
    early_parts = (gate_part, up_part)
    gate_part = product_rows(normed2[1:], gates[1:], result=gate_part)
    up_part = product_rows(normed2[1:], ups[1:], result=up_part)
    hidden = (jax.nn.silu(gate_part) * up_part).astype(jnp.bfloat16)
    near = (gate_hops[-reach], gate_hops[reach])
    far = order_of(size)[-1][-1]
    second = (normed2[0][0], up_hops[-reach], up_hops[reach])
    third = early_parts + (gate_hops[far], up_hops[far])
    _, downs = circulate(ff_down, 1, (near, second, third))
    ffn = tp_scatter_sum(product_columns(hidden, downs, place, core))
    total = resid.astype(jnp.float32) + ffn
    squares = tp_sum(jnp.sum(total * total, axis=-1))[:, None]
    scale = lax.rsqrt(squares / D + EPS)
    return (total * scale * final_gain.astype(jnp.float32)).astype(jnp.bfloat16)


MESH = pl.DeviceIdType.MESH
F32 = jnp.float32
BF16 = jnp.bfloat16
WIDE = 256


def silu(v):
    return v / (1.0 + jnp.exp(-v))


def mm(a, b):
    return jnp.dot(a, b, preferred_element_type=F32)


def layer_kernel(
    tok_h,
    mixg_h,
    ffng_h,
    lastg_h,
    q_h,
    k_h,
    v_h,
    g_h,
    o_h,
    rate_s,
    scale_s,
    fg_h,
    fu_h,
    fd_h,
    cos_h,
    sin_h,
    out_h,
    tok,
    gn,
    gl,
    gf,
    gs,
    gr,
    cos_ref,
    sin_ref,
    Ps,
    P,
    O,
    G,
    U,
    Dn,
    pr,
    gsend,
    gated,
    sm,
    pm,
    rm,
    R,
    N2,
    gacc,
    uacc,
    hid,
    sx,
    rx,
    pmine,
    sz,
    rz,
    tot,
    ss_s,
    ss_r,
    lsem,
    ssem,
    wsem,
    asem,
    osem,
):
    rows, feat = tok_h.shape
    width = 2 * feat
    rw = q_h.shape[0]
    cw = o_h.shape[1]
    half_ff = fg_h.shape[1] // 2
    heads = rate_s.shape[0]
    f = lax.axis_index("fs")
    x = lax.axis_index("tp")
    c = f % 2
    y = (f // 2) % 2
    z = f // 4
    b = z // 2
    zp = 4 * b + 1 - z
    zm = 3 - z
    near_o = 2 - b
    far_o = 3 * (1 - b)
    near = jnp.logical_or(z == 1, z == 2)
    far = jnp.logical_not(near)
    y1, c1, x1 = 1 - y, 1 - c, 1 - x

    def dev(zz, yy, cc, xx):
        return ((zz * 2 + yy) * 2 + cc, xx)

    here = x == b
    away = jnp.logical_not(here)
    roles = (None, near, far, here, away)
    pools = ((0, 28), (28, 36), (28, 36), (64, 8), (64, 8))
    sends = [[] for _ in roles]
    role = [0]

    def put(src, dst, sem, to):
        base, size = pools[role[0]]
        copies = sends[role[0]]
        index = base + len(copies) % size

        def copy():
            return pltpu.make_async_remote_copy(
                src_ref=src(),
                dst_ref=dst(),
                send_sem=ssem.at[index],
                recv_sem=sem(),
                device_id=to,
                device_id_type=MESH,
            )

        if len(copies) >= size:
            copies[len(copies) - size]().wait_send()
        copy().start()
        copies.append(copy)

    def only(who, *acts):
        @pl.when(who)
        def _():
            role[0] = [who is r for r in roles].index(True)
            for act, *args in acts:
                act(*args)
            role[0] = 0

    def got(ref, sem, name="got"):
        copy = pltpu.make_async_remote_copy(
            src_ref=ref,
            dst_ref=ref,
            send_sem=ssem.at[0],
            recv_sem=sem,
            device_id=dev(z, y, c1, x),
            device_id_type=MESH,
        )
        with jax.named_scope(name):
            copy.wait_recv()

    local = []

    def take(src, dst):
        copy = pltpu.make_async_copy(src, dst, lsem.at[len(local)])
        copy.start()
        local.append(copy)
        return copy

    def row_slot(buf):
        def slot(zz, yy, cc):
            start = pl.multiple_of(((zz * 2 + yy) * 2 + cc) * rw, rw)
            return buf.at[pl.ds(start, rw), :]

        return slot

    def col_slot(buf):
        def slot(zz, yy, cc):
            return buf.at[zz * 2 + yy, :, pl.ds(pl.multiple_of(cc * cw, cw), cw)]

        return slot

    deep = half_ff // 2

    def down_slot(k):
        def slot(zz, yy, cc):
            return Dn.at[zz * 2 + yy, pl.ds(k * deep, deep), pl.ds(pl.multiple_of(cc * cw, cw), cw)]

        return slot

    sP, sO, sG, sU = row_slot(P), col_slot(O), row_slot(G), row_slot(U)
    slots = (sP, sO, sG, sU, down_slot(0), down_slot(1))
    DOWN = (4, 5)

    def sem_of(kind, zz, yy, cc):
        return wsem.at[kind, (zz * 2 + yy) * 2 + cc]

    def fwd(kind, zz, yy, cc, to):
        ref = functools.partial(slots[kind], zz, yy, cc)
        put(ref, ref, functools.partial(sem_of, kind, zz, yy, cc), to)

    def arrive(kind, zz, yy, cc):
        side = "sib" if cc is c1 else "row" if yy is y1 else "col"
        got(slots[kind](zz, yy, cc), sem_of(kind, zz, yy, cc), f"{side}{kind}")

    sib = dev(z, y, c1, x)
    row = dev(z, y1, c, x)
    peer = dev(zp, y, c, x)
    xdev = dev(z, y, c, x1)
    mirror = dev(zm, y, c, x)

    parts = [ref.shape[1] // 2 for ref in (q_h, k_h, v_h, g_h)]
    ends = np.cumsum([0] + parts).tolist()
    mine = pl.multiple_of(((z * 2 + y) * 2 + c) * rw, rw)
    own_p, stage_p = [], []
    for i, ref in enumerate((q_h, k_h, v_h, g_h)):
        to = pl.ds(ends[i], parts[i])
        at = pl.ds(pl.multiple_of(y * parts[i], 128), parts[i])
        own_p.append(take(ref.at[:, at], P.at[pl.ds(mine, rw), to]))
        at = pl.ds(pl.multiple_of(y1 * parts[i], 128), parts[i])
        stage_p.append(take(ref.at[:, at], Ps.at[:, to]))
    own_o = take(o_h, sO(z, y, c))
    own_t = [take(tok_h, tok.at[0, x])] + [take(ref, gn.at[x, k]) for k, ref in enumerate((mixg_h, ffng_h))]
    own_t += [take(cos_h, cos_ref), take(sin_h, sin_ref), take(lastg_h, gl)]
    gs[...] = jnp.where(lax.broadcasted_iota(jnp.int32, gs.shape, 0) == 0, scale_s[0], scale_s[1])
    at_b = pl.multiple_of(b * half_ff, 128)
    at_o = pl.multiple_of((1 - b) * half_ff, 128)
    own_g = take(fg_h.at[:, pl.ds(at_b, half_ff)], sG(z, y, c))
    own_u = take(fu_h.at[:, pl.ds(at_b, half_ff)], sU(z, y, c))
    own_d = take(fd_h.at[pl.ds(at_b, half_ff), :], col_slot(Dn)(z, y, c))

    barrier = pltpu.get_barrier_semaphore()
    friends = [sib, row, xdev] + [dev((z + k) % 4, y, c, x) for k in (1, 2, 3)]
    for to in friends:
        pl.semaphore_signal(barrier, inc=1, device_id=to, device_id_type=MESH)
    pl.semaphore_wait(barrier, len(friends))

    put(lambda: tok_h, lambda: tok.at[0, x], lambda: asem.at[0], xdev)
    put(lambda: mixg_h, lambda: gn.at[x, 0], lambda: asem.at[1], xdev)
    put(lambda: ffng_h, lambda: gn.at[x, 1], lambda: asem.at[35], xdev)

    other = {
        2: lambda: fg_h.at[:, pl.ds(at_o, half_ff)],
        3: lambda: fu_h.at[:, pl.ds(at_o, half_ff)],
        4: lambda: fd_h.at[pl.ds(at_o, deep), :],
        5: lambda: fd_h.at[pl.ds(pl.multiple_of(at_o + deep, 16), deep), :],
    }
    beyond = dev(near_o, y, c, x)

    def own(kind, to):
        fwd(kind, z, y, c, to)

    def cross(kind):
        slot = functools.partial(slots[kind], z, y, c)
        put(other[kind], slot, functools.partial(sem_of, kind, z, y, c), beyond)

    def relay(kind, zz, *to):
        arrive(kind, zz, y, c)
        for device in to + (row, sib):
            fwd(kind, zz, y, c, device)

    def arrive_down(*place):
        for kind in DOWN:
            arrive(kind, *place)

    def down(act, *args):
        return [(act, kind) + args for kind in DOWN]

    def share(kind):
        for zz in (z, zp, near_o, far_o):
            arrive(kind, zz, y1, c)
            fwd(kind, zz, y1, c, sib)

    def line(zz, yy, *to):
        arrive(0, zz, yy, c)
        for device in to + (sib,):
            fwd(0, zz, yy, c, device)

    for copy in stage_p + own_p:
        copy.wait()
    put(lambda: Ps, lambda: sP(z, y, c), lambda: sem_of(0, z, y, c), row)
    own(0, peer)
    only(near, (own, 0, beyond))
    own(0, sib)
    put(lambda: tok_h, lambda: tok.at[1, x], lambda: asem.at[2], row)
    put(lambda: gs, lambda: gr, lambda: asem.at[3], row)
    own_o.wait()
    own(1, row)
    own(1, peer)
    only(near, (own, 1, beyond))
    own(1, sib)
    own_g.wait()
    own(2, row)
    own(2, sib)
    only(far, (line, z, y1, peer), (own, 2, peer), (line, zp, y), (relay, 1, zp), (line, zp, y1))
    only(
        near,
        (line, z, y1, peer, beyond),
        (line, zp, y, beyond),
        (line, near_o, y, peer),
        (relay, 1, zp, beyond),
        (relay, 1, near_o, peer),
        (line, zp, y1, beyond),
        (line, near_o, y1, peer),
    )

    for copy in own_t:
        copy.wait()
    got(tok.at[0, x1], asem.at[0], "tok")
    got(gn.at[x1, 0], asem.at[1])
    got(gn.at[x1, 1], asem.at[35])

    def norm_rows(first, second, gain_row, dst, base):
        chunk = 32
        gains = [gn[half, gain_row].astype(F32) for half in range(2)]

        @pl.loop(0, rows // chunk)
        def _(i):
            at = pl.ds(pl.multiple_of(i * chunk, chunk), chunk)
            one = first[at, :].astype(F32)
            two = second[at, :].astype(F32)
            total = jnp.sum(one * one, axis=1, keepdims=True) + jnp.sum(two * two, axis=1, keepdims=True)
            scale = lax.rsqrt(total / width + EPS)
            to = pl.ds(pl.multiple_of(base + i * chunk, chunk), chunk)
            for half, values in enumerate((one, two)):
                for k in range(feat // 128):
                    part = values[:, k * 128 : (k + 1) * 128] * scale * gains[half][k : k + 1, :]
                    dst[to, half * feat + k * 128 : half * feat + (k + 1) * 128] = part.astype(BF16)

    norm_rows(tok.at[0, 0], tok.at[0, 1], 0, N2, 0)
    got(tok.at[1, x], asem.at[2], "tok")
    put(lambda: tok.at[1, x], lambda: tok.at[1, x], lambda: asem.at[4], xdev)
    got(gr, asem.at[3])
    own_u.wait()
    own_d.wait()
    only(
        far,
        (line, near_o, y),
        (line, near_o, y1),
        (relay, 1, near_o),
        (cross, 2),
        (line, far_o, y),
        (line, far_o, y1),
        (relay, 1, far_o),
        (own, 3, peer),
        (cross, 3),
    )
    only(
        near,
        (line, far_o, y, peer),
        (line, far_o, y1, peer),
        (relay, 1, far_o, peer),
        (own, 2, peer),
        (cross, 2),
        (relay, 2, zp),
        (cross, 3),
    )
    got(tok.at[1, x1], asem.at[4], "tok")
    norm_rows(tok.at[1, 0], tok.at[1, 1], 0, N2, rows)
    for zz in range(4):
        for yy in range(2):
            arrive(0, zz, yy, c1)

    @pl.loop(0, P.shape[1] // WIDE)
    def _(j):
        at = pl.ds(pl.multiple_of(j * WIDE, WIDE), WIDE)
        pr[:, at] = mm(N2[...], P[:, at])

    blk = rows // 2
    t = lax.broadcasted_iota(jnp.int32, (rows, rows), 0)
    s = lax.broadcasted_iota(jnp.int32, (rows, rows), 1)
    late_t, late_s = t >= blk, s >= blk
    apart = (t - s).astype(F32)
    into = (t - (blk - 1)).astype(F32)
    left = ((blk - 1) - s).astype(F32)
    causal = t >= s
    lane = lax.broadcasted_iota(jnp.int32, (rows, 2 * DK), 1)
    early = (lane % DK) < DK // 2
    first_head = lane < DK

    def turn(v):
        swapped = jnp.where(early, pltpu.roll(v, 2 * DK - DK // 2, 1), pltpu.roll(v, DK // 2, 1))
        return v * cos_ref[...] + swapped * sin_ref[...]

    def retain_rows(at, scales, dst):
        s0, s1 = scales[0:1, 0:1], scales[1:2, 0:1]
        for two in range(heads // 4):
            cols = slice(ends[0] + two * 2 * DK, ends[0] + (two + 1) * 2 * DK)
            query = turn(pr[at, cols]).astype(BF16)
            cols = slice(ends[1] + two * 2 * DK, ends[1] + (two + 1) * 2 * DK)
            key = (turn(pr[at, cols]) * DK ** (-0.5)).astype(BF16)
            for side in range(2):
                h = 2 * two + side
                rate = rate_s[y * (heads // 2) + h]
                keep = first_head if side == 0 else jnp.logical_not(first_head)
                part = jnp.where(keep, query, jnp.zeros_like(query))
                scores = lax.dot_general(part, key, (((1,), (1,)), ((), ())), preferred_element_type=F32)
                la0, la1 = -(rate * s0), -(rate * s1)
                power = jnp.where(late_t, la1, la0) * apart
                power = jnp.where(jnp.logical_and(late_t, jnp.logical_not(late_s)), la1 * into + la0 * left, power)
                scores = scores * jnp.where(causal, jnp.exp(jnp.where(causal, power, 0.0)), 0.0)
                high = scores.astype(BF16)
                low = (scores - high.astype(F32)).astype(BF16)
                value = pr[at, ends[2] + h * DV : ends[2] + (h + 1) * DV].astype(BF16)
                ret = mm(high, value) + mm(low, value)
                ret = ret * lax.rsqrt(jnp.mean(ret * ret, axis=1, keepdims=True) + EPS)
                gate = pr[at, ends[3] + h * DV : ends[3] + (h + 1) * DV]
                dst[:, h * DV : (h + 1) * DV] = (ret * silu(gate)).astype(BF16)

    retain_rows(slice(rows, 2 * rows), gr, gsend)
    put(lambda: gsend, lambda: gated.at[y], lambda: asem.at[5], row)
    retain_rows(slice(0, rows), gs, gated.at[y])
    only(far, (relay, 2, zp), (own, 3, row), (own, 3, sib))
    only(near, (relay, 2, near_o, peer))
    share(1)
    for zz in range(4):
        for yy in range(2):
            arrive(1, zz, yy, c1)
    got(gated.at[y1], asem.at[5], "gated")

    per = feat // WIDE
    half_o = O.shape[1] // 2

    def out_block(side, j):
        weights = O.at[side * per + j]
        return mm(gated[0], weights[0:half_o, :]) + mm(gated[1], weights[half_o:, :])

    def send_mix(j):
        put(lambda: sm.at[j], lambda: rm.at[j], lambda: asem.at[6 + j], xdev)

    for j in range(per):
        sm[j] = out_block(x1, j).astype(BF16)
        send_mix(j)
    for j in range(per):
        pm[j] = out_block(x, j).astype(BF16)

    only(far, (relay, 2, near_o), *down(own, row), *down(own, sib))
    only(
        near,
        (relay, 2, far_o, peer),
        (own, 3, peer),
        (own, 3, row),
        (own, 3, sib),
        (relay, 3, zp),
    )

    def block(j):
        return pl.ds(j * WIDE, WIDE)

    def send_resid(j):
        put(lambda: R.at[0, x, :, block(j)], lambda: R.at[1, x, :, block(j)], lambda: asem.at[10 + j], mirror)
        put(lambda: R.at[0, x, :, block(j)], lambda: R.at[0, x, :, block(j)], lambda: asem.at[14 + j], xdev)

    def pass_resid(j):
        got(R.at[1, x, :, block(j)], asem.at[10 + j], "R1")
        put(lambda: R.at[1, x, :, block(j)], lambda: R.at[1, x, :, block(j)], lambda: asem.at[18 + j], xdev)

    for j in range(per):
        got(rm.at[j], asem.at[6 + j], "mix")
        mix = pm[j].astype(F32) + rm[j].astype(F32)
        R[0, x, :, block(j)] = (tok[0, x, :, block(j)].astype(F32) + mix).astype(BF16)
        send_resid(j)
    only(far, (relay, 2, far_o), *down(own, peer), (relay, 3, zp))
    only(near, (relay, 3, near_o, peer), (relay, 3, far_o, peer), *down(own, row), *down(own, sib))
    pass_resid(0)
    pass_resid(1)
    only(near, *down(cross), *down(own, peer))
    only(far, *down(cross), (relay, 3, near_o))
    pass_resid(2)
    pass_resid(3)
    only(near, *down(relay, zp))
    only(far, (relay, 3, far_o))
    share(2)
    for j in range(per):
        got(R.at[0, x1, :, block(j)], asem.at[14 + j], "R0x")
    norm_rows(R.at[0, 0], R.at[0, 1], 1, N2, 0)
    for j in range(per):
        got(R.at[1, x1, :, block(j)], asem.at[18 + j], "R1x")
    norm_rows(R.at[1, 0], R.at[1, 1], 1, N2, rows)

    theirs, ours = slice(rows, 2 * rows), slice(0, rows)

    def over_columns(act):
        whole = half_ff // WIDE

        @pl.loop(0, whole)
        def _(j):
            act(pl.ds(pl.multiple_of(j * WIDE, WIDE), WIDE))

        if half_ff % WIDE:
            act(pl.ds(whole * WIDE, half_ff % WIDE))

    def gate_columns(at):
        gacc[:, at] = silu(mm(N2[...], G[:, at]))

    def up_of(part, at, *chips):
        total = 0.0
        for zz, yy in chips:
            deep_at = pl.ds(pl.multiple_of((zz * 2 + yy) * 2 * rw, 2 * rw), 2 * rw)
            total = total + mm(N2[part, deep_at], U[deep_at, at])
        return total

    def up_columns(at):
        for part in (theirs, ours):
            uacc[part, at] = up_of(
                part, at, (z, y), (zp, y), (near_o, y), (far_o, y), (z, y1), (zp, y1), (near_o, y1)
            )

    def hidden_columns(at):
        for part in (theirs, ours):
            up = uacc[part, at] + up_of(part, at, (far_o, y1))
            hid[part, at] = (gacc[part, at] * up).astype(BF16)

    for zz in range(4):
        for yy in range(2):
            arrive(2, zz, yy, c1)
    over_columns(gate_columns)
    only(near, *down(relay, near_o, peer))
    only(far, *down(relay, zp))
    for zz in (z, zp, near_o, far_o):
        arrive(3, zz, y, c1)
    for zz in (z, zp, near_o):
        arrive(3, zz, y1, c)
        fwd(3, zz, y1, c, sib)
    for zz in (z, zp, near_o):
        arrive(3, zz, y1, c1)
    over_columns(up_columns)
    arrive(3, far_o, y1, c)
    fwd(3, far_o, y1, c, sib)
    only(near, *down(relay, far_o, peer))
    only(far, *down(relay, near_o))
    arrive(3, far_o, y1, c1)
    over_columns(hidden_columns)

    at_end = far.astype(jnp.int32)

    def chip(half, i):
        return jnp.where(i % 2 == 1, 3 * half, 1 + half), jnp.where(i >= 2, y1, y)

    def columns(i):
        zz, yy = chip(x, i)
        return pl.ds(pl.multiple_of(((zz - 2 * x) * 2 + yy) * WIDE, WIDE), WIDE)

    def send_x(i, k, start):
        at = pl.ds(start, rows)
        put(lambda: sx.at[i, at, :], lambda: rx.at[i, at, :], lambda: asem.at[22 + 2 * i + k], xdev)

    def give(zz, yy, i, part):
        sx[i, part, :] = mm(hid[part, :], Dn[zz * 2 + yy]).astype(BF16)
        send_x(i, 0 if part is theirs else 1, part.start)

    def keep(zz, yy, i):
        pmine[i] = mm(hid[...], Dn[zz * 2 + yy])

    def ready(zz):
        for kind in DOWN:
            arrive(kind, zz, y1, c)
            fwd(kind, zz, y1, c, sib)

    def combine(i):
        got(rx.at[i, pl.ds(rows, rows), :], asem.at[22 + 2 * i], "rx")
        sz[i] = (pmine[i, theirs, :] + rx[i, theirs, :].astype(F32)).astype(BF16)
        put(lambda: sz.at[i], lambda: rz.at[i], lambda: asem.at[30 + i], mirror)

    def add(i):
        got(rx.at[i, pl.ds(0, rows), :], asem.at[23 + 2 * i], "rx")
        resid = R[0, x, :, columns(i)].astype(F32)
        tot[i] = resid + (pmine[i, ours, :] + rx[i, ours, :].astype(F32))

    def out_copy(i):
        return pltpu.make_async_copy(tot.at[i], out_h.at[:, columns(i)], osem.at[i])

    def close(i):
        got(rz.at[i], asem.at[30 + i], "rz")
        now = tot[i] + rz[i].astype(F32)
        tot[i] = now
        square = now * now
        return square[:, : WIDE // 2] + square[:, WIDE // 2 :]

    first = (at_end, 1 - at_end, 2 + at_end, 3 - at_end)
    order = [jnp.where(here, i, k) for k, i in enumerate(first)]
    b0, b1, b2, b3 = first
    arrive_down(z, y, c1)
    arrive_down(zp, y, c1)
    arrive_down(near_o, y, c1)
    only(away, (give, z, y, b0, theirs), (give, zp, y, b1, theirs))
    only(here, (give, near_o, y, 0, theirs), (keep, z, y, b0))
    only(far, *down(relay, far_o))
    arrive_down(far_o, y, c1)
    ready(z)
    ready(zp)
    only(here, (give, far_o, y, 1, theirs), (keep, zp, y, b1), (give, near_o, y, 0, ours), (give, far_o, y, 1, ours))
    arrive_down(z, y1, c1)
    arrive_down(zp, y1, c1)
    only(away, (give, z, y1, b2, theirs), (give, zp, y1, b3, theirs), (keep, near_o, y, 0), (keep, far_o, y, 1))
    combine(order[0])
    only(away, (give, z, y, b0, ours), (give, zp, y, b1, ours))
    combine(order[1])
    ready(near_o)
    only(away, (give, z, y1, b2, ours), (give, zp, y1, b3, ours))
    only(here, (keep, z, y1, b2), (keep, zp, y1, b3))
    arrive_down(near_o, y1, c1)
    only(here, (give, near_o, y1, 2, theirs), (give, near_o, y1, 2, ours))
    only(away, (keep, near_o, y1, 2))
    combine(order[2])
    ready(far_o)
    arrive_down(far_o, y1, c1)
    only(here, (give, far_o, y1, 3, theirs), (give, far_o, y1, 3, ours))
    only(away, (keep, far_o, y1, 3))
    add(order[0])
    add(order[1])
    squares = close(order[0])
    combine(order[3])
    squares = squares + close(order[1])
    add(order[2])
    add(order[3])
    squares = squares + close(order[2])
    squares = squares + close(order[3])
    mine_sq = jnp.broadcast_to(jnp.sum(squares, axis=1, keepdims=True), (rows, 128))
    ss_s[...] = mine_sq.T[0:8, :]
    put(lambda: ss_s, lambda: ss_r, lambda: asem.at[34], xdev)
    for who, (_, size), copies in zip(roles, pools, sends):

        def drain(copies=copies[-size:]):
            for copy in copies:
                copy().wait_send()

        drain() if who is None else pl.when(who)(drain)

    gf[...] = gl[...].astype(F32)
    got(ss_r, asem.at[34], "ss")
    total = ss_s[0:1, :] + ss_r[0:1, :]
    total = jnp.broadcast_to(total, (128, rows)).T[:, 0:1]
    scale = lax.rsqrt(total / width + EPS)
    for i in range(4):
        zz, yy = chip(x, i)
        for k in range(WIDE // 128):
            gain = gf[pl.ds(((zz - 2 * x) * 2 + yy) * (WIDE // 128) + k, 1), :]
            lanes = slice(k * 128, (k + 1) * 128)
            tot[i, :, lanes] = tot[i, :, lanes] * scale * gain
        out_copy(i).start()
    for i in range(4):
        out_copy(i).wait()


def tables(rows):
    half = DK // 2
    inverse = np.float32(THETA) ** (-np.arange(half, dtype=np.float32) / np.float32(half))
    angle = (np.arange(rows, dtype=np.float32) % SEQ_LEN)[:, None] * inverse
    cosine, sine = np.cos(angle), np.sin(angle)
    return (
        np.concatenate([cosine] * 4, axis=1).astype(np.float32),
        np.concatenate([-sine, sine, -sine, sine], axis=1).astype(np.float32),
    )


def fused(
    tokens,
    mix_gain,
    query_weight,
    key_weight,
    value_weight,
    output_gate_weight,
    out_weight,
    head_rates,
    block_scale,
    ffn_gain,
    ff_gate,
    ff_up,
    ff_down,
    final_gain,
):
    rows, feat = tokens.shape
    size = lax.axis_size("fs")
    chips = size // 2
    width = 2 * feat
    half_ff = ff_gate.shape[1] // 2
    joint = sum(w.shape[1] for w in (query_weight, key_weight, value_weight, output_gate_weight)) // 2
    heads = head_rates.shape[0]
    cosine, sine = tables(rows)
    cw = out_weight.shape[1]
    hbm = pl.BlockSpec(memory_space=pl.ANY)
    smem = pl.BlockSpec(memory_space=pltpu.SMEM)
    dma = pltpu.SemaphoreType.DMA
    out = pl.pallas_call(
        layer_kernel,
        out_shape=jax.ShapeDtypeStruct((rows, feat), F32),
        in_specs=[hbm] * 9 + [smem] * 2 + [hbm] * 5,
        out_specs=hbm,
        scratch_shapes=[
            pltpu.VMEM((2, 2, rows, feat), BF16),
            pltpu.VMEM((2, 2, feat // 128, 128), BF16),
            pltpu.VMEM((feat // 128, 128), BF16),
            pltpu.VMEM((feat // 128, 128), F32),
            pltpu.VMEM((8, 128), F32),
            pltpu.VMEM((8, 128), F32),
            pltpu.VMEM((rows, 128), F32),
            pltpu.VMEM((rows, 128), F32),
            pltpu.VMEM((query_weight.shape[0], joint), BF16),
            pltpu.VMEM((width, joint), BF16),
            pltpu.VMEM((chips, out_weight.shape[0], 2 * cw), BF16),
            pltpu.VMEM((width, half_ff), BF16),
            pltpu.VMEM((width, half_ff), BF16),
            pltpu.VMEM((chips, half_ff, 2 * cw), BF16),
            pltpu.VMEM((2 * rows, joint), F32),
            pltpu.VMEM((rows, heads * DV // 2), BF16),
            pltpu.VMEM((2, rows, heads * DV // 2), BF16),
            pltpu.VMEM((feat // WIDE, rows, WIDE), BF16),
            pltpu.VMEM((feat // WIDE, rows, WIDE), BF16),
            pltpu.VMEM((feat // WIDE, rows, WIDE), BF16),
            pltpu.VMEM((2, 2, rows, feat), BF16),
            pltpu.VMEM((2 * rows, width), BF16),
            pltpu.VMEM((2 * rows, half_ff), F32),
            pltpu.VMEM((2 * rows, half_ff), F32),
            pltpu.VMEM((2 * rows, half_ff), BF16),
            pltpu.VMEM((4, 2 * rows, WIDE), BF16),
            pltpu.VMEM((4, 2 * rows, WIDE), BF16),
            pltpu.VMEM((4, 2 * rows, WIDE), F32),
            pltpu.VMEM((4, rows, WIDE), BF16),
            pltpu.VMEM((4, rows, WIDE), BF16),
            pltpu.VMEM((4, rows, WIDE), F32),
            pltpu.VMEM((8, rows), F32),
            pltpu.VMEM((8, rows), F32),
            dma((18,)),
            dma((72,)),
            dma((6, size)),
            dma((36,)),
            dma((4,)),
        ],
        compiler_params=pltpu.CompilerParams(
            collective_id=0, has_side_effects=True, vmem_limit_bytes=60 * 2**20
        ),
    )(
        tokens,
        mix_gain.reshape(feat // 128, 128),
        ffn_gain.reshape(feat // 128, 128),
        final_gain.reshape(feat // 128, 128),
        query_weight,
        key_weight,
        value_weight,
        output_gate_weight,
        out_weight,
        head_rates,
        block_scale,
        ff_gate,
        ff_up,
        ff_down,
        cosine,
        sine,
    )
    return out.astype(BF16)


def kernel_fits(mesh, tokens, query_weight, ff_gate, head_rates):
    size, parts = mesh.shape["fs"], mesh.shape["tp"]
    if size != 4 * 2 * 2 or parts != 2:
        return False
    rows, width = tokens.shape[0] // size, tokens.shape[1]
    return (
        rows == SEQ_LEN
        and SEQ_LEN == 2 * BLK
        and width // size * 2 == WIDE
        and ff_gate.shape[1] % (4 * 128) == 0
        and head_rates.shape[0] % (4 * parts) == 0
    )


def dispatch(mesh, *args):
    fits = kernel_fits(mesh, args[0], args[2], args[10], args[7])
    return jax.shard_map(
        fused if fits else body,
        mesh=mesh,
        in_specs=SPECS,
        out_specs=P("fs", "tp"),
        check_vma=False,
    )(*args)


SPECS = (
    P("fs", "tp"),
    P("tp"),
    P("fs", "tp"),
    P("fs", "tp"),
    P("fs", "tp"),
    P("fs", "tp"),
    P("tp", "fs"),
    P("tp"),
    P("fs"),
    P("tp"),
    P("fs", "tp"),
    P("fs", "tp"),
    P("tp", "fs"),
    P("tp"),
)


def solution(mesh):
    return functools.partial(dispatch, mesh)
```

```python
import functools

import jax
import jax.numpy as jnp
import numpy as np
from jax import lax
from jax.experimental import pallas as pl
from jax.experimental.pallas import tpu as pltpu
from jax.sharding import PartitionSpec as P

D = 2048
DK = 64
DV = 128
BLK = 128
SEQ_LEN = 256


EPS = 1e-06
THETA = 10000.0


def rms_norm(values, gain):
    scale = lax.rsqrt(jnp.mean(values * values, axis=-1, keepdims=True) + EPS)
    return values * scale * gain.astype(jnp.float32)


def rotate(values, positions):
    half = values.shape[-1] // 2
    inverse = THETA ** (-jnp.arange(half, dtype=jnp.float32) / half)
    angle = positions.astype(jnp.float32)[:, None] * inverse
    cosine = jnp.cos(angle)[:, None, :]
    sine = jnp.sin(angle)[:, None, :]
    first = values[..., :half]
    second = values[..., half:]
    return jnp.concatenate(
        [first * cosine - second * sine, second * cosine + first * sine], axis=-1
    )


def retain(query, key, value, rates, scales):
    rows, heads_here, width_k = query.shape
    width_v = value.shape[-1]
    nblk = rows // BLK
    hi = lax.Precision.HIGHEST
    qblk = query.astype(jnp.float32).reshape(nblk, BLK, heads_here, width_k)
    kblk = key.astype(jnp.float32).reshape(nblk, BLK, heads_here, width_k)
    vblk = value.astype(jnp.float32).reshape(nblk, BLK, heads_here, width_v)
    logdec = -rates[None, :] * scales[:, None]
    steps = jnp.arange(BLK, dtype=jnp.float32)
    offset = steps[:, None] - steps[None, :]
    causal = offset >= 0
    inside = jnp.where(
        causal[None, None],
        jnp.exp(logdec[:, :, None, None] * jnp.where(causal, offset, 0.0)[None, None]),
        0.0,
    )
    scores = jnp.einsum("nchd,nmhd->nhcm", qblk, kblk, precision=hi) * inside
    inner = jnp.einsum("nhcm,nmhe->nche", scores, vblk, precision=hi)
    zeta = jnp.exp(logdec[:, :, None] * (BLK - 1.0 - steps)[None, None, :])
    kv_block = jnp.einsum(
        "nchd,nche->nhde", kblk * jnp.transpose(zeta, (0, 2, 1))[..., None], vblk, precision=hi
    )
    hold = jnp.exp(logdec * BLK)
    per_seq = SEQ_LEN // BLK
    fresh = (jnp.arange(nblk, dtype=jnp.int32) % per_seq == 0).astype(jnp.float32)

    def advance(state, inputs):
        kv_now, hold_now, fresh_now = inputs
        before = state * (1.0 - fresh_now)
        return (before * hold_now[:, None, None] + kv_now, before)

    start = jnp.zeros((heads_here, width_k, width_v), jnp.float32)
    _, before = lax.scan(advance, start, (kv_block, hold, fresh), unroll=True)
    xi = jnp.exp(logdec[:, :, None] * (steps + 1.0)[None, None, :])
    cross = jnp.einsum(
        "nchd,nhde->nche", qblk * jnp.transpose(xi, (0, 2, 1))[..., None], before, precision=hi
    )
    total = inner + cross
    total = total * lax.rsqrt(jnp.mean(total * total, axis=-1, keepdims=True) + EPS)
    return total.reshape(rows, heads_here * width_v)


def chip_ring(size):
    chips = size // 2
    return list(range(0, chips, 2)) + list(range(1, chips, 2))[::-1]


def ring_place(size):
    ring = chip_ring(size)
    me = lax.axis_index("fs")
    chip = me // 2
    place = jnp.zeros((), jnp.int32)
    for index, member in enumerate(ring):
        place = jnp.where(chip == member, index, place)
    return place, me % 2


def after(value, *others):
    return lax.optimization_barrier((value,) + tuple(others))[0]


def circulate(block, axis, gates=()):
    size = lax.axis_size("fs")
    ring = chip_ring(size)
    chips = len(ring)
    onward = [
        (2 * ring[i] + core, 2 * ring[(i + 1) % chips] + core)
        for i in range(chips)
        for core in range(2)
    ]
    back = [(target, source) for source, target in onward]
    swap = [(i, i ^ 1) for i in range(size)]
    held = {0: block}
    reach = (chips - 1) // 2
    down = up = block
    for step in range(1, reach + 1):
        if len(gates) >= step and gates[step - 1]:
            down = after(down, *gates[step - 1])
            up = after(up, *gates[step - 1])
        down = lax.ppermute(down, "fs", onward)
        up = lax.ppermute(up, "fs", back)
        held[-step] = down
        held[step] = up
    if chips % 2 == 0 and chips > 1:
        cut = 1 - axis
        half = block.shape[cut] // 2
        if len(gates) > reach and gates[reach]:
            down = after(down, *gates[reach])
            up = after(up, *gates[reach])
        first = lax.ppermute(lax.slice_in_dim(down, 0, half, axis=cut), "fs", onward)
        second = lax.ppermute(lax.slice_in_dim(up, half, None, axis=cut), "fs", back)
        held[reach + 1] = jnp.concatenate([first, second], axis=cut)
    groups = []
    for offsets in order_of(size):
        own = jnp.concatenate([held[o] for o in offsets], axis=axis)
        groups.append((own, lax.ppermute(own, "fs", swap)))
    return held, groups


def order_of(size):
    chips = size // 2
    reach = (chips - 1) // 2
    groups = [list(range(-reach, reach + 1))]
    if chips > 1 and chips % 2 == 0:
        groups.append([reach + 1])
    return groups


def lane_of(values, lane, wide):
    count = values.shape[1] // (2 * wide)
    return [values[:, (2 * c + lane) * wide : (2 * c + lane + 1) * wide] for c in range(count)]


def to_ring(values, place, core):
    size = lax.axis_size("fs")
    wide = values.shape[1] // size
    ring = chip_ring(size)
    chips = len(ring)
    groups = order_of(size)
    start = (place + groups[0][0] + chips) % chips
    lanes = []
    for lane in range(2):
        pieces = lane_of(values, lane, wide)
        ringed = jnp.concatenate([pieces[c] for c in ring] * 2, axis=1)
        lanes.append(lax.dynamic_slice_in_dim(ringed, start * wide, chips * wide, axis=1))
    own = jnp.where(core == 0, lanes[0], lanes[1])
    other = jnp.where(core == 0, lanes[1], lanes[0])
    result, edge = [], 0
    for offsets in groups:
        end = edge + len(offsets) * wide
        result.append((own[:, edge:end], other[:, edge:end]))
        edge = end
    return result


def from_ring(groups, place, core):
    size = lax.axis_size("fs")
    ring = chip_ring(size)
    chips = len(ring)
    own = jnp.concatenate([own for own, _ in groups], axis=1)
    other = jnp.concatenate([other for _, other in groups], axis=1)
    wide = own.shape[1] // chips
    start = (2 * chips - place - order_of(size)[0][0]) % chips
    lanes = []
    for lane in range(2):
        straight = jnp.where(core == lane, own, other)
        doubled = jnp.concatenate([straight, straight], axis=1)
        lanes.append(lax.dynamic_slice_in_dim(doubled, start * wide, chips * wide, axis=1))
    spot = {c: i for i, c in enumerate(ring)}
    return jnp.concatenate(
        [
            lanes[lane][:, spot[c] * wide : (spot[c] + 1) * wide]
            for c in range(chips)
            for lane in range(2)
        ],
        axis=1,
    )


def tp_gather(values, axis):
    if lax.axis_size("tp") != 2:
        return lax.all_gather(values, "tp", axis=axis, tiled=True)
    other = lax.ppermute(values, "tp", [(0, 1), (1, 0)])
    mine = lax.axis_index("tp") == 0
    return jnp.concatenate(
        [jnp.where(mine, values, other), jnp.where(mine, other, values)], axis=axis
    )


def tp_sum(values):
    if lax.axis_size("tp") != 2:
        return lax.psum(values, "tp")
    return values + lax.ppermute(values, "tp", [(0, 1), (1, 0)])


def tp_scatter_sum(partial):
    if lax.axis_size("tp") != 2:
        pieces = lax.all_to_all(
            partial.reshape(partial.shape[0], lax.axis_size("tp"), -1), "tp", 1, 1
        )
        return jnp.sum(pieces.astype(jnp.float32), axis=1)
    half = partial.shape[1] // 2
    low = lax.axis_index("tp") == 0
    keep = jnp.where(low, partial[:, :half], partial[:, half:])
    send = jnp.where(low, partial[:, half:], partial[:, :half])
    got = lax.ppermute(send, "tp", [(0, 1), (1, 0)])
    return keep.astype(jnp.float32) + got.astype(jnp.float32)


def product_rows(left, groups, columns=slice(None), result=0.0):
    for pieces, blocks in zip(left, groups):
        for piece, block in zip(pieces, blocks):
            result = result + jnp.dot(
                piece, block[:, columns], preferred_element_type=jnp.float32
            )
    return result


def product_columns(left, groups, place, core, columns=None):
    terms = []
    for blocks in groups:
        pair = []
        for block in blocks:
            if columns is None:
                dims, right = (((1,), (0,)), ((), ())), block
            else:
                dims, right = (((1,), (1,)), ((), ())), block[:, columns]
            term = lax.dot_general(left, right, dims, preferred_element_type=jnp.float32)
            pair.append(term.astype(jnp.bfloat16))
        terms.append(pair)
    return from_ring(terms, place, core)


def body(
    tokens,
    mix_gain,
    query_weight,
    key_weight,
    value_weight,
    output_gate_weight,
    out_weight,
    head_rates,
    block_scale,
    ffn_gain,
    ff_gate,
    ff_up,
    ff_down,
    final_gain,
):
    rows = tokens.shape[0]
    heads_here = head_rates.shape[0]
    size = lax.axis_size("fs")
    place, core = ring_place(size)
    reach = (size // 2 - 1) // 2
    positions = jnp.arange(rows, dtype=jnp.int32) % SEQ_LEN

    bundle = jnp.concatenate(
        [query_weight, key_weight, value_weight, output_gate_weight, out_weight.T], axis=1
    )
    hops, proj = circulate(bundle, 0)
    last = (hops[-reach], hops[reach])

    whole = tp_gather(tokens, 1)
    gains = tp_gather(jnp.stack([mix_gain, ffn_gain]), 1)
    normed = rms_norm(whole.astype(jnp.float32), gains[0]).astype(jnp.bfloat16)
    width = bundle.shape[1] - out_weight.shape[0]
    projected = product_rows(to_ring(normed, place, core), proj, slice(0, width))
    ends = [query_weight.shape[1], key_weight.shape[1], value_weight.shape[1]]
    qproj, kproj, vproj, gproj = jnp.split(
        projected, [ends[0], ends[0] + ends[1], sum(ends)], axis=1
    )
    query = rotate(qproj.reshape(rows, heads_here, DK), positions).astype(jnp.bfloat16)
    key = (rotate(kproj.reshape(rows, heads_here, DK), positions) * DK ** (-0.5)).astype(
        jnp.bfloat16
    )
    value = vproj.astype(jnp.bfloat16).reshape(rows, heads_here, DV)
    normret = retain(query, key, value, head_rates, block_scale)
    gated = (normret * jax.nn.silu(gproj)).astype(jnp.bfloat16)
    opposite = tuple(hops[o] for o in order_of(size)[-1])
    gate_hops, gates = circulate(ff_gate, 0, ((), opposite, (projected,)))
    up_hops, ups = circulate(ff_up, 0, (last, (), (gated,)))
    mix = tp_scatter_sum(product_columns(gated, proj, place, core, slice(width, None)))
    resid = (tokens.astype(jnp.float32) + mix).astype(jnp.bfloat16)
    whole2 = tp_gather(resid, 1)
    normed2 = to_ring(
        rms_norm(whole2.astype(jnp.float32), gains[1]).astype(jnp.bfloat16), place, core
    )
    gate_part = product_rows(normed2[:1], gates[:1])
    up_part = product_rows(normed2[:1], ups[:1])
    early_parts = (gate_part, up_part)
    gate_part = product_rows(normed2[1:], gates[1:], result=gate_part)
    up_part = product_rows(normed2[1:], ups[1:], result=up_part)
    hidden = (jax.nn.silu(gate_part) * up_part).astype(jnp.bfloat16)
    near = (gate_hops[-reach], gate_hops[reach])
    far = order_of(size)[-1][-1]
    second = (normed2[0][0], up_hops[-reach], up_hops[reach])
    third = early_parts + (gate_hops[far], up_hops[far])
    _, downs = circulate(ff_down, 1, (near, second, third))
    ffn = tp_scatter_sum(product_columns(hidden, downs, place, core))
    total = resid.astype(jnp.float32) + ffn
    squares = tp_sum(jnp.sum(total * total, axis=-1))[:, None]
    scale = lax.rsqrt(squares / D + EPS)
    return (total * scale * final_gain.astype(jnp.float32)).astype(jnp.bfloat16)


MESH = pl.DeviceIdType.MESH
F32 = jnp.float32
BF16 = jnp.bfloat16
WIDE = 256


def silu(v):
    return v / (1.0 + jnp.exp(-v))


def mm(a, b):
    return jnp.dot(a, b, preferred_element_type=F32)


def layer_kernel(
    tok_h,
    mixg_h,
    ffng_h,
    lastg_h,
    q_h,
    k_h,
    v_h,
    g_h,
    o_h,
    rate_s,
    scale_s,
    fg_h,
    fu_h,
    fd_h,
    cos_h,
    sin_h,
    out_h,
    tok,
    gn,
    gl,
    gf,
    gs,
    gr,
    cos_ref,
    sin_ref,
    Ps,
    P,
    O,
    G,
    U,
    Dn,
    pr,
    gsend,
    gated,
    sm,
    pm,
    rm,
    R,
    N2,
    gacc,
    uacc,
    hid,
    sx,
    rx,
    pmine,
    sz,
    rz,
    rd,
    tot,
    ss_s,
    ss_r,
    lsem,
    ssem,
    wsem,
    asem,
    osem,
):
    rows, feat = tok_h.shape
    width = 2 * feat
    rw = q_h.shape[0]
    cw = o_h.shape[1]
    half_ff = fg_h.shape[1] // 2
    heads = rate_s.shape[0]
    f = lax.axis_index("fs")
    x = lax.axis_index("tp")
    c = f % 2
    y = (f // 2) % 2
    z = f // 4
    b = z // 2
    zp = 4 * b + 1 - z
    zm = 3 - z
    near_o = 2 - b
    far_o = 3 * (1 - b)
    near = jnp.logical_or(z == 1, z == 2)
    far = jnp.logical_not(near)
    y1, c1, x1 = 1 - y, 1 - c, 1 - x

    def dev(zz, yy, cc, xx):
        return ((zz * 2 + yy) * 2 + cc, xx)

    here = x == b
    away = jnp.logical_not(here)
    end_here, end_away = jnp.logical_and(far, here), jnp.logical_and(far, away)
    mid_here, mid_away = jnp.logical_and(near, here), jnp.logical_and(near, away)
    roles = (None, near, far, here, away, end_here, end_away, mid_here, mid_away)
    pools = ((0, 28), (28, 36), (28, 36), (64, 8), (64, 8), (72, 1), (72, 1), (72, 1), (72, 1))
    sends = [[] for _ in roles]
    drained = [0 for _ in roles]
    role = [0]

    def put(src, dst, sem, to):
        base, size = pools[role[0]]
        copies = sends[role[0]]
        index = base + len(copies) % size

        def copy():
            return pltpu.make_async_remote_copy(
                src_ref=src(),
                dst_ref=dst(),
                send_sem=ssem.at[index],
                recv_sem=sem(),
                device_id=to,
                device_id_type=MESH,
            )

        if len(copies) - size >= drained[role[0]]:
            copies[len(copies) - size]().wait_send()
        copy().start()
        copies.append(copy)

    def drain(*which):
        for k, who in enumerate(roles):
            if which and not any(who is w for w in which):
                continue
            size = pools[k][1]
            copies = sends[k][max(drained[k], len(sends[k]) - size) :]

            def wait(copies=copies):
                for copy in copies:
                    copy().wait_send()

            if copies:
                wait() if who is None else pl.when(who)(wait)
            drained[k] = len(sends[k])

    def only(who, *acts):
        @pl.when(who)
        def _():
            role[0] = [who is r for r in roles].index(True)
            for act, *args in acts:
                act(*args)
            role[0] = 0

    def got(ref, sem, name="got"):
        copy = pltpu.make_async_remote_copy(
            src_ref=ref,
            dst_ref=ref,
            send_sem=ssem.at[0],
            recv_sem=sem,
            device_id=dev(z, y, c1, x),
            device_id_type=MESH,
        )
        with jax.named_scope(name):
            copy.wait_recv()

    local = []

    def take(src, dst):
        copy = pltpu.make_async_copy(src, dst, lsem.at[len(local)])
        copy.start()
        local.append(copy)
        return copy

    def row_slot(buf):
        def slot(zz, yy, cc):
            start = pl.multiple_of(((zz * 2 + yy) * 2 + cc) * rw, rw)
            return buf.at[pl.ds(start, rw), :]

        return slot

    def col_slot(buf):
        def slot(zz, yy, cc):
            return buf.at[zz * 2 + yy, :, pl.ds(pl.multiple_of(cc * cw, cw), cw)]

        return slot

    deep = half_ff // 2

    def down_slot(k):
        def slot(zz, yy, cc):
            return Dn.at[zz * 2 + yy, pl.ds(k * deep, deep), pl.ds(pl.multiple_of(cc * cw, cw), cw)]

        return slot

    sP, sO, sG, sU = row_slot(P), col_slot(O), row_slot(G), row_slot(U)
    slots = (sP, sO, sG, sU, down_slot(0), down_slot(1))
    DOWN = (4, 5)

    def sem_of(kind, zz, yy, cc):
        return wsem.at[kind, (zz * 2 + yy) * 2 + cc]

    def fwd(kind, zz, yy, cc, to):
        ref = functools.partial(slots[kind], zz, yy, cc)
        put(ref, ref, functools.partial(sem_of, kind, zz, yy, cc), to)

    def arrive(kind, zz, yy, cc):
        side = "sib" if cc is c1 else "row" if yy is y1 else "col"
        got(slots[kind](zz, yy, cc), sem_of(kind, zz, yy, cc), f"{side}{kind}")

    sib = dev(z, y, c1, x)
    row = dev(z, y1, c, x)
    peer = dev(zp, y, c, x)
    xdev = dev(z, y, c, x1)
    mirror = dev(zm, y, c, x)
    diagonal = dev(zm, y, c, x1)

    parts = [ref.shape[1] // 2 for ref in (q_h, k_h, v_h, g_h)]
    ends = np.cumsum([0] + parts).tolist()
    mine = pl.multiple_of(((z * 2 + y) * 2 + c) * rw, rw)
    own_p, stage_p = [], []
    for i, ref in enumerate((q_h, k_h, v_h, g_h)):
        to = pl.ds(ends[i], parts[i])
        at = pl.ds(pl.multiple_of(y * parts[i], 128), parts[i])
        own_p.append(take(ref.at[:, at], P.at[pl.ds(mine, rw), to]))
        at = pl.ds(pl.multiple_of(y1 * parts[i], 128), parts[i])
        stage_p.append(take(ref.at[:, at], Ps.at[:, to]))
    own_o = take(o_h, sO(z, y, c))
    own_t = [take(tok_h, tok.at[0, x])] + [take(ref, gn.at[x, k]) for k, ref in enumerate((mixg_h, ffng_h))]
    own_t += [take(cos_h, cos_ref), take(sin_h, sin_ref), take(lastg_h, gl)]
    gs[...] = jnp.where(lax.broadcasted_iota(jnp.int32, gs.shape, 0) == 0, scale_s[0], scale_s[1])
    at_b = pl.multiple_of(b * half_ff, 128)
    at_o = pl.multiple_of((1 - b) * half_ff, 128)
    own_g = take(fg_h.at[:, pl.ds(at_b, half_ff)], sG(z, y, c))
    own_u = take(fu_h.at[:, pl.ds(at_b, half_ff)], sU(z, y, c))
    own_d = take(fd_h.at[pl.ds(at_b, half_ff), :], col_slot(Dn)(z, y, c))

    barrier = pltpu.get_barrier_semaphore()
    friends = [sib, row, xdev, diagonal] + [dev((z + k) % 4, y, c, x) for k in (1, 2, 3)]
    for to in friends:
        pl.semaphore_signal(barrier, inc=1, device_id=to, device_id_type=MESH)
    pl.semaphore_wait(barrier, len(friends))

    put(lambda: tok_h, lambda: tok.at[0, x], lambda: asem.at[0], xdev)
    put(lambda: mixg_h, lambda: gn.at[x, 0], lambda: asem.at[1], xdev)
    put(lambda: ffng_h, lambda: gn.at[x, 1], lambda: asem.at[35], xdev)

    other = {
        2: lambda: fg_h.at[:, pl.ds(at_o, half_ff)],
        3: lambda: fu_h.at[:, pl.ds(at_o, half_ff)],
        4: lambda: fd_h.at[pl.ds(at_o, deep), :],
        5: lambda: fd_h.at[pl.ds(pl.multiple_of(at_o + deep, 16), deep), :],
    }
    beyond = dev(near_o, y, c, x)

    def own(kind, to):
        fwd(kind, z, y, c, to)

    def cross(kind):
        slot = functools.partial(slots[kind], z, y, c)
        put(other[kind], slot, functools.partial(sem_of, kind, z, y, c), beyond)

    def relay(kind, zz, *to):
        arrive(kind, zz, y, c)
        for device in to + (row, sib):
            fwd(kind, zz, y, c, device)

    def arrive_down(*place):
        for kind in DOWN:
            arrive(kind, *place)

    def down(act, *args):
        return [(act, kind) + args for kind in DOWN]

    def lend(kind):
        arrive(kind, z, y1, c)
        fwd(kind, z, y1, c, peer)
        fwd(kind, z, y1, c, sib)

    def relay_in(kind, zz):
        arrive(kind, zz, y, c)
        fwd(kind, zz, y, c, sib)

    def shared(kind, zz):
        arrive(kind, zz, y1, c)
        fwd(kind, zz, y1, c, sib)

    def share(kind):
        for zz in (z, zp, near_o, far_o):
            arrive(kind, zz, y1, c)
            fwd(kind, zz, y1, c, sib)

    def line(zz, yy, *to):
        arrive(0, zz, yy, c)
        for device in to + (sib,):
            fwd(0, zz, yy, c, device)

    for copy in stage_p + own_p:
        copy.wait()
    put(lambda: Ps, lambda: sP(z, y, c), lambda: sem_of(0, z, y, c), row)
    own(0, peer)
    only(near, (own, 0, beyond))
    own(0, sib)
    put(lambda: tok_h, lambda: tok.at[1, x], lambda: asem.at[2], row)
    put(lambda: gs, lambda: gr, lambda: asem.at[3], row)
    own_o.wait()
    own(1, row)
    own(1, peer)
    only(near, (own, 1, beyond))
    own(1, sib)
    own_g.wait()
    own(2, row)
    own(2, sib)
    only(far, (line, z, y1, peer), (own, 2, peer), (line, zp, y), (relay, 1, zp), (line, zp, y1))
    only(
        near,
        (line, z, y1, peer, beyond),
        (line, zp, y, beyond),
        (line, near_o, y, peer),
        (relay, 1, zp, beyond),
        (relay, 1, near_o, peer),
        (line, zp, y1, beyond),
        (line, near_o, y1, peer),
    )

    for copy in own_t:
        copy.wait()
    got(tok.at[0, x1], asem.at[0], "tok")
    got(gn.at[x1, 0], asem.at[1])
    got(gn.at[x1, 1], asem.at[35])

    def norm_rows(first, second, gain_row, dst, base):
        chunk = 32
        gains = [gn[half, gain_row].astype(F32) for half in range(2)]

        @pl.loop(0, rows // chunk)
        def _(i):
            at = pl.ds(pl.multiple_of(i * chunk, chunk), chunk)
            one = first[at, :].astype(F32)
            two = second[at, :].astype(F32)
            total = jnp.sum(one * one, axis=1, keepdims=True) + jnp.sum(two * two, axis=1, keepdims=True)
            scale = lax.rsqrt(total / width + EPS)
            to = pl.ds(pl.multiple_of(base + i * chunk, chunk), chunk)
            for half, values in enumerate((one, two)):
                for k in range(feat // 128):
                    part = values[:, k * 128 : (k + 1) * 128] * scale * gains[half][k : k + 1, :]
                    dst[to, half * feat + k * 128 : half * feat + (k + 1) * 128] = part.astype(BF16)

    norm_rows(tok.at[0, 0], tok.at[0, 1], 0, N2, 0)
    got(tok.at[1, x], asem.at[2], "tok")
    put(lambda: tok.at[1, x], lambda: tok.at[1, x], lambda: asem.at[4], xdev)
    got(gr, asem.at[3])
    own_u.wait()
    own_d.wait()
    only(
        far,
        (line, near_o, y),
        (line, near_o, y1),
        (relay, 1, near_o),
        (own, 3, row),
        (cross, 2),
        (line, far_o, y),
        (line, far_o, y1),
        (relay, 1, far_o),
        (own, 3, peer),
        (cross, 3),
    )
    only(
        near,
        (line, far_o, y, peer),
        (line, far_o, y1, peer),
        (relay, 1, far_o, peer),
        (own, 2, peer),
        (cross, 2),
        (relay, 2, zp),
        (cross, 3),
    )
    got(tok.at[1, x1], asem.at[4], "tok")
    norm_rows(tok.at[1, 0], tok.at[1, 1], 0, N2, rows)
    for zz in range(4):
        for yy in range(2):
            arrive(0, zz, yy, c1)

    @pl.loop(0, P.shape[1] // WIDE)
    def _(j):
        at = pl.ds(pl.multiple_of(j * WIDE, WIDE), WIDE)
        pr[:, at] = mm(N2[...], P[:, at])

    blk = rows // 2
    t = lax.broadcasted_iota(jnp.int32, (rows, rows), 0)
    s = lax.broadcasted_iota(jnp.int32, (rows, rows), 1)
    late_t, late_s = t >= blk, s >= blk
    apart = (t - s).astype(F32)
    into = (t - (blk - 1)).astype(F32)
    left = ((blk - 1) - s).astype(F32)
    causal = t >= s
    lane = lax.broadcasted_iota(jnp.int32, (rows, 2 * DK), 1)
    early = (lane % DK) < DK // 2
    first_head = lane < DK

    def turn(v):
        swapped = jnp.where(early, pltpu.roll(v, 2 * DK - DK // 2, 1), pltpu.roll(v, DK // 2, 1))
        return v * cos_ref[...] + swapped * sin_ref[...]

    def retain_rows(at, scales, dst):
        s0, s1 = scales[0:1, 0:1], scales[1:2, 0:1]
        for two in range(heads // 4):
            cols = slice(ends[0] + two * 2 * DK, ends[0] + (two + 1) * 2 * DK)
            query = turn(pr[at, cols]).astype(BF16)
            cols = slice(ends[1] + two * 2 * DK, ends[1] + (two + 1) * 2 * DK)
            key = (turn(pr[at, cols]) * DK ** (-0.5)).astype(BF16)
            for side in range(2):
                h = 2 * two + side
                rate = rate_s[y * (heads // 2) + h]
                keep = first_head if side == 0 else jnp.logical_not(first_head)
                part = jnp.where(keep, query, jnp.zeros_like(query))
                scores = lax.dot_general(part, key, (((1,), (1,)), ((), ())), preferred_element_type=F32)
                la0, la1 = -(rate * s0), -(rate * s1)
                power = jnp.where(late_t, la1, la0) * apart
                power = jnp.where(jnp.logical_and(late_t, jnp.logical_not(late_s)), la1 * into + la0 * left, power)
                scores = scores * jnp.where(causal, jnp.exp(jnp.where(causal, power, 0.0)), 0.0)
                high = scores.astype(BF16)
                low = (scores - high.astype(F32)).astype(BF16)
                value = pr[at, ends[2] + h * DV : ends[2] + (h + 1) * DV].astype(BF16)
                ret = mm(high, value) + mm(low, value)
                ret = ret * lax.rsqrt(jnp.mean(ret * ret, axis=1, keepdims=True) + EPS)
                gate = pr[at, ends[3] + h * DV : ends[3] + (h + 1) * DV]
                dst[:, h * DV : (h + 1) * DV] = (ret * silu(gate)).astype(BF16)

    retain_rows(slice(rows, 2 * rows), gr, gsend)
    put(lambda: gsend, lambda: gated.at[y], lambda: asem.at[5], row)
    retain_rows(slice(0, rows), gs, gated.at[y])
    only(far, (relay, 2, zp), (own, 3, sib))
    only(near, (relay, 2, near_o, peer))
    share(1)
    for zz in range(4):
        for yy in range(2):
            arrive(1, zz, yy, c1)
    got(gated.at[y1], asem.at[5], "gated")

    per = feat // WIDE
    half_o = O.shape[1] // 2

    def out_block(side, j):
        weights = O.at[side * per + j]
        return mm(gated[0], weights[0:half_o, :]) + mm(gated[1], weights[half_o:, :])

    def send_mix(j):
        put(lambda: sm.at[j], lambda: rm.at[j], lambda: asem.at[6 + j], xdev)

    for j in range(per):
        sm[j] = out_block(x1, j).astype(BF16)
        send_mix(j)
    for j in range(per):
        pm[j] = out_block(x, j).astype(BF16)

    only(far, (relay, 2, near_o), *down(own, row), *down(own, sib))
    only(
        near,
        (relay, 2, far_o, peer),
        (own, 3, peer),
        (own, 3, row),
        (own, 3, sib),
        (relay_in, 3, zp),
    )

    def block(j):
        return pl.ds(j * WIDE, WIDE)

    def send_resid(j):
        put(lambda: R.at[0, x, :, block(j)], lambda: R.at[1, x, :, block(j)], lambda: asem.at[10 + j], mirror)
        put(lambda: R.at[0, x, :, block(j)], lambda: R.at[0, x, :, block(j)], lambda: asem.at[14 + j], xdev)

    def pass_resid(j):
        got(R.at[1, x, :, block(j)], asem.at[10 + j], "R1")
        put(lambda: R.at[1, x, :, block(j)], lambda: R.at[1, x, :, block(j)], lambda: asem.at[18 + j], xdev)

    for j in range(per):
        got(rm.at[j], asem.at[6 + j], "mix")
        mix = pm[j].astype(F32) + rm[j].astype(F32)
        R[0, x, :, block(j)] = (tok[0, x, :, block(j)].astype(F32) + mix).astype(BF16)
        send_resid(j)
    only(far, (relay, 2, far_o), *down(own, peer), (lend, 3), (relay, 3, zp))
    only(near, (relay, 3, near_o, peer), (relay, 3, far_o, peer), *down(own, row), *down(own, sib))
    pass_resid(0)
    pass_resid(1)
    only(near, *down(cross), *down(own, peer))
    only(far, *down(cross), (relay, 3, near_o))
    pass_resid(2)
    pass_resid(3)
    only(near, *down(relay_in, zp))
    only(far, *down(lend), (relay, 3, far_o))
    share(2)
    for j in range(per):
        got(R.at[0, x1, :, block(j)], asem.at[14 + j], "R0x")
    norm_rows(R.at[0, 0], R.at[0, 1], 1, N2, 0)
    for j in range(per):
        got(R.at[1, x1, :, block(j)], asem.at[18 + j], "R1x")
    norm_rows(R.at[1, 0], R.at[1, 1], 1, N2, rows)

    theirs, ours = slice(rows, 2 * rows), slice(0, rows)

    def over_columns(act):
        whole = half_ff // WIDE

        @pl.loop(0, whole)
        def _(j):
            act(pl.ds(pl.multiple_of(j * WIDE, WIDE), WIDE))

        if half_ff % WIDE:
            act(pl.ds(whole * WIDE, half_ff % WIDE))

    def gate_columns(at):
        gacc[:, at] = silu(mm(N2[...], G[:, at]))

    def up_of(part, at, *chips):
        total = 0.0
        for zz, yy in chips:
            deep_at = pl.ds(pl.multiple_of((zz * 2 + yy) * 2 * rw, 2 * rw), 2 * rw)
            total = total + mm(N2[part, deep_at], U[deep_at, at])
        return total

    def up_columns(at):
        for part in (theirs, ours):
            uacc[part, at] = up_of(
                part, at, (z, y), (zp, y), (near_o, y), (far_o, y), (z, y1), (zp, y1), (near_o, y1)
            )

    def hidden_columns(at):
        for part in (theirs, ours):
            up = uacc[part, at] + up_of(part, at, (far_o, y1))
            hid[part, at] = (gacc[part, at] * up).astype(BF16)

    def share_up(zz):
        arrive(3, zz, y1, c)
        fwd(3, zz, y1, c, sib)

    only(near, (shared, 3, z), *down(shared, z))
    share_up(zp)
    for zz in range(4):
        for yy in range(2):
            arrive(2, zz, yy, c1)
    over_columns(gate_columns)
    share_up(near_o)
    only(near, *down(relay, near_o, peer))
    only(far, *down(relay, zp))
    for zz in (z, zp, near_o, far_o):
        arrive(3, zz, y, c1)
    for zz in (z, zp, near_o):
        arrive(3, zz, y1, c1)
    over_columns(up_columns)
    share_up(far_o)
    only(near, *down(relay, far_o, peer))
    arrive(3, far_o, y1, c1)
    over_columns(hidden_columns)

    at_end = far.astype(jnp.int32)

    def chip(half, i):
        return jnp.where(i % 2 == 1, 3 * half, 1 + half), jnp.where(i >= 2, y1, y)

    def columns(i):
        zz, yy = chip(x, i)
        return pl.ds(pl.multiple_of(((zz - 2 * x) * 2 + yy) * WIDE, WIDE), WIDE)

    def send_x(i, k, start):
        at = pl.ds(start, rows)
        put(lambda: sx.at[i, at, :], lambda: rx.at[i, at, :], lambda: asem.at[22 + 2 * i + k], xdev)

    def give(zz, yy, i, part):
        sx[i, part, :] = mm(hid[part, :], Dn[zz * 2 + yy]).astype(BF16)
        send_x(i, 0 if part is theirs else 1, part.start)

    def give_last(zz, yy):
        sx[3, theirs, :] = mm(hid[theirs, :], Dn[zz * 2 + yy]).astype(BF16)
        put(lambda: sx.at[3, pl.ds(rows, rows), :], lambda: rd, lambda: asem.at[36], diagonal)

    def keep(zz, yy, i):
        pmine[i] = mm(hid[...], Dn[zz * 2 + yy])

    def ready(zz):
        for kind in DOWN:
            arrive(kind, zz, y1, c)
            fwd(kind, zz, y1, c, sib)

    def combine(i):
        got(rx.at[i, pl.ds(rows, rows), :], asem.at[22 + 2 * i], "rx")
        sz[i] = (pmine[i, theirs, :] + rx[i, theirs, :].astype(F32)).astype(BF16)
        put(lambda: sz.at[i], lambda: rz.at[i], lambda: asem.at[30 + i], mirror)

    def pass_last():
        sz[3] = pmine[3, theirs, :].astype(BF16)
        put(lambda: sz.at[3], lambda: rz.at[3], lambda: asem.at[33], mirror)

    def take_last():
        got(rd, asem.at[36], "rd")
        tot[3] = tot[3] + rd[...].astype(F32)

    def add(i):
        got(rx.at[i, pl.ds(0, rows), :], asem.at[23 + 2 * i], "rx")
        resid = R[0, x, :, columns(i)].astype(F32)
        tot[i] = resid + (pmine[i, ours, :] + rx[i, ours, :].astype(F32))

    def out_copy(i):
        return pltpu.make_async_copy(tot.at[i], out_h.at[:, columns(i)], osem.at[i])

    def close(i):
        got(rz.at[i], asem.at[30 + i], "rz")
        now = tot[i] + rz[i].astype(F32)
        tot[i] = now
        square = now * now
        return square[:, : WIDE // 2] + square[:, WIDE // 2 :]

    first = (at_end, 1 - at_end, 2 + at_end, 3 - at_end)
    order = [jnp.where(here, i, k) for k, i in enumerate(first)]
    b0, b1, b2, b3 = first
    arrive_down(z, y, c1)
    arrive_down(zp, y, c1)
    only(
        away,
        (give, z, y, b0, theirs),
        (give, zp, y, b1, theirs),
        (give, z, y, b0, ours),
    )
    only(here, (keep, z, y, b0), (keep, zp, y, b1))
    only(far, *down(relay, near_o))
    arrive_down(near_o, y, c1)
    only(here, (give, near_o, y, 0, theirs))
    only(far, *down(relay, far_o))
    ready(zp)
    arrive_down(far_o, y, c1)
    only(here, (give, far_o, y, 1, theirs), (give, near_o, y, 0, ours), (give, far_o, y, 1, ours))
    arrive_down(z, y1, c1)
    arrive_down(zp, y1, c1)
    only(
        away,
        (give, z, y1, b2, theirs),
        (give, zp, y1, b3, theirs),
        (give, zp, y, b1, ours),
        (give, z, y1, b2, ours),
        (give, zp, y1, b3, ours),
        (keep, near_o, y, 0),
        (keep, far_o, y, 1),
    )
    only(here, (keep, z, y1, b2), (keep, zp, y1, b3))
    combine(order[0])
    ready(near_o)
    combine(order[1])
    arrive_down(near_o, y1, c1)
    only(here, (give, near_o, y1, 2, theirs), (give, near_o, y1, 2, ours))
    only(away, (keep, near_o, y1, 2))
    only(here, (combine, order[2]), (combine, order[3]))
    ready(far_o)
    arrive_down(far_o, y1, c1)
    only(end_here, (give_last, far_o, y1))
    only(mid_here, (give, far_o, y1, 3, theirs))
    only(here, (give, far_o, y1, 3, ours))
    only(away, (keep, far_o, y1, 3))
    only(end_away, (pass_last,))
    drain(near, far)
    only(away, (combine, 2))
    add(order[0])
    add(order[1])
    squares = close(order[0])
    only(mid_away, (combine, 3))
    squares = squares + close(order[1])
    add(order[2])
    add(order[3])
    only(end_here, (take_last,))
    squares = squares + close(order[2])
    squares = squares + close(order[3])
    mine_sq = jnp.broadcast_to(jnp.sum(squares, axis=1, keepdims=True), (rows, 128))
    ss_s[...] = mine_sq.T[0:8, :]
    put(lambda: ss_s, lambda: ss_r, lambda: asem.at[34], xdev)
    gf[...] = gl[...].astype(F32)
    drain()
    got(ss_r, asem.at[34], "ss")
    total = ss_s[0:1, :] + ss_r[0:1, :]
    total = jnp.broadcast_to(total, (128, rows)).T[:, 0:1]
    scale = lax.rsqrt(total / width + EPS)
    for i in range(4):
        zz, yy = chip(x, i)
        for k in range(WIDE // 128):
            gain = gf[pl.ds(((zz - 2 * x) * 2 + yy) * (WIDE // 128) + k, 1), :]
            lanes = slice(k * 128, (k + 1) * 128)
            tot[i, :, lanes] = tot[i, :, lanes] * scale * gain
        out_copy(i).start()
    for i in range(4):
        out_copy(i).wait()


def tables(rows):
    half = DK // 2
    inverse = np.float32(THETA) ** (-np.arange(half, dtype=np.float32) / np.float32(half))
    angle = (np.arange(rows, dtype=np.float32) % SEQ_LEN)[:, None] * inverse
    cosine, sine = np.cos(angle), np.sin(angle)
    return (
        np.concatenate([cosine] * 4, axis=1).astype(np.float32),
        np.concatenate([-sine, sine, -sine, sine], axis=1).astype(np.float32),
    )


def fused(
    tokens,
    mix_gain,
    query_weight,
    key_weight,
    value_weight,
    output_gate_weight,
    out_weight,
    head_rates,
    block_scale,
    ffn_gain,
    ff_gate,
    ff_up,
    ff_down,
    final_gain,
):
    rows, feat = tokens.shape
    size = lax.axis_size("fs")
    chips = size // 2
    width = 2 * feat
    half_ff = ff_gate.shape[1] // 2
    joint = sum(w.shape[1] for w in (query_weight, key_weight, value_weight, output_gate_weight)) // 2
    heads = head_rates.shape[0]
    cosine, sine = tables(rows)
    cw = out_weight.shape[1]
    hbm = pl.BlockSpec(memory_space=pl.ANY)
    smem = pl.BlockSpec(memory_space=pltpu.SMEM)
    dma = pltpu.SemaphoreType.DMA
    out = pl.pallas_call(
        layer_kernel,
        out_shape=jax.ShapeDtypeStruct((rows, feat), F32),
        in_specs=[hbm] * 9 + [smem] * 2 + [hbm] * 5,
        out_specs=hbm,
        scratch_shapes=[
            pltpu.VMEM((2, 2, rows, feat), BF16),
            pltpu.VMEM((2, 2, feat // 128, 128), BF16),
            pltpu.VMEM((feat // 128, 128), BF16),
            pltpu.VMEM((feat // 128, 128), F32),
            pltpu.VMEM((8, 128), F32),
            pltpu.VMEM((8, 128), F32),
            pltpu.VMEM((rows, 128), F32),
            pltpu.VMEM((rows, 128), F32),
            pltpu.VMEM((query_weight.shape[0], joint), BF16),
            pltpu.VMEM((width, joint), BF16),
            pltpu.VMEM((chips, out_weight.shape[0], 2 * cw), BF16),
            pltpu.VMEM((width, half_ff), BF16),
            pltpu.VMEM((width, half_ff), BF16),
            pltpu.VMEM((chips, half_ff, 2 * cw), BF16),
            pltpu.VMEM((2 * rows, joint), F32),
            pltpu.VMEM((rows, heads * DV // 2), BF16),
            pltpu.VMEM((2, rows, heads * DV // 2), BF16),
            pltpu.VMEM((feat // WIDE, rows, WIDE), BF16),
            pltpu.VMEM((feat // WIDE, rows, WIDE), BF16),
            pltpu.VMEM((feat // WIDE, rows, WIDE), BF16),
            pltpu.VMEM((2, 2, rows, feat), BF16),
            pltpu.VMEM((2 * rows, width), BF16),
            pltpu.VMEM((2 * rows, half_ff), F32),
            pltpu.VMEM((2 * rows, half_ff), F32),
            pltpu.VMEM((2 * rows, half_ff), BF16),
            pltpu.VMEM((4, 2 * rows, WIDE), BF16),
            pltpu.VMEM((4, 2 * rows, WIDE), BF16),
            pltpu.VMEM((4, 2 * rows, WIDE), F32),
            pltpu.VMEM((4, rows, WIDE), BF16),
            pltpu.VMEM((4, rows, WIDE), BF16),
            pltpu.VMEM((rows, WIDE), BF16),
            pltpu.VMEM((4, rows, WIDE), F32),
            pltpu.VMEM((8, rows), F32),
            pltpu.VMEM((8, rows), F32),
            dma((18,)),
            dma((73,)),
            dma((6, size)),
            dma((37,)),
            dma((4,)),
        ],
        compiler_params=pltpu.CompilerParams(
            collective_id=0, has_side_effects=True, vmem_limit_bytes=60 * 2**20
        ),
    )(
        tokens,
        mix_gain.reshape(feat // 128, 128),
        ffn_gain.reshape(feat // 128, 128),
        final_gain.reshape(feat // 128, 128),
        query_weight,
        key_weight,
        value_weight,
        output_gate_weight,
        out_weight,
        head_rates,
        block_scale,
        ff_gate,
        ff_up,
        ff_down,
        cosine,
        sine,
    )
    return out.astype(BF16)


def kernel_fits(mesh, tokens, query_weight, ff_gate, head_rates):
    size, parts = mesh.shape["fs"], mesh.shape["tp"]
    if size != 4 * 2 * 2 or parts != 2:
        return False
    rows, width = tokens.shape[0] // size, tokens.shape[1]
    return (
        rows == SEQ_LEN
        and SEQ_LEN == 2 * BLK
        and width // size * 2 == WIDE
        and ff_gate.shape[1] % (4 * 128) == 0
        and head_rates.shape[0] % (4 * parts) == 0
    )


def dispatch(mesh, *args):
    fits = kernel_fits(mesh, args[0], args[2], args[10], args[7])
    return jax.shard_map(
        fused if fits else body,
        mesh=mesh,
        in_specs=SPECS,
        out_specs=P("fs", "tp"),
        check_vma=False,
    )(*args)


SPECS = (
    P("fs", "tp"),
    P("tp"),
    P("fs", "tp"),
    P("fs", "tp"),
    P("fs", "tp"),
    P("fs", "tp"),
    P("tp", "fs"),
    P("tp"),
    P("fs"),
    P("tp"),
    P("fs", "tp"),
    P("fs", "tp"),
    P("tp", "fs"),
    P("tp"),
)


def solution(mesh):
    return functools.partial(dispatch, mesh)
```

```python
import functools

import jax
import jax.numpy as jnp
import numpy as np
from jax import lax
from jax.experimental import pallas as pl
from jax.experimental.pallas import tpu as pltpu
from jax.sharding import PartitionSpec as P

D = 2048
DK = 64
DV = 128
BLK = 128
SEQ_LEN = 256


EPS = 1e-06
THETA = 10000.0


def rms_norm(values, gain):
    scale = lax.rsqrt(jnp.mean(values * values, axis=-1, keepdims=True) + EPS)
    return values * scale * gain.astype(jnp.float32)


def rotate(values, positions):
    half = values.shape[-1] // 2
    inverse = THETA ** (-jnp.arange(half, dtype=jnp.float32) / half)
    angle = positions.astype(jnp.float32)[:, None] * inverse
    cosine = jnp.cos(angle)[:, None, :]
    sine = jnp.sin(angle)[:, None, :]
    first = values[..., :half]
    second = values[..., half:]
    return jnp.concatenate(
        [first * cosine - second * sine, second * cosine + first * sine], axis=-1
    )


def retain(query, key, value, rates, scales):
    rows, heads_here, width_k = query.shape
    width_v = value.shape[-1]
    nblk = rows // BLK
    hi = lax.Precision.HIGHEST
    qblk = query.astype(jnp.float32).reshape(nblk, BLK, heads_here, width_k)
    kblk = key.astype(jnp.float32).reshape(nblk, BLK, heads_here, width_k)
    vblk = value.astype(jnp.float32).reshape(nblk, BLK, heads_here, width_v)
    logdec = -rates[None, :] * scales[:, None]
    steps = jnp.arange(BLK, dtype=jnp.float32)
    offset = steps[:, None] - steps[None, :]
    causal = offset >= 0
    inside = jnp.where(
        causal[None, None],
        jnp.exp(logdec[:, :, None, None] * jnp.where(causal, offset, 0.0)[None, None]),
        0.0,
    )
    scores = jnp.einsum("nchd,nmhd->nhcm", qblk, kblk, precision=hi) * inside
    inner = jnp.einsum("nhcm,nmhe->nche", scores, vblk, precision=hi)
    zeta = jnp.exp(logdec[:, :, None] * (BLK - 1.0 - steps)[None, None, :])
    kv_block = jnp.einsum(
        "nchd,nche->nhde", kblk * jnp.transpose(zeta, (0, 2, 1))[..., None], vblk, precision=hi
    )
    hold = jnp.exp(logdec * BLK)
    per_seq = SEQ_LEN // BLK
    fresh = (jnp.arange(nblk, dtype=jnp.int32) % per_seq == 0).astype(jnp.float32)

    def advance(state, inputs):
        kv_now, hold_now, fresh_now = inputs
        before = state * (1.0 - fresh_now)
        return (before * hold_now[:, None, None] + kv_now, before)

    start = jnp.zeros((heads_here, width_k, width_v), jnp.float32)
    _, before = lax.scan(advance, start, (kv_block, hold, fresh), unroll=True)
    xi = jnp.exp(logdec[:, :, None] * (steps + 1.0)[None, None, :])
    cross = jnp.einsum(
        "nchd,nhde->nche", qblk * jnp.transpose(xi, (0, 2, 1))[..., None], before, precision=hi
    )
    total = inner + cross
    total = total * lax.rsqrt(jnp.mean(total * total, axis=-1, keepdims=True) + EPS)
    return total.reshape(rows, heads_here * width_v)


def chip_ring(size):
    chips = size // 2
    return list(range(0, chips, 2)) + list(range(1, chips, 2))[::-1]


def ring_place(size):
    ring = chip_ring(size)
    me = lax.axis_index("fs")
    chip = me // 2
    place = jnp.zeros((), jnp.int32)
    for index, member in enumerate(ring):
        place = jnp.where(chip == member, index, place)
    return place, me % 2


def after(value, *others):
    return lax.optimization_barrier((value,) + tuple(others))[0]


def circulate(block, axis, gates=()):
    size = lax.axis_size("fs")
    ring = chip_ring(size)
    chips = len(ring)
    onward = [
        (2 * ring[i] + core, 2 * ring[(i + 1) % chips] + core)
        for i in range(chips)
        for core in range(2)
    ]
    back = [(target, source) for source, target in onward]
    swap = [(i, i ^ 1) for i in range(size)]
    held = {0: block}
    reach = (chips - 1) // 2
    down = up = block
    for step in range(1, reach + 1):
        if len(gates) >= step and gates[step - 1]:
            down = after(down, *gates[step - 1])
            up = after(up, *gates[step - 1])
        down = lax.ppermute(down, "fs", onward)
        up = lax.ppermute(up, "fs", back)
        held[-step] = down
        held[step] = up
    if chips % 2 == 0 and chips > 1:
        cut = 1 - axis
        half = block.shape[cut] // 2
        if len(gates) > reach and gates[reach]:
            down = after(down, *gates[reach])
            up = after(up, *gates[reach])
        first = lax.ppermute(lax.slice_in_dim(down, 0, half, axis=cut), "fs", onward)
        second = lax.ppermute(lax.slice_in_dim(up, half, None, axis=cut), "fs", back)
        held[reach + 1] = jnp.concatenate([first, second], axis=cut)
    groups = []
    for offsets in order_of(size):
        own = jnp.concatenate([held[o] for o in offsets], axis=axis)
        groups.append((own, lax.ppermute(own, "fs", swap)))
    return held, groups


def order_of(size):
    chips = size // 2
    reach = (chips - 1) // 2
    groups = [list(range(-reach, reach + 1))]
    if chips > 1 and chips % 2 == 0:
        groups.append([reach + 1])
    return groups


def lane_of(values, lane, wide):
    count = values.shape[1] // (2 * wide)
    return [values[:, (2 * c + lane) * wide : (2 * c + lane + 1) * wide] for c in range(count)]


def to_ring(values, place, core):
    size = lax.axis_size("fs")
    wide = values.shape[1] // size
    ring = chip_ring(size)
    chips = len(ring)
    groups = order_of(size)
    start = (place + groups[0][0] + chips) % chips
    lanes = []
    for lane in range(2):
        pieces = lane_of(values, lane, wide)
        ringed = jnp.concatenate([pieces[c] for c in ring] * 2, axis=1)
        lanes.append(lax.dynamic_slice_in_dim(ringed, start * wide, chips * wide, axis=1))
    own = jnp.where(core == 0, lanes[0], lanes[1])
    other = jnp.where(core == 0, lanes[1], lanes[0])
    result, edge = [], 0
    for offsets in groups:
        end = edge + len(offsets) * wide
        result.append((own[:, edge:end], other[:, edge:end]))
        edge = end
    return result


def from_ring(groups, place, core):
    size = lax.axis_size("fs")
    ring = chip_ring(size)
    chips = len(ring)
    own = jnp.concatenate([own for own, _ in groups], axis=1)
    other = jnp.concatenate([other for _, other in groups], axis=1)
    wide = own.shape[1] // chips
    start = (2 * chips - place - order_of(size)[0][0]) % chips
    lanes = []
    for lane in range(2):
        straight = jnp.where(core == lane, own, other)
        doubled = jnp.concatenate([straight, straight], axis=1)
        lanes.append(lax.dynamic_slice_in_dim(doubled, start * wide, chips * wide, axis=1))
    spot = {c: i for i, c in enumerate(ring)}
    return jnp.concatenate(
        [
            lanes[lane][:, spot[c] * wide : (spot[c] + 1) * wide]
            for c in range(chips)
            for lane in range(2)
        ],
        axis=1,
    )


def tp_gather(values, axis):
    if lax.axis_size("tp") != 2:
        return lax.all_gather(values, "tp", axis=axis, tiled=True)
    other = lax.ppermute(values, "tp", [(0, 1), (1, 0)])
    mine = lax.axis_index("tp") == 0
    return jnp.concatenate(
        [jnp.where(mine, values, other), jnp.where(mine, other, values)], axis=axis
    )


def tp_sum(values):
    if lax.axis_size("tp") != 2:
        return lax.psum(values, "tp")
    return values + lax.ppermute(values, "tp", [(0, 1), (1, 0)])


def tp_scatter_sum(partial):
    if lax.axis_size("tp") != 2:
        pieces = lax.all_to_all(
            partial.reshape(partial.shape[0], lax.axis_size("tp"), -1), "tp", 1, 1
        )
        return jnp.sum(pieces.astype(jnp.float32), axis=1)
    half = partial.shape[1] // 2
    low = lax.axis_index("tp") == 0
    keep = jnp.where(low, partial[:, :half], partial[:, half:])
    send = jnp.where(low, partial[:, half:], partial[:, :half])
    got = lax.ppermute(send, "tp", [(0, 1), (1, 0)])
    return keep.astype(jnp.float32) + got.astype(jnp.float32)


def product_rows(left, groups, columns=slice(None), result=0.0):
    for pieces, blocks in zip(left, groups):
        for piece, block in zip(pieces, blocks):
            result = result + jnp.dot(
                piece, block[:, columns], preferred_element_type=jnp.float32
            )
    return result


def product_columns(left, groups, place, core, columns=None):
    terms = []
    for blocks in groups:
        pair = []
        for block in blocks:
            if columns is None:
                dims, right = (((1,), (0,)), ((), ())), block
            else:
                dims, right = (((1,), (1,)), ((), ())), block[:, columns]
            term = lax.dot_general(left, right, dims, preferred_element_type=jnp.float32)
            pair.append(term.astype(jnp.bfloat16))
        terms.append(pair)
    return from_ring(terms, place, core)


def body(
    tokens,
    mix_gain,
    query_weight,
    key_weight,
    value_weight,
    output_gate_weight,
    out_weight,
    head_rates,
    block_scale,
    ffn_gain,
    ff_gate,
    ff_up,
    ff_down,
    final_gain,
):
    rows = tokens.shape[0]
    heads_here = head_rates.shape[0]
    size = lax.axis_size("fs")
    place, core = ring_place(size)
    reach = (size // 2 - 1) // 2
    positions = jnp.arange(rows, dtype=jnp.int32) % SEQ_LEN

    bundle = jnp.concatenate(
        [query_weight, key_weight, value_weight, output_gate_weight, out_weight.T], axis=1
    )
    hops, proj = circulate(bundle, 0)
    last = (hops[-reach], hops[reach])

    whole = tp_gather(tokens, 1)
    gains = tp_gather(jnp.stack([mix_gain, ffn_gain]), 1)
    normed = rms_norm(whole.astype(jnp.float32), gains[0]).astype(jnp.bfloat16)
    width = bundle.shape[1] - out_weight.shape[0]
    projected = product_rows(to_ring(normed, place, core), proj, slice(0, width))
    ends = [query_weight.shape[1], key_weight.shape[1], value_weight.shape[1]]
    qproj, kproj, vproj, gproj = jnp.split(
        projected, [ends[0], ends[0] + ends[1], sum(ends)], axis=1
    )
    query = rotate(qproj.reshape(rows, heads_here, DK), positions).astype(jnp.bfloat16)
    key = (rotate(kproj.reshape(rows, heads_here, DK), positions) * DK ** (-0.5)).astype(
        jnp.bfloat16
    )
    value = vproj.astype(jnp.bfloat16).reshape(rows, heads_here, DV)
    normret = retain(query, key, value, head_rates, block_scale)
    gated = (normret * jax.nn.silu(gproj)).astype(jnp.bfloat16)
    opposite = tuple(hops[o] for o in order_of(size)[-1])
    gate_hops, gates = circulate(ff_gate, 0, ((), opposite, (projected,)))
    up_hops, ups = circulate(ff_up, 0, (last, (), (gated,)))
    mix = tp_scatter_sum(product_columns(gated, proj, place, core, slice(width, None)))
    resid = (tokens.astype(jnp.float32) + mix).astype(jnp.bfloat16)
    whole2 = tp_gather(resid, 1)
    normed2 = to_ring(
        rms_norm(whole2.astype(jnp.float32), gains[1]).astype(jnp.bfloat16), place, core
    )
    gate_part = product_rows(normed2[:1], gates[:1])
    up_part = product_rows(normed2[:1], ups[:1])
    early_parts = (gate_part, up_part)
    gate_part = product_rows(normed2[1:], gates[1:], result=gate_part)
    up_part = product_rows(normed2[1:], ups[1:], result=up_part)
    hidden = (jax.nn.silu(gate_part) * up_part).astype(jnp.bfloat16)
    near = (gate_hops[-reach], gate_hops[reach])
    far = order_of(size)[-1][-1]
    second = (normed2[0][0], up_hops[-reach], up_hops[reach])
    third = early_parts + (gate_hops[far], up_hops[far])
    _, downs = circulate(ff_down, 1, (near, second, third))
    ffn = tp_scatter_sum(product_columns(hidden, downs, place, core))
    total = resid.astype(jnp.float32) + ffn
    squares = tp_sum(jnp.sum(total * total, axis=-1))[:, None]
    scale = lax.rsqrt(squares / D + EPS)
    return (total * scale * final_gain.astype(jnp.float32)).astype(jnp.bfloat16)


MESH = pl.DeviceIdType.MESH
F32 = jnp.float32
BF16 = jnp.bfloat16
WIDE = 256


def silu(v):
    return v / (1.0 + jnp.exp(-v))


def mm(a, b):
    return jnp.dot(a, b, preferred_element_type=F32)


def layer_kernel(
    tok_h,
    mixg_h,
    ffng_h,
    lastg_h,
    q_h,
    k_h,
    v_h,
    g_h,
    o_h,
    rate_s,
    scale_s,
    fg_h,
    fu_h,
    fd_h,
    cos_h,
    sin_h,
    out_h,
    tok,
    gn,
    gl,
    gf,
    gs,
    gr,
    cos_ref,
    sin_ref,
    Ps,
    P,
    O,
    G,
    U,
    Dn,
    pr,
    gsend,
    gated,
    sm,
    pm,
    rm,
    R,
    N2,
    gacc,
    uacc,
    hid,
    sx,
    rx,
    pmine,
    sz,
    rz,
    rd,
    tot,
    ss_s,
    ss_r,
    lsem,
    ssem,
    wsem,
    asem,
    osem,
):
    rows, feat = tok_h.shape
    width = 2 * feat
    rw = q_h.shape[0]
    cw = o_h.shape[1]
    half_ff = fg_h.shape[1] // 2
    heads = rate_s.shape[0]
    f = lax.axis_index("fs")
    x = lax.axis_index("tp")
    c = f % 2
    y = (f // 2) % 2
    z = f // 4
    b = z // 2
    zp = 4 * b + 1 - z
    zm = 3 - z
    near_o = 2 - b
    far_o = 3 * (1 - b)
    near = jnp.logical_or(z == 1, z == 2)
    far = jnp.logical_not(near)
    y1, c1, x1 = 1 - y, 1 - c, 1 - x

    def dev(zz, yy, cc, xx):
        return ((zz * 2 + yy) * 2 + cc, xx)

    here = x == b
    away = jnp.logical_not(here)
    end_here, end_away = jnp.logical_and(far, here), jnp.logical_and(far, away)
    mid_here, mid_away = jnp.logical_and(near, here), jnp.logical_and(near, away)
    roles = (None, near, far, here, away, end_here, end_away, mid_here, mid_away)
    pools = ((0, 28), (28, 36), (28, 36), (64, 8), (64, 8), (72, 1), (72, 1), (72, 1), (72, 1))
    sends = [[] for _ in roles]
    drained = [0 for _ in roles]
    role = [0]

    def put(src, dst, sem, to):
        base, size = pools[role[0]]
        copies = sends[role[0]]
        index = base + len(copies) % size

        def copy():
            return pltpu.make_async_remote_copy(
                src_ref=src(),
                dst_ref=dst(),
                send_sem=ssem.at[index],
                recv_sem=sem(),
                device_id=to,
                device_id_type=MESH,
            )

        if len(copies) - size >= drained[role[0]]:
            copies[len(copies) - size]().wait_send()
        copy().start()
        copies.append(copy)

    def drain(*which):
        for k, who in enumerate(roles):
            if which and not any(who is w for w in which):
                continue
            size = pools[k][1]
            copies = sends[k][max(drained[k], len(sends[k]) - size) :]

            def wait(copies=copies):
                for copy in copies:
                    copy().wait_send()

            if copies:
                wait() if who is None else pl.when(who)(wait)
            drained[k] = len(sends[k])

    def only(who, *acts):
        @pl.when(who)
        def _():
            role[0] = [who is r for r in roles].index(True)
            for act, *args in acts:
                act(*args)
            role[0] = 0

    def got(ref, sem, name="got"):
        copy = pltpu.make_async_remote_copy(
            src_ref=ref,
            dst_ref=ref,
            send_sem=ssem.at[0],
            recv_sem=sem,
            device_id=dev(z, y, c1, x),
            device_id_type=MESH,
        )
        with jax.named_scope(name):
            copy.wait_recv()

    local = []

    def take(src, dst):
        copy = pltpu.make_async_copy(src, dst, lsem.at[len(local)])
        copy.start()
        local.append(copy)
        return copy

    def row_slot(buf):
        def slot(zz, yy, cc):
            start = pl.multiple_of(((zz * 2 + yy) * 2 + cc) * rw, rw)
            return buf.at[pl.ds(start, rw), :]

        return slot

    def col_slot(buf):
        def slot(zz, yy, cc):
            return buf.at[zz * 2 + yy, :, pl.ds(pl.multiple_of(cc * cw, cw), cw)]

        return slot

    deep = half_ff // 2

    def down_slot(k):
        def slot(zz, yy, cc):
            return Dn.at[zz * 2 + yy, pl.ds(k * deep, deep), pl.ds(pl.multiple_of(cc * cw, cw), cw)]

        return slot

    sP, sO, sG, sU = row_slot(P), col_slot(O), row_slot(G), row_slot(U)
    slots = (sP, sO, sG, sU, down_slot(0), down_slot(1))
    DOWN = (4, 5)

    def sem_of(kind, zz, yy, cc):
        return wsem.at[kind, (zz * 2 + yy) * 2 + cc]

    def fwd(kind, zz, yy, cc, to):
        ref = functools.partial(slots[kind], zz, yy, cc)
        put(ref, ref, functools.partial(sem_of, kind, zz, yy, cc), to)

    def arrive(kind, zz, yy, cc):
        side = "sib" if cc is c1 else "row" if yy is y1 else "col"
        got(slots[kind](zz, yy, cc), sem_of(kind, zz, yy, cc), f"{side}{kind}")

    sib = dev(z, y, c1, x)
    row = dev(z, y1, c, x)
    peer = dev(zp, y, c, x)
    xdev = dev(z, y, c, x1)
    mirror = dev(zm, y, c, x)
    diagonal = dev(zm, y, c, x1)

    parts = [ref.shape[1] // 2 for ref in (q_h, k_h, v_h, g_h)]
    ends = np.cumsum([0] + parts).tolist()
    mine = pl.multiple_of(((z * 2 + y) * 2 + c) * rw, rw)
    own_p, stage_p = [], []
    for i, ref in enumerate((q_h, k_h, v_h, g_h)):
        to = pl.ds(ends[i], parts[i])
        at = pl.ds(pl.multiple_of(y * parts[i], 128), parts[i])
        own_p.append(take(ref.at[:, at], P.at[pl.ds(mine, rw), to]))
        at = pl.ds(pl.multiple_of(y1 * parts[i], 128), parts[i])
        stage_p.append(take(ref.at[:, at], Ps.at[:, to]))
    own_o = take(o_h, sO(z, y, c))
    own_t = [take(tok_h, tok.at[0, x])] + [take(ref, gn.at[x, k]) for k, ref in enumerate((mixg_h, ffng_h))]
    own_t += [take(cos_h, cos_ref), take(sin_h, sin_ref), take(lastg_h, gl)]
    gs[...] = jnp.where(lax.broadcasted_iota(jnp.int32, gs.shape, 0) == 0, scale_s[0], scale_s[1])
    at_b = pl.multiple_of(b * half_ff, 128)
    at_o = pl.multiple_of((1 - b) * half_ff, 128)
    own_g = take(fg_h.at[:, pl.ds(at_b, half_ff)], sG(z, y, c))
    own_u = take(fu_h.at[:, pl.ds(at_b, half_ff)], sU(z, y, c))
    own_d = take(fd_h.at[pl.ds(at_b, half_ff), :], col_slot(Dn)(z, y, c))

    barrier = pltpu.get_barrier_semaphore()
    friends = [sib, row, xdev, diagonal] + [dev((z + k) % 4, y, c, x) for k in (1, 2, 3)]
    for to in friends:
        pl.semaphore_signal(barrier, inc=1, device_id=to, device_id_type=MESH)
    pl.semaphore_wait(barrier, len(friends))

    put(lambda: tok_h, lambda: tok.at[0, x], lambda: asem.at[0], xdev)
    put(lambda: mixg_h, lambda: gn.at[x, 0], lambda: asem.at[1], xdev)
    put(lambda: ffng_h, lambda: gn.at[x, 1], lambda: asem.at[35], xdev)

    other = {
        2: lambda: fg_h.at[:, pl.ds(at_o, half_ff)],
        3: lambda: fu_h.at[:, pl.ds(at_o, half_ff)],
        4: lambda: fd_h.at[pl.ds(at_o, deep), :],
        5: lambda: fd_h.at[pl.ds(pl.multiple_of(at_o + deep, 16), deep), :],
    }
    beyond = dev(near_o, y, c, x)

    def own(kind, to):
        fwd(kind, z, y, c, to)

    def cross(kind):
        slot = functools.partial(slots[kind], z, y, c)
        put(other[kind], slot, functools.partial(sem_of, kind, z, y, c), beyond)

    def relay(kind, zz, *to):
        arrive(kind, zz, y, c)
        for device in to + (row, sib):
            fwd(kind, zz, y, c, device)

    def arrive_down(*place):
        for kind in DOWN:
            arrive(kind, *place)

    def down(act, *args):
        return [(act, kind) + args for kind in DOWN]

    def lend(kind):
        arrive(kind, z, y1, c)
        fwd(kind, z, y1, c, peer)
        fwd(kind, z, y1, c, sib)

    def relay_in(kind, zz):
        arrive(kind, zz, y, c)
        fwd(kind, zz, y, c, sib)

    def shared(kind, zz):
        arrive(kind, zz, y1, c)
        fwd(kind, zz, y1, c, sib)

    def share(kind):
        for zz in (z, zp, near_o, far_o):
            arrive(kind, zz, y1, c)
            fwd(kind, zz, y1, c, sib)

    def line(zz, yy, *to):
        arrive(0, zz, yy, c)
        for device in to + (sib,):
            fwd(0, zz, yy, c, device)

    for copy in stage_p + own_p:
        copy.wait()
    put(lambda: Ps, lambda: sP(z, y, c), lambda: sem_of(0, z, y, c), row)
    own(0, peer)
    only(near, (own, 0, beyond))
    own(0, sib)
    put(lambda: tok_h, lambda: tok.at[1, x], lambda: asem.at[2], row)
    put(lambda: gs, lambda: gr, lambda: asem.at[3], row)
    own_o.wait()
    own(1, row)
    own(1, peer)
    only(near, (own, 1, beyond))
    own(1, sib)
    own_g.wait()
    own(2, row)
    own(2, sib)
    only(far, (line, z, y1, peer), (own, 2, peer), (line, zp, y), (relay, 1, zp), (line, zp, y1))
    only(
        near,
        (line, z, y1, peer, beyond),
        (line, zp, y, beyond),
        (line, near_o, y, peer),
        (relay, 1, zp, beyond),
        (relay, 1, near_o, peer),
        (line, zp, y1, beyond),
        (line, near_o, y1, peer),
    )

    for copy in own_t:
        copy.wait()
    got(tok.at[0, x1], asem.at[0], "tok")
    got(gn.at[x1, 0], asem.at[1])
    got(gn.at[x1, 1], asem.at[35])

    def norm_rows(first, second, gain_row, dst, base):
        chunk = 32
        gains = [gn[half, gain_row].astype(F32) for half in range(2)]

        @pl.loop(0, rows // chunk)
        def _(i):
            at = pl.ds(pl.multiple_of(i * chunk, chunk), chunk)
            one = first[at, :].astype(F32)
            two = second[at, :].astype(F32)
            total = jnp.sum(one * one, axis=1, keepdims=True) + jnp.sum(two * two, axis=1, keepdims=True)
            scale = lax.rsqrt(total / width + EPS)
            to = pl.ds(pl.multiple_of(base + i * chunk, chunk), chunk)
            for half, values in enumerate((one, two)):
                for k in range(feat // 128):
                    part = values[:, k * 128 : (k + 1) * 128] * scale * gains[half][k : k + 1, :]
                    dst[to, half * feat + k * 128 : half * feat + (k + 1) * 128] = part.astype(BF16)

    norm_rows(tok.at[0, 0], tok.at[0, 1], 0, N2, 0)
    got(tok.at[1, x], asem.at[2], "tok")
    put(lambda: tok.at[1, x], lambda: tok.at[1, x], lambda: asem.at[4], xdev)
    got(gr, asem.at[3])
    own_u.wait()
    own_d.wait()
    only(
        far,
        (line, near_o, y),
        (line, near_o, y1),
        (relay, 1, near_o),
        (own, 3, row),
        (cross, 2),
        (line, far_o, y),
        (line, far_o, y1),
        (relay, 1, far_o),
        (own, 3, peer),
        (cross, 3),
    )
    only(
        near,
        (line, far_o, y, peer),
        (line, far_o, y1, peer),
        (relay, 1, far_o, peer),
        (own, 2, peer),
        (cross, 2),
        (relay, 2, zp),
        (cross, 3),
    )
    got(tok.at[1, x1], asem.at[4], "tok")
    norm_rows(tok.at[1, 0], tok.at[1, 1], 0, N2, rows)
    for zz in range(4):
        for yy in range(2):
            arrive(0, zz, yy, c1)

    @pl.loop(0, P.shape[1] // WIDE)
    def _(j):
        at = pl.ds(pl.multiple_of(j * WIDE, WIDE), WIDE)
        pr[:, at] = mm(N2[...], P[:, at])

    blk = rows // 2
    t = lax.broadcasted_iota(jnp.int32, (rows, rows), 0)
    s = lax.broadcasted_iota(jnp.int32, (rows, rows), 1)
    late_t, late_s = t >= blk, s >= blk
    apart = (t - s).astype(F32)
    into = (t - (blk - 1)).astype(F32)
    left = ((blk - 1) - s).astype(F32)
    causal = t >= s
    lane = lax.broadcasted_iota(jnp.int32, (rows, 2 * DK), 1)
    early = (lane % DK) < DK // 2
    first_head = lane < DK

    def turn(v):
        swapped = jnp.where(early, pltpu.roll(v, 2 * DK - DK // 2, 1), pltpu.roll(v, DK // 2, 1))
        return v * cos_ref[...] + swapped * sin_ref[...]

    def retain_rows(at, scales, dst):
        s0, s1 = scales[0:1, 0:1], scales[1:2, 0:1]
        for two in range(heads // 4):
            cols = slice(ends[0] + two * 2 * DK, ends[0] + (two + 1) * 2 * DK)
            query = turn(pr[at, cols]).astype(BF16)
            cols = slice(ends[1] + two * 2 * DK, ends[1] + (two + 1) * 2 * DK)
            key = (turn(pr[at, cols]) * DK ** (-0.5)).astype(BF16)
            for side in range(2):
                h = 2 * two + side
                rate = rate_s[y * (heads // 2) + h]
                keep = first_head if side == 0 else jnp.logical_not(first_head)
                part = jnp.where(keep, query, jnp.zeros_like(query))
                scores = lax.dot_general(part, key, (((1,), (1,)), ((), ())), preferred_element_type=F32)
                la0, la1 = -(rate * s0), -(rate * s1)
                power = jnp.where(late_t, la1, la0) * apart
                power = jnp.where(jnp.logical_and(late_t, jnp.logical_not(late_s)), la1 * into + la0 * left, power)
                scores = scores * jnp.where(causal, jnp.exp(jnp.where(causal, power, 0.0)), 0.0)
                high = scores.astype(BF16)
                low = (scores - high.astype(F32)).astype(BF16)
                value = pr[at, ends[2] + h * DV : ends[2] + (h + 1) * DV].astype(BF16)
                ret = mm(high, value) + mm(low, value)
                ret = ret * lax.rsqrt(jnp.mean(ret * ret, axis=1, keepdims=True) + EPS)
                gate = pr[at, ends[3] + h * DV : ends[3] + (h + 1) * DV]
                dst[:, h * DV : (h + 1) * DV] = (ret * silu(gate)).astype(BF16)

    retain_rows(slice(rows, 2 * rows), gr, gsend)
    put(lambda: gsend, lambda: gated.at[y], lambda: asem.at[5], row)
    retain_rows(slice(0, rows), gs, gated.at[y])
    only(far, (relay, 2, zp), (own, 3, sib))
    only(near, (relay, 2, near_o, peer))
    share(1)
    for zz in range(4):
        for yy in range(2):
            arrive(1, zz, yy, c1)
    got(gated.at[y1], asem.at[5], "gated")

    per = feat // WIDE
    half_o = O.shape[1] // 2

    def out_block(side, j):
        weights = O.at[side * per + j]
        return mm(gated[0], weights[0:half_o, :]) + mm(gated[1], weights[half_o:, :])

    def send_mix(j):
        put(lambda: sm.at[j], lambda: rm.at[j], lambda: asem.at[6 + j], xdev)

    for j in range(per):
        sm[j] = out_block(x1, j).astype(BF16)
        send_mix(j)
    for j in range(per):
        pm[j] = out_block(x, j).astype(BF16)

    only(far, (relay, 2, near_o), *down(own, row), *down(own, sib))
    only(
        near,
        (relay, 2, far_o, peer),
        (own, 3, peer),
        (own, 3, row),
        (own, 3, sib),
        (relay_in, 3, zp),
    )

    def block(j):
        return pl.ds(j * WIDE, WIDE)

    def send_resid(j):
        put(lambda: R.at[0, x, :, block(j)], lambda: R.at[1, x, :, block(j)], lambda: asem.at[10 + j], mirror)
        put(lambda: R.at[0, x, :, block(j)], lambda: R.at[0, x, :, block(j)], lambda: asem.at[14 + j], xdev)

    def pass_resid(j):
        got(R.at[1, x, :, block(j)], asem.at[10 + j], "R1")
        put(lambda: R.at[1, x, :, block(j)], lambda: R.at[1, x, :, block(j)], lambda: asem.at[18 + j], xdev)

    for j in range(per):
        got(rm.at[j], asem.at[6 + j], "mix")
        mix = pm[j].astype(F32) + rm[j].astype(F32)
        R[0, x, :, block(j)] = (tok[0, x, :, block(j)].astype(F32) + mix).astype(BF16)
        send_resid(j)
    only(far, (relay, 2, far_o), *down(own, peer), (lend, 3), (relay, 3, zp))
    only(near, (relay, 3, near_o, peer), (relay, 3, far_o, peer), *down(own, row), *down(own, sib))
    pass_resid(0)
    pass_resid(1)
    only(near, *down(cross), *down(own, peer))
    only(far, *down(cross), (relay, 3, near_o))
    pass_resid(2)
    pass_resid(3)
    only(near, *down(relay_in, zp))
    only(far, *down(lend), (relay, 3, far_o))
    share(2)
    for j in range(per):
        got(R.at[0, x1, :, block(j)], asem.at[14 + j], "R0x")
    norm_rows(R.at[0, 0], R.at[0, 1], 1, N2, 0)
    for j in range(per):
        got(R.at[1, x1, :, block(j)], asem.at[18 + j], "R1x")
    norm_rows(R.at[1, 0], R.at[1, 1], 1, N2, rows)

    theirs, ours = slice(rows, 2 * rows), slice(0, rows)

    def over_columns(act):
        whole = half_ff // WIDE

        @pl.loop(0, whole)
        def _(j):
            act(pl.ds(pl.multiple_of(j * WIDE, WIDE), WIDE))

        if half_ff % WIDE:
            act(pl.ds(whole * WIDE, half_ff % WIDE))

    def gate_columns(at):
        gacc[:, at] = silu(mm(N2[...], G[:, at]))

    def up_of(part, at, *chips):
        total = 0.0
        for zz, yy in chips:
            deep_at = pl.ds(pl.multiple_of((zz * 2 + yy) * 2 * rw, 2 * rw), 2 * rw)
            total = total + mm(N2[part, deep_at], U[deep_at, at])
        return total

    def up_columns(at):
        for part in (theirs, ours):
            uacc[part, at] = up_of(
                part, at, (z, y), (zp, y), (near_o, y), (far_o, y), (z, y1), (zp, y1), (near_o, y1)
            )

    def hidden_columns(at):
        for part in (theirs, ours):
            up = uacc[part, at] + up_of(part, at, (far_o, y1))
            hid[part, at] = (gacc[part, at] * up).astype(BF16)

    def share_up(zz):
        arrive(3, zz, y1, c)
        fwd(3, zz, y1, c, sib)

    only(near, (shared, 3, z))
    share_up(zp)
    for zz in range(4):
        for yy in range(2):
            arrive(2, zz, yy, c1)
    over_columns(gate_columns)
    share_up(near_o)
    only(far, *down(relay, zp))
    for zz in (z, zp, near_o, far_o):
        arrive(3, zz, y, c1)
    for zz in (z, zp, near_o):
        arrive(3, zz, y1, c1)
    over_columns(up_columns)
    share_up(far_o)
    only(near, *down(relay, near_o, peer))
    arrive(3, far_o, y1, c1)
    over_columns(hidden_columns)

    at_end = far.astype(jnp.int32)

    def chip(half, i):
        return jnp.where(i % 2 == 1, 3 * half, 1 + half), jnp.where(i >= 2, y1, y)

    def columns(i):
        zz, yy = chip(x, i)
        return pl.ds(pl.multiple_of(((zz - 2 * x) * 2 + yy) * WIDE, WIDE), WIDE)

    def send_x(i, k, start):
        at = pl.ds(start, rows)
        put(lambda: sx.at[i, at, :], lambda: rx.at[i, at, :], lambda: asem.at[22 + 2 * i + k], xdev)

    def give(zz, yy, i, part):
        sx[i, part, :] = mm(hid[part, :], Dn[zz * 2 + yy]).astype(BF16)
        send_x(i, 0 if part is theirs else 1, part.start)

    def give_last(zz, yy):
        sx[3, theirs, :] = mm(hid[theirs, :], Dn[zz * 2 + yy]).astype(BF16)
        put(lambda: sx.at[3, pl.ds(rows, rows), :], lambda: rd, lambda: asem.at[36], diagonal)

    def keep(zz, yy, i):
        pmine[i] = mm(hid[...], Dn[zz * 2 + yy])

    def ready(zz):
        for kind in DOWN:
            arrive(kind, zz, y1, c)
            fwd(kind, zz, y1, c, sib)

    def combine(i):
        got(rx.at[i, pl.ds(rows, rows), :], asem.at[22 + 2 * i], "rx")
        sz[i] = (pmine[i, theirs, :] + rx[i, theirs, :].astype(F32)).astype(BF16)
        put(lambda: sz.at[i], lambda: rz.at[i], lambda: asem.at[30 + i], mirror)

    def pass_last():
        sz[3] = pmine[3, theirs, :].astype(BF16)
        put(lambda: sz.at[3], lambda: rz.at[3], lambda: asem.at[33], mirror)

    def take_last():
        got(rd, asem.at[36], "rd")
        tot[3] = tot[3] + rd[...].astype(F32)

    def add(i):
        got(rx.at[i, pl.ds(0, rows), :], asem.at[23 + 2 * i], "rx")
        resid = R[0, x, :, columns(i)].astype(F32)
        tot[i] = resid + (pmine[i, ours, :] + rx[i, ours, :].astype(F32))

    def out_copy(i):
        return pltpu.make_async_copy(tot.at[i], out_h.at[:, columns(i)], osem.at[i])

    def close(i):
        got(rz.at[i], asem.at[30 + i], "rz")
        now = tot[i] + rz[i].astype(F32)
        tot[i] = now
        square = now * now
        return square[:, : WIDE // 2] + square[:, WIDE // 2 :]

    first = (at_end, 1 - at_end, 2 + at_end, 3 - at_end)
    order = [jnp.where(here, i, k) for k, i in enumerate(first)]
    b0, b1, b2, b3 = first
    arrive_down(z, y, c1)
    arrive_down(zp, y, c1)
    only(
        away,
        (give, z, y, b0, theirs),
        (give, zp, y, b1, theirs),
        (give, z, y, b0, ours),
    )
    only(here, (keep, z, y, b0), (keep, zp, y, b1))
    only(far, *down(relay, near_o))
    only(near, *down(relay, far_o, peer))
    arrive_down(near_o, y, c1)
    only(here, (give, near_o, y, 0, theirs))
    only(far, *down(relay, far_o))
    only(near, *down(shared, z))
    ready(zp)
    arrive_down(far_o, y, c1)
    only(here, (give, far_o, y, 1, theirs), (give, near_o, y, 0, ours), (give, far_o, y, 1, ours))
    arrive_down(z, y1, c1)
    arrive_down(zp, y1, c1)
    only(
        away,
        (give, z, y1, b2, theirs),
        (give, zp, y1, b3, theirs),
        (give, zp, y, b1, ours),
        (give, z, y1, b2, ours),
        (give, zp, y1, b3, ours),
        (keep, near_o, y, 0),
        (keep, far_o, y, 1),
    )
    only(here, (keep, z, y1, b2), (keep, zp, y1, b3))
    combine(order[0])
    ready(near_o)
    combine(order[1])
    arrive_down(near_o, y1, c1)
    only(here, (give, near_o, y1, 2, theirs), (give, near_o, y1, 2, ours))
    only(away, (keep, near_o, y1, 2))
    only(here, (combine, order[2]), (combine, order[3]))
    ready(far_o)
    arrive_down(far_o, y1, c1)
    only(end_here, (give_last, far_o, y1))
    only(mid_here, (give, far_o, y1, 3, theirs))
    only(here, (give, far_o, y1, 3, ours))
    only(away, (keep, far_o, y1, 3))
    only(end_away, (pass_last,))
    drain(near, far)
    only(away, (combine, 2))
    add(order[0])
    add(order[1])
    squares = close(order[0])
    only(mid_away, (combine, 3))
    squares = squares + close(order[1])
    add(order[2])
    add(order[3])
    only(end_here, (take_last,))
    squares = squares + close(order[2])
    squares = squares + close(order[3])
    mine_sq = jnp.broadcast_to(jnp.sum(squares, axis=1, keepdims=True), (rows, 128))
    ss_s[...] = mine_sq.T[0:8, :]
    put(lambda: ss_s, lambda: ss_r, lambda: asem.at[34], xdev)
    gf[...] = gl[...].astype(F32)
    drain()
    got(ss_r, asem.at[34], "ss")
    total = ss_s[0:1, :] + ss_r[0:1, :]
    total = jnp.broadcast_to(total, (128, rows)).T[:, 0:1]
    scale = lax.rsqrt(total / width + EPS)
    for i in range(4):
        zz, yy = chip(x, i)
        for k in range(WIDE // 128):
            gain = gf[pl.ds(((zz - 2 * x) * 2 + yy) * (WIDE // 128) + k, 1), :]
            lanes = slice(k * 128, (k + 1) * 128)
            tot[i, :, lanes] = tot[i, :, lanes] * scale * gain
        out_copy(i).start()
    for i in range(4):
        out_copy(i).wait()


def tables(rows):
    half = DK // 2
    inverse = np.float32(THETA) ** (-np.arange(half, dtype=np.float32) / np.float32(half))
    angle = (np.arange(rows, dtype=np.float32) % SEQ_LEN)[:, None] * inverse
    cosine, sine = np.cos(angle), np.sin(angle)
    return (
        np.concatenate([cosine] * 4, axis=1).astype(np.float32),
        np.concatenate([-sine, sine, -sine, sine], axis=1).astype(np.float32),
    )


def fused(
    tokens,
    mix_gain,
    query_weight,
    key_weight,
    value_weight,
    output_gate_weight,
    out_weight,
    head_rates,
    block_scale,
    ffn_gain,
    ff_gate,
    ff_up,
    ff_down,
    final_gain,
):
    rows, feat = tokens.shape
    size = lax.axis_size("fs")
    chips = size // 2
    width = 2 * feat
    half_ff = ff_gate.shape[1] // 2
    joint = sum(w.shape[1] for w in (query_weight, key_weight, value_weight, output_gate_weight)) // 2
    heads = head_rates.shape[0]
    cosine, sine = tables(rows)
    cw = out_weight.shape[1]
    hbm = pl.BlockSpec(memory_space=pl.ANY)
    smem = pl.BlockSpec(memory_space=pltpu.SMEM)
    dma = pltpu.SemaphoreType.DMA
    out = pl.pallas_call(
        layer_kernel,
        out_shape=jax.ShapeDtypeStruct((rows, feat), F32),
        in_specs=[hbm] * 9 + [smem] * 2 + [hbm] * 5,
        out_specs=hbm,
        scratch_shapes=[
            pltpu.VMEM((2, 2, rows, feat), BF16),
            pltpu.VMEM((2, 2, feat // 128, 128), BF16),
            pltpu.VMEM((feat // 128, 128), BF16),
            pltpu.VMEM((feat // 128, 128), F32),
            pltpu.VMEM((8, 128), F32),
            pltpu.VMEM((8, 128), F32),
            pltpu.VMEM((rows, 128), F32),
            pltpu.VMEM((rows, 128), F32),
            pltpu.VMEM((query_weight.shape[0], joint), BF16),
            pltpu.VMEM((width, joint), BF16),
            pltpu.VMEM((chips, out_weight.shape[0], 2 * cw), BF16),
            pltpu.VMEM((width, half_ff), BF16),
            pltpu.VMEM((width, half_ff), BF16),
            pltpu.VMEM((chips, half_ff, 2 * cw), BF16),
            pltpu.VMEM((2 * rows, joint), F32),
            pltpu.VMEM((rows, heads * DV // 2), BF16),
            pltpu.VMEM((2, rows, heads * DV // 2), BF16),
            pltpu.VMEM((feat // WIDE, rows, WIDE), BF16),
            pltpu.VMEM((feat // WIDE, rows, WIDE), BF16),
            pltpu.VMEM((feat // WIDE, rows, WIDE), BF16),
            pltpu.VMEM((2, 2, rows, feat), BF16),
            pltpu.VMEM((2 * rows, width), BF16),
            pltpu.VMEM((2 * rows, half_ff), F32),
            pltpu.VMEM((2 * rows, half_ff), F32),
            pltpu.VMEM((2 * rows, half_ff), BF16),
            pltpu.VMEM((4, 2 * rows, WIDE), BF16),
            pltpu.VMEM((4, 2 * rows, WIDE), BF16),
            pltpu.VMEM((4, 2 * rows, WIDE), F32),
            pltpu.VMEM((4, rows, WIDE), BF16),
            pltpu.VMEM((4, rows, WIDE), BF16),
            pltpu.VMEM((rows, WIDE), BF16),
            pltpu.VMEM((4, rows, WIDE), F32),
            pltpu.VMEM((8, rows), F32),
            pltpu.VMEM((8, rows), F32),
            dma((18,)),
            dma((73,)),
            dma((6, size)),
            dma((37,)),
            dma((4,)),
        ],
        compiler_params=pltpu.CompilerParams(
            collective_id=0, has_side_effects=True, vmem_limit_bytes=60 * 2**20
        ),
    )(
        tokens,
        mix_gain.reshape(feat // 128, 128),
        ffn_gain.reshape(feat // 128, 128),
        final_gain.reshape(feat // 128, 128),
        query_weight,
        key_weight,
        value_weight,
        output_gate_weight,
        out_weight,
        head_rates,
        block_scale,
        ff_gate,
        ff_up,
        ff_down,
        cosine,
        sine,
    )
    return out.astype(BF16)


def kernel_fits(mesh, tokens, query_weight, ff_gate, head_rates):
    size, parts = mesh.shape["fs"], mesh.shape["tp"]
    if size != 4 * 2 * 2 or parts != 2:
        return False
    rows, width = tokens.shape[0] // size, tokens.shape[1]
    return (
        rows == SEQ_LEN
        and SEQ_LEN == 2 * BLK
        and width // size * 2 == WIDE
        and ff_gate.shape[1] % (4 * 128) == 0
        and head_rates.shape[0] % (4 * parts) == 0
    )


def dispatch(mesh, *args):
    fits = kernel_fits(mesh, args[0], args[2], args[10], args[7])
    return jax.shard_map(
        fused if fits else body,
        mesh=mesh,
        in_specs=SPECS,
        out_specs=P("fs", "tp"),
        check_vma=False,
    )(*args)


SPECS = (
    P("fs", "tp"),
    P("tp"),
    P("fs", "tp"),
    P("fs", "tp"),
    P("fs", "tp"),
    P("fs", "tp"),
    P("tp", "fs"),
    P("tp"),
    P("fs"),
    P("tp"),
    P("fs", "tp"),
    P("fs", "tp"),
    P("tp", "fs"),
    P("tp"),
)


def solution(mesh):
    return functools.partial(dispatch, mesh)
```
